256 devices in a mesh: sp: 64 (over z, x, core), tp: 4 (over y).
Axes of the slice: x: 4, y: 4, z: 8, core: 2. Of those that a mesh axis runs over, the one named last changes fastest.
Arguments:
- residual_in: bfloat16 [65536, 2048], P(('sp', 'tp')), may hold values from -6 to 6
- gate_outer: bfloat16 [65536, 1024], P('sp', 'tp'), may hold values from -6 to 6
- gate_inner: bfloat16 [65536, 1024], P('sp', 'tp'), may hold values from -6 to 6
- conv_input: bfloat16 [65536, 1024], P('sp', 'tp'), may hold values from -6 to 6
- conv_taps: bfloat16 [3, 1024], P(None, 'tp'), may hold values from -5 to 5
- norm_gain: bfloat16 [1024], P('tp'), may hold values from 0.099609375 to 1.8984375
- out_weight: bfloat16 [1024, 2048], P('tp'), may hold values from -0.1875 to 0.1875
- moe_gain: bfloat16 [2048], replicated, may hold values from 0.099609375 to 1.8984375
- expert_ids: int32 [65536, 2], P(('sp', 'tp')), may hold values from 0 to 63, all different within a row; in each aligned block of 256 rows (0 to 255, 256 to 511, ...) at most 16 rows name the same one
- group_prob: float32 [65536], P(('sp', 'tp')), may hold values from 0.3 to 1
- route_prob: float32 [65536, 2], P(('sp', 'tp')), may hold values from 0.1 to 1
- expert_gate: bfloat16 [64, 2048, 512], P('sp'), may hold values from -0.125 to 0.125
- expert_up: bfloat16 [64, 2048, 512], P('sp'), may hold values from -0.125 to 0.125
- expert_down: bfloat16 [64, 512, 2048], P('sp'), may hold values from -0.25 to 0.25
Outputs:
- layer_out: bfloat16 [65536, 2048], P(('sp', 'tp'))
The draws below stay inside these ranges and needn't reach their ends.
Inputs may be any that keep to these rules, and one draw needn't show every extreme that they name: `expert_ids`: each row names 2 different experts. Within the rows of one device (aligned blocks of 256 rows) no expert is named more than 16 times.
All inputs are finite; a program needn't handle non-finite values.
Results may differ from the reference program's by a relative error of at most 0.0075.
Values may be sent and summed in bfloat16 or wider, within the bound.
A program may use at most 64 MiB of HBM per device.

```python
import math
import jax
import jax.numpy as jnp
import numpy as np
from jax import lax

D = 2048
CONV = 1024
FE = 512
KW = 3
TOPK = 2
ROWS_DEV = 256
TOKENS = 65536
EXPERTS = 64
CAPACITY = 16


def draw_conv_taps(key, part):
    first, second = jax.random.split(key)
    base = jnp.clip(jax.random.normal(first, (KW, CONV), jnp.float32), -3.0, 3.0) / jnp.sqrt(jnp.float32(KW))
    levels = jnp.array([0.35, 0.7, 1.4, 2.8], jnp.float32)
    shuffled = levels[jax.random.permutation(second, 4)]
    quarter = jnp.arange(CONV, dtype=jnp.int32) * 4 // CONV
    return (base * shuffled[quarter][None, :]).astype(jnp.bfloat16)


def shard_levels(stream_key, extent, pieces, low, high):
    factor_of, own = 1.0, jax.random.fold_in(stream_key, 6)
    for position, blocks in pieces:
        steps = jnp.exp(jax.random.uniform(jax.random.fold_in(own, position), (blocks,), jnp.float32, low / len(pieces), high / len(pieces)))
        factor_of = factor_of * jnp.repeat(steps, extent[position] // blocks).reshape([-1 if axis == position else 1 for axis in range(len(extent))])
    return factor_of


def assign_block(key, own, number, rows, number_of, top, reach, slope):
    ranking = jax.random.permutation(key, number_of)
    heavy_load, common = shares(number_of, rows * top, reach, slope, True), shares(number_of, rows * top, reach, slope, False)
    places = jnp.arange(number_of)

    def named(sizes, turn):
        used = int((sizes > 0).sum())
        fixed = max(1, used // 4)
        moved = fixed + (places - fixed + turn * (used - fixed)) % max(1, number_of - fixed)
        return jnp.zeros((number_of,), jnp.int32).at[ranking[jnp.where(places < fixed, places, moved)]].set(jnp.asarray(sizes, jnp.int32))

    sizes = jnp.where(number % 4 == 0, named(heavy_load, number // 4), named(common, number - number // 4 - 1))
    mixed = jax.random.permutation(jax.random.fold_in(own, 3), number_of)
    donor, receiver = mixed[0:number_of // 2 * 2:2], mixed[1:number_of // 2 * 2:2]
    margin = jnp.minimum(sizes[donor] - 1, reach - sizes[receiver]) // 2
    margin = jnp.where((donor == ranking[0]) | (receiver == ranking[0]) | (sizes[receiver] == 0), 0, jnp.maximum(margin, 0))
    moved = jax.random.randint(jax.random.fold_in(own, 4), (number_of // 2,), 0, 1 << 20) % (margin + 1)
    sizes = sizes.at[donor].add(-moved).at[receiver].add(moved)
    items = jnp.searchsorted(jnp.cumsum(sizes), jnp.arange(rows * top), side="right").astype(jnp.int32)
    listing = items.reshape(top, rows).T
    listing = listing[jax.random.permutation(jax.random.fold_in(own, 1), rows)]
    turn = jax.random.randint(jax.random.fold_in(own, 2), (rows, 1), 0, top)
    return jnp.take_along_axis(listing, (jnp.arange(top)[None, :] + turn) % top, axis=1)


def shares(count, total, reach, slope, full):
    loads = [(1 << 20) // math.isqrt(rank ** slope) + 1 for rank in range(1, count + 1)]
    largest = reach if full else min(reach, max(-(-total // count), total * loads[0] // sum(loads)))
    least = 1 if total - largest >= count - 1 else 0
    holding, rest = [largest] + [least] * (count - 1), total - largest - least * (count - 1)
    while rest > 0:
        candidates = [i for i in range(1, count) if holding[i] < largest] or [i for i in range(1, count) if holding[i] < reach]
        pool, left = sum([loads[i] for i in candidates]), rest
        for i in candidates:
            more = min(reach - holding[i], max(1, left * loads[i] // pool), rest)
            holding[i] = holding[i] + more
            rest = rest - more
    return np.array(holding)


def normal_values(stream_key, dims, deviation, most, cuts=(), kind=jnp.bfloat16):
    values = jax.random.normal(stream_key, dims, jnp.float32) * deviation
    if len(cuts) > 0:
        values = shard_levels(stream_key, dims, cuts, -0.22, 0.18) * values
    return jnp.clip(values, min=-most, max=most).astype(kind)


def setup_inputs(seed: int = 0) -> dict:
    key_list = jax.random.split(jax.random.key(seed), 15)
    residual_in = normal_values(key_list[0], (TOKENS, D), 1.0, 6.0, ((0, 256),))
    gate_outer = normal_values(key_list[1], (TOKENS, CONV), 1.0, 6.0, ((0, 64), (1, 4)))
    gate_inner = normal_values(key_list[2], (TOKENS, CONV), 1.0, 6.0, ((0, 64), (1, 4)))
    conv_input = normal_values(key_list[3], (TOKENS, CONV), 1.0, 6.0, ((0, 64), (1, 4)))
    conv_taps = draw_conv_taps(jax.random.fold_in(key_list[14], 71), 0)
    norm_gain = jnp.clip(1.0 + 0.18 * jax.random.normal(key_list[5], (CONV,), jnp.float32), 0.099609375, 1.8984375).astype(jnp.bfloat16)
    out_weight = normal_values(key_list[6], (CONV, D), CONV ** -0.5, 0.1875, ((0, 4),))
    moe_gain = jnp.clip(1.0 + 0.18 * jax.random.normal(key_list[7], (D,), jnp.float32), 0.099609375, 1.8984375).astype(jnp.bfloat16)
    expert_ids_keys = jax.random.split(jax.random.fold_in(key_list[8], 1), TOKENS // ROWS_DEV)
    expert_ids_turns = jax.random.permutation(jax.random.fold_in(key_list[8], 3), TOKENS // ROWS_DEV)
    expert_ids = jax.vmap(lambda own, number: assign_block(jax.random.fold_in(key_list[8], 2), own, number, ROWS_DEV, EXPERTS, TOPK, CAPACITY, 2))(expert_ids_keys, expert_ids_turns).reshape((TOKENS, TOPK))
    group_prob = jnp.clip(0.3 + 0.7 * jax.random.uniform(key_list[9], (TOKENS,), jnp.float32) ** shard_levels(key_list[9], (TOKENS,), ((0, 256),), -0.2, 0.2), 0.3, 1.0)
    route_prob = jnp.clip(0.1 + 0.9 * jax.random.uniform(key_list[10], (TOKENS, TOPK), jnp.float32) ** shard_levels(key_list[10], (TOKENS, TOPK), ((0, 256),), -0.2, 0.2), 0.1, 1.0)
    expert_gate = normal_values(key_list[11], (EXPERTS, D, FE), D ** -0.5, 0.125, ((0, 64),))
    expert_up = normal_values(key_list[12], (EXPERTS, D, FE), D ** -0.5, 0.125, ((0, 64),))
    expert_down = normal_values(key_list[13], (EXPERTS, FE, D), FE ** -0.5, 0.25, ((0, 64),))
    return dict(residual_in=residual_in, gate_outer=gate_outer, gate_inner=gate_inner, conv_input=conv_input, conv_taps=conv_taps, norm_gain=norm_gain, out_weight=out_weight, moe_gain=moe_gain, expert_ids=expert_ids, group_prob=group_prob, route_prob=route_prob, expert_gate=expert_gate, expert_up=expert_up, expert_down=expert_down)


EPSILON = 1e-06

def rms_norm(values, gain):
    floats = values.astype(jnp.float32)
    factor = lax.rsqrt(lax.optimization_barrier(jnp.mean(floats * floats, axis=-1, keepdims=True)) + EPSILON)
    return floats * factor * gain.astype(jnp.float32)

def reference(residual_in, gate_outer, gate_inner, conv_input, conv_taps, norm_gain, out_weight, moe_gain, expert_ids, group_prob, route_prob, expert_gate, expert_up, expert_down):
    inner = gate_inner.astype(jnp.float32) * conv_input.astype(jnp.float32)
    padded = jnp.concatenate([jnp.zeros((KW - 1, CONV), jnp.float32), inner], axis=0)
    tap_f = conv_taps.astype(jnp.float32)
    filtered = jnp.zeros((TOKENS, CONV), jnp.float32)
    for offset in range(KW):
        filtered = filtered + tap_f[offset][None, :] * padded[offset:offset + TOKENS]
    mixed = (gate_outer.astype(jnp.float32) * filtered).astype(jnp.bfloat16)
    normed = rms_norm(mixed, norm_gain).astype(jnp.bfloat16)
    residual = (residual_in.astype(jnp.float32) + jnp.dot(normed, out_weight, preferred_element_type=jnp.float32)).astype(jnp.bfloat16)
    routed_in = rms_norm(residual, moe_gain).astype(jnp.bfloat16)
    slots = TOKENS * TOPK
    block_rows = 256
    flat_e = expert_ids.reshape(-1).astype(jnp.int32)
    order = jnp.argsort(flat_e, stable=True).astype(jnp.int32)
    sorted_e = flat_e[order]
    counts = jnp.bincount(flat_e, length=EXPERTS).astype(jnp.int32)
    padded_counts = (counts + block_rows - 1) // block_rows * block_rows
    pad_end = jnp.cumsum(padded_counts).astype(jnp.int32)
    pad_start = pad_end - padded_counts
    seg_start = (jnp.cumsum(counts) - counts).astype(jnp.int32)
    dest = pad_start[sorted_e] + jnp.arange(slots, dtype=jnp.int32) - seg_start[sorted_e]
    block_count = (slots + block_rows - 1) // block_rows + EXPERTS
    total_rows = block_count * block_rows
    buffer_slot = jnp.full((total_rows,), slots, jnp.int32).at[dest].set(order)
    block_expert = jnp.minimum(jnp.searchsorted(pad_end, jnp.arange(block_count, dtype=jnp.int32) * block_rows, side='right'), EXPERTS - 1).astype(jnp.int32)
    rows_pad = jnp.concatenate([routed_in, jnp.zeros((1, D), jnp.bfloat16)], axis=0)

    def one_block(items):
        slot_ids, expert = items
        token_row = jnp.where(slot_ids < slots, slot_ids // TOPK, TOKENS)
        block_in = rows_pad[token_row]
        gate_act = jnp.dot(block_in, expert_gate[expert], preferred_element_type=jnp.float32)
        up_act = jnp.dot(block_in, expert_up[expert], preferred_element_type=jnp.float32)
        hidden = (jax.nn.silu(gate_act) * up_act).astype(jnp.bfloat16)
        return jnp.dot(hidden, expert_down[expert], preferred_element_type=jnp.float32).astype(jnp.bfloat16)
    results = lax.map(one_block, (buffer_slot.reshape(block_count, block_rows), block_expert)).reshape(total_rows, D)
    slot_out = jnp.zeros((slots + 1, D), jnp.bfloat16).at[buffer_slot].set(results)[:slots]
    weights = group_prob[:, None] * route_prob / lax.optimization_barrier(jnp.sum(route_prob, axis=1, keepdims=True))
    expert_sum = lax.optimization_barrier(jnp.sum(slot_out.reshape(TOKENS, TOPK, D).astype(jnp.float32) * weights[:, :, None], axis=1))
    return (residual.astype(jnp.float32) + expert_sum).astype(jnp.bfloat16)
```

```python
import jax
import jax.numpy as jnp
from jax import lax
from jax.experimental import pallas as pl
from jax.experimental.pallas import tpu as pltpu
from jax.sharding import PartitionSpec as P

EPSILON = 1e-06
NZ = 8
CAP = 16
NC = 4
MESH = pl.DeviceIdType.MESH
BF = jnp.bfloat16
F32 = jnp.float32


def moe_kernel(
    rows_ref,
    res_ref,
    meta_ref,
    wg_hbm,
    wu_hbm,
    wd_hbm,
    out_ref,
    metas,
    hop1,
    hop2,
    sel3,
    pack3,
    hop3,
    hop4,
    packed,
    arrived,
    results,
    ret0,
    ret1,
    big2,
    ret3,
    ret4,
    back4,
    send2,
    part2,
    send1,
    part1,
    hid,
    wg,
    wu,
    wd,
    wsem,
    msend,
    mrecv,
    zsend,
    zrecv,
    xsend,
    xrecv,
    ysend,
    yrecv,
    rsend,
    rrecv,
):
    tok, width = rows_ref.shape
    nj = lax.axis_size("sp") // NZ
    grp = nj * CAP
    half = grp // 2
    cw = width // NC
    sp = lax.axis_index("sp")
    tp = lax.axis_index("tp")
    z = sp // nj
    me_j = sp % nj
    step = (1, -1)
    near = (1, NZ - 1)
    far = (2, NZ - 2)
    both = [(n, d) for n in range(NC) for d in (0, 1)]

    def zval(offset):
        return lax.rem(z + offset + NZ, NZ)

    def zid(offset):
        return (zval(offset) * nj + me_j, tp)

    def jid(offset):
        return (z * nj + lax.rem(me_j + offset, nj), tp)

    def cols_of(n):
        return slice(n * cw, (n + 1) * cw)

    def slot_rows(b, j):
        return pl.ds(pl.multiple_of(b * grp + j * CAP, CAP), CAP)

    sent = []

    def remote(src, dst, send, recv, device):
        return pltpu.make_async_remote_copy(
            src_ref=src, dst_ref=dst, send_sem=send, recv_sem=recv, device_id=device, device_id_type=MESH
        )

    def start(copy):
        copy.start()
        sent.append(copy)

    wcopies = [
        pltpu.make_async_copy(wg_hbm.at[0], wg, wsem.at[0]),
        pltpu.make_async_copy(wu_hbm.at[0], wu, wsem.at[1]),
        pltpu.make_async_copy(wd_hbm.at[0], wd, wsem.at[2]),
    ]
    for copy in wcopies:
        copy.start()

    barrier = pltpu.get_barrier_semaphore()
    for offset in range(1, NZ):
        pl.semaphore_signal(barrier, inc=1, device_id=zid(offset), device_id_type=MESH)
    for offset in range(1, nj):
        pl.semaphore_signal(barrier, inc=1, device_id=jid(offset), device_id_type=MESH)
    pl.semaphore_wait(barrier, NZ + nj - 2)

    def mcopy(offset):
        return remote(meta_ref, metas.at[offset], msend.at[offset], mrecv.at[offset], zid(offset))

    for offset in range(1, NZ):
        start(mcopy(offset))

    def zcopy(hop, d, n):
        cols = cols_of(n)
        if hop == 0:
            src, dst = rows_ref.at[:, cols], hop1.at[d, :, cols]
        elif hop == 1:
            src, dst = hop1.at[d, :, cols], hop2.at[d, :, cols]
        elif hop == 2:
            src, dst = pack3.at[d, :, cols], hop3.at[d, :, cols]
        else:
            src, dst = hop3.at[d, grp : grp + half, cols], hop4.at[d * half : (d + 1) * half, cols]
        return remote(src, dst, zsend.at[hop, d, n], zrecv.at[hop, d, n], zid(step[d]))

    for n, d in both:
        start(zcopy(0, d, n))

    def meta_of(offset):
        return meta_ref if offset == 0 else metas.at[offset]

    def slots_of(rows, target, first):
        return (lax.broadcasted_iota(jnp.int32, (rows, tok), 0) + (first + target * grp)).astype(F32)

    def select(offset, target, rows, first=0):
        ref = meta_of(offset)
        slot = slots_of(rows, target, first)
        hit = jnp.where(slot == ref[0:1, :], 1.0, 0.0) + jnp.where(slot == ref[1:2, :], 1.0, 0.0)
        return hit.astype(BF)

    def spread(offset, target, rows, first=0):
        ref = meta_of(offset)
        slot = slots_of(rows, target, first)
        hit = jnp.where(slot == ref[0:1, :], ref[2:3, :], 0.0) + jnp.where(slot == ref[1:2, :], ref[3:4, :], 0.0)
        return hit.astype(BF)

    def combine(weights, rows):
        return lax.dot_general(weights, rows, (((0,), (0,)), ((), ())), preferred_element_type=F32)

    def xsource(b):
        if b < 5:
            return packed.at[b]
        if b < 7:
            return hop3.at[b - 5]
        return hop4

    def ytarget(b):
        if b == 0:
            return ret0
        if b < 3:
            return ret1.at[b - 1]
        if b < 5:
            return big2.at[b - 3]
        if b < 7:
            return ret3.at[b - 5]
        return ret4

    def xstart(b):
        src = xsource(b)
        for offset in range(1, nj):
            their = slot_rows(0, lax.rem(me_j + offset, nj))
            start(remote(src.at[their, :], arrived.at[slot_rows(b, me_j), :], xsend.at[b, offset], xrecv.at[b, offset], jid(offset)))
        arrived[slot_rows(b, me_j), :] = src[slot_rows(0, me_j), :]

    def xwait(b):
        for offset in range(1, nj):
            mine = slot_rows(b, me_j)
            remote(arrived.at[mine, :], arrived.at[mine, :], xsend.at[b, offset], xrecv.at[b, offset], jid(offset)).wait_recv()

    def ystart(b):
        dst = ytarget(b)
        for offset in range(1, nj):
            their = slot_rows(b, lax.rem(me_j + offset, nj))
            start(remote(results.at[their, :], dst.at[slot_rows(0, me_j), :], ysend.at[b, offset], yrecv.at[b, offset], jid(offset)))
        dst[slot_rows(0, me_j), :] = results[slot_rows(b, me_j), :]

    def ywait(b):
        dst = ytarget(b)
        for offset in range(1, nj):
            mine = slot_rows(0, me_j)
            remote(dst.at[mine, :], dst.at[mine, :], ysend.at[b, offset], yrecv.at[b, offset], jid(offset)).wait_recv()

    def pack(b, offset, block):
        chosen = select(offset, z, grp)
        for n in range(NC):
            cols = cols_of(n)
            packed[b, :, cols] = jnp.dot(chosen, block[:, cols], preferred_element_type=F32).astype(BF)

    fe = wg.shape[1]
    fw = fe // 2

    def experts(first, count):
        rows = count * grp
        base = first * grp

        def up(f, carry):
            cols = pl.ds(pl.multiple_of(f * fw, fw), fw)
            act = arrived[base : base + rows, :]
            g = jnp.dot(act, wg[:, cols], preferred_element_type=F32)
            u = jnp.dot(act, wu[:, cols], preferred_element_type=F32)
            hid[0:rows, cols] = (g * jax.nn.sigmoid(g) * u).astype(BF)
            return carry

        lax.fori_loop(0, 2, up, 0)

        def down(n, carry):
            cols = pl.ds(pl.multiple_of(n * cw, cw), cw)
            r = jnp.dot(hid[0:rows, :], wd[:, cols], preferred_element_type=F32)
            results[base : base + rows, cols] = r.astype(BF)
            return carry

        lax.fori_loop(0, NC, down, 0)

    pack(0, 0, rows_ref)
    xstart(0)
    for n, d in both:
        zcopy(0, d, n).wait_recv()
        start(zcopy(1, d, n))
    for offset in range(1, NZ):
        mcopy(offset).wait_recv()
    for d in (0, 1):
        pack(1 + d, near[d], hop1.at[d])
        xstart(1 + d)
    for copy in wcopies:
        copy.wait()
    xwait(0)
    experts(0, 1)
    ystart(0)
    for d in (0, 1):
        sel3[d, 0:grp, :] = select(far[d], zval(step[d]), grp)
        sel3[d, grp : grp + half, :] = select(far[d], zval(2 * step[d]), half, d * half)
    for n, d in both:
        zcopy(1, d, n).wait_recv()
        cols = cols_of(n)
        pack3[d, :, cols] = jnp.dot(sel3[d], hop2[d, :, cols], preferred_element_type=F32).astype(BF)
        start(zcopy(2, d, n))
    for d in (0, 1):
        pack(3 + d, far[d], hop2.at[d])
        xstart(3 + d)
    xwait(1)
    xwait(2)
    experts(1, 2)
    ystart(1)
    ystart(2)
    for n, d in both:
        zcopy(2, d, n).wait_recv()
        start(zcopy(3, d, n))
    xstart(5)
    xstart(6)
    xwait(3)
    xwait(4)
    experts(3, 2)
    ystart(3)
    ystart(4)
    for n, d in both:
        zcopy(3, d, n).wait_recv()
    xstart(7)
    xwait(5)
    xwait(6)
    experts(5, 2)
    ystart(5)
    ystart(6)
    xwait(7)
    experts(7, 1)
    ystart(7)

    def rcopy(kind, d, n):
        cols = cols_of(n)
        if kind == 0:
            src, dst = ret4.at[d * half : (d + 1) * half, cols], back4.at[d, :, cols]
        elif kind == 1:
            src, dst = ret3.at[d, :, cols], big2.at[d, grp : 2 * grp, cols]
        elif kind == 2:
            src, dst = back4.at[d, :, cols], big2.at[d, 2 * grp : 2 * grp + half, cols]
        elif kind == 3:
            src, dst = send2.at[d, :, cols], part2.at[d, :, cols]
        else:
            src, dst = send1.at[d, :, cols], part1.at[d, :, cols]
        return remote(src, dst, rsend.at[kind, d, n], rrecv.at[kind, d, n], zid(-step[d]))

    ywait(5)
    ywait(6)
    for n, d in both:
        start(rcopy(1, d, n))
    ywait(7)
    for n, d in both:
        start(rcopy(0, d, n))
    for b in range(5):
        ywait(b)
    for n, d in both:
        rcopy(0, d, n).wait_recv()
        start(rcopy(2, d, n))
    for n, d in both:
        rcopy(1, d, n).wait_recv()
        rcopy(2, d, n).wait_recv()
        cols = cols_of(n)
        total = combine(spread(far[d], z, grp), big2[d, 0:grp, cols])
        total = total + combine(spread(far[d], zval(step[d]), grp), big2[d, grp : 2 * grp, cols])
        total = total + combine(spread(far[d], zval(2 * step[d]), half, d * half), big2[d, 2 * grp : 2 * grp + half, cols])
        send2[d, :, cols] = total.astype(BF)
        start(rcopy(3, d, n))
    for n, d in both:
        rcopy(3, d, n).wait_recv()
        cols = cols_of(n)
        total = part2[d, :, cols].astype(F32) + combine(spread(near[d], z, grp), ret1[d, :, cols])
        send1[d, :, cols] = total.astype(BF)
        start(rcopy(4, d, n))
    own = spread(0, z, grp)
    for n in range(NC):
        rcopy(4, 0, n).wait_recv()
        rcopy(4, 1, n).wait_recv()
        cols = cols_of(n)
        total = res_ref[:, cols].astype(F32) + combine(own, ret0[:, cols])
        total = total + part1[0, :, cols].astype(F32) + part1[1, :, cols].astype(F32)
        out_ref[:, cols] = total.astype(BF)
    for copy in sent:
        copy.wait_send()


def moe(rows, res, meta, wg, wu, wd):
    tok, width = rows.shape
    fe = wg.shape[2]
    nj = lax.axis_size("sp") // NZ
    grp = nj * CAP
    half = grp // 2
    vmem = pl.BlockSpec(memory_space=pltpu.VMEM)
    hbm = pl.BlockSpec(memory_space=pl.ANY)
    dma = pltpu.SemaphoreType.DMA
    shapes = [
        ((NZ,) + meta.shape, F32),
        ((2, tok, width), BF),
        ((2, tok, width), BF),
        ((2, grp + half, tok), BF),
        ((2, grp + half, width), BF),
        ((2, grp + half, width), BF),
        ((grp, width), BF),
        ((5, grp, width), BF),
        ((8 * grp, width), BF),
        ((8 * grp, width), BF),
        ((grp, width), BF),
        ((2, grp, width), BF),
        ((2, 2 * grp + half, width), BF),
        ((2, grp, width), BF),
        ((grp, width), BF),
        ((2, half, width), BF),
        ((2, tok, width), BF),
        ((2, tok, width), BF),
        ((2, tok, width), BF),
        ((2, tok, width), BF),
        ((2 * grp, fe), BF),
        (wg.shape[1:], BF),
        (wu.shape[1:], BF),
        (wd.shape[1:], BF),
    ]
    sems = [(3,), (NZ,), (NZ,), (4, 2, NC), (4, 2, NC), (8, nj), (8, nj), (8, nj), (8, nj), (5, 2, NC), (5, 2, NC)]
    return pl.pallas_call(
        moe_kernel,
        out_shape=jax.ShapeDtypeStruct((tok, width), BF),
        in_specs=[vmem, vmem, vmem, hbm, hbm, hbm],
        out_specs=vmem,
        scratch_shapes=[pltpu.VMEM(s, t) for s, t in shapes] + [dma(s) for s in sems],
        compiler_params=pltpu.CompilerParams(
            collective_id=0, has_side_effects=True, vmem_limit_bytes=60 * 1024 * 1024
        ),
        name="moe",
    )(rows, res, meta, wg, wu, wd)


def from_behind(shard, axis, by):
    devices = lax.axis_size(axis)
    pairs = [(i, i + by) for i in range(devices) if 0 <= i + by < devices]
    return lax.ppermute(shard, axis, pairs)


def rms_norm(values, gain):
    floats = values.astype(F32)
    factor = lax.rsqrt(jnp.mean(floats * floats, axis=-1, keepdims=True) + EPSILON)
    return floats * factor * gain.astype(F32)


def slot_meta(expert_ids, group_prob, route_prob, experts_all):
    tok = expert_ids.shape[0]
    lane = jnp.arange(experts_all, dtype=jnp.int32)[None, :]
    hot0 = (expert_ids[:, 0:1] == lane).astype(BF)
    hot1 = (expert_ids[:, 1:2] == lane).astype(BF)
    row = jnp.arange(tok, dtype=jnp.int32)
    before = (row[:, None] > row[None, :]).astype(BF)
    ranks = jnp.dot(before, jnp.concatenate([hot0, hot1], axis=1), preferred_element_type=F32)
    count0 = jnp.sum(hot0.astype(F32), axis=0, keepdims=True)
    rank0 = jnp.sum(ranks[:, :experts_all] * hot0, axis=1)
    rank1 = jnp.sum((ranks[:, experts_all:] + count0) * hot1, axis=1)
    pos0 = expert_ids[:, 0].astype(F32) * CAP + rank0
    pos1 = expert_ids[:, 1].astype(F32) * CAP + rank1
    weights = group_prob[:, None] * route_prob / jnp.sum(route_prob, axis=1, keepdims=True)
    zero = jnp.zeros_like(pos0)
    return jnp.stack([pos0, pos1, weights[:, 0], weights[:, 1], zero, zero, zero, zero], axis=0)


def body(
    residual_in,
    gate_outer,
    gate_inner,
    conv_input,
    conv_taps,
    norm_gain,
    out_weight,
    moe_gain,
    expert_ids,
    group_prob,
    route_prob,
    expert_gate,
    expert_up,
    expert_down,
):
    seq_rows, channels = conv_input.shape
    taps_count = conv_taps.shape[0]
    inner = gate_inner.astype(F32) * conv_input.astype(F32)
    earlier = from_behind(inner[seq_rows - (taps_count - 1) :], "sp", 1)
    padded = jnp.concatenate([earlier, inner], axis=0)
    tap_f = conv_taps.astype(F32)
    filtered = jnp.zeros((seq_rows, channels), F32)
    for offset in range(taps_count):
        filtered = filtered + tap_f[offset][None, :] * padded[offset : offset + seq_rows]
    mixed_out = (gate_outer.astype(F32) * filtered).astype(BF)
    gathered = lax.all_to_all(mixed_out, "tp", split_axis=0, concat_axis=1, tiled=True)
    full_weight, full_gain = (
        lax.all_gather(out_weight, "tp", axis=0, tiled=True),
        lax.all_gather(norm_gain, "tp", axis=0, tiled=True),
    )
    normed = rms_norm(gathered, full_gain).astype(BF)
    projected = jnp.dot(normed, full_weight, preferred_element_type=F32)
    residual = (residual_in.astype(F32) + projected).astype(BF)
    routed_in = rms_norm(residual, moe_gain).astype(BF)
    experts_all = expert_gate.shape[0] * lax.axis_size("sp")
    meta = slot_meta(expert_ids, group_prob, route_prob, experts_all)
    return moe(routed_in, residual, meta, expert_gate, expert_up, expert_down)


def solution(mesh):
    in_specs = (
        P(("sp", "tp"), None),
        P("sp", "tp"),
        P("sp", "tp"),
        P("sp", "tp"),
        P(None, "tp"),
        P("tp"),
        P("tp", None),
        P(),
        P(("sp", "tp"), None),
        P(("sp", "tp")),
        P(("sp", "tp"), None),
        P("sp", None, None),
        P("sp", None, None),
        P("sp", None, None),
    )
    out_specs = P(("sp", "tp"), None)
    return jax.shard_map(body, mesh=mesh, in_specs=in_specs, out_specs=out_specs, check_vma=False)
```

```python
import jax
import jax.numpy as jnp
from jax import lax
from jax.experimental import pallas as pl
from jax.experimental.pallas import tpu as pltpu
from jax.sharding import PartitionSpec as P

EPSILON = 1e-06
NZ = 8
CAP = 16
NC = 4
MESH = pl.DeviceIdType.MESH
BF = jnp.bfloat16
F32 = jnp.float32


def moe_kernel(
    rows_ref,
    res_ref,
    meta_ref,
    wg_hbm,
    wu_hbm,
    wd_hbm,
    out_ref,
    metas,
    hop1,
    hop2,
    sel3,
    sel4,
    pack3,
    pack4,
    gather3,
    gather4,
    pass4,
    packed,
    arrived,
    results,
    ret0,
    ret1,
    ret2,
    got3,
    back4,
    got4,
    ret3,
    ret4,
    send2,
    part2,
    send1,
    part1,
    hid,
    wg,
    wu,
    wd,
    wsem,
    msend,
    mrecv,
    zsend,
    zrecv,
    xsend,
    xrecv,
    ysend,
    yrecv,
    gsend,
    grecv,
    bsend,
    brecv,
    rsend,
    rrecv,
):
    tok, width = rows_ref.shape
    nj = lax.axis_size("sp") // NZ
    grp = nj * CAP
    others = grp - CAP
    cw = width // NC
    hw = cw // 2
    sp = lax.axis_index("sp")
    tp = lax.axis_index("tp")
    z = sp // nj
    me_j = sp % nj
    step = (1, -1)
    near = (1, NZ - 1)
    far = (2, NZ - 2)
    both = [(n, d) for n in range(NC) for d in (0, 1)]

    def zval(offset):
        return lax.rem(z + offset + NZ, NZ)

    def zid(offset):
        return (zval(offset) * nj + me_j, tp)

    def jid(offset):
        return (z * nj + lax.rem(me_j + offset, nj), tp)

    def cols_of(n):
        return slice(n * cw, (n + 1) * cw)

    def half_of(n):
        return slice(n * hw, (n + 1) * hw)

    def part_of(n, d):
        return slice(n * cw + d * hw, n * cw + (d + 1) * hw)

    def slot_rows(b, j):
        return pl.ds(pl.multiple_of(b * grp + j * CAP, CAP), CAP)

    def block_rows(b):
        return slice(b * grp, (b + 1) * grp)

    sent = []

    def remote(src, dst, send, recv, device):
        return pltpu.make_async_remote_copy(
            src_ref=src, dst_ref=dst, send_sem=send, recv_sem=recv, device_id=device, device_id_type=MESH
        )

    def start(copy):
        copy.start()
        sent.append(copy)

    def wait_bytes(ref, sem):
        pltpu.make_async_copy(ref, ref, sem).wait()

    wcopies = [
        pltpu.make_async_copy(wg_hbm.at[0], wg, wsem.at[0]),
        pltpu.make_async_copy(wu_hbm.at[0], wu, wsem.at[1]),
        pltpu.make_async_copy(wd_hbm.at[0], wd, wsem.at[2]),
    ]
    for copy in wcopies:
        copy.start()

    barrier = pltpu.get_barrier_semaphore()
    for offset in range(1, NZ):
        pl.semaphore_signal(barrier, inc=1, device_id=zid(offset), device_id_type=MESH)
    for offset in range(1, nj):
        pl.semaphore_signal(barrier, inc=1, device_id=jid(offset), device_id_type=MESH)
    pl.semaphore_wait(barrier, NZ + nj - 2)

    def mcopy(offset):
        return remote(meta_ref, metas.at[offset], msend.at[offset], mrecv.at[offset], zid(offset))

    for offset in range(1, NZ):
        start(mcopy(offset))

    def zcopy(hop, d, n):
        cols = cols_of(n)
        if hop == 0:
            src, dst = rows_ref.at[:, cols], hop1.at[d, :, cols]
        elif hop == 1:
            src, dst = hop1.at[d, :, cols], hop2.at[d, :, cols]
        elif hop == 2:
            src, dst = gather3.at[d, :, cols], arrived.at[block_rows(5 + d), cols]
        elif hop == 3:
            src, dst = gather4.at[d, :, half_of(n)], pass4.at[d, :, half_of(n)]
        else:
            src, dst = pass4.at[d, :, half_of(n)], arrived.at[block_rows(7), part_of(n, d)]
        return remote(src, dst, zsend.at[hop, d, n], zrecv.at[hop, d, n], zid(step[d]))

    for n, d in both:
        start(zcopy(0, d, n))

    def meta_of(offset):
        return meta_ref if offset == 0 else metas.at[offset]

    def slots_of(target):
        return (lax.broadcasted_iota(jnp.int32, (grp, tok), 0) + target * grp).astype(F32)

    def select(offset, target):
        ref = meta_of(offset)
        slot = slots_of(target)
        hit = jnp.where(slot == ref[0:1, :], 1.0, 0.0) + jnp.where(slot == ref[1:2, :], 1.0, 0.0)
        return hit.astype(BF)

    def spread(offset, target):
        ref = meta_of(offset)
        slot = slots_of(target)
        hit = jnp.where(slot == ref[0:1, :], ref[2:3, :], 0.0) + jnp.where(slot == ref[1:2, :], ref[3:4, :], 0.0)
        return hit.astype(BF)

    def combine(weights, rows):
        return lax.dot_general(weights, rows, (((0,), (0,)), ((), ())), preferred_element_type=F32)

    def ytarget(b):
        return ret0 if b == 0 else ret1.at[b - 1] if b < 3 else ret2.at[b - 3]

    def xstart(b):
        for offset in range(1, nj):
            their = slot_rows(0, lax.rem(me_j + offset, nj))
            start_only(remote(packed.at[b, their, :], arrived.at[slot_rows(b, me_j), :], xsend.at[b], xrecv.at[b], jid(offset)))
        arrived[slot_rows(b, me_j), :] = packed[b, slot_rows(0, me_j), :]
        pending.append((packed.at[b, 0:others, :], xsend.at[b]))

    pending = []

    def start_only(copy):
        copy.start()

    def xwait(b):
        wait_bytes(arrived.at[b * grp : b * grp + others, :], xrecv.at[b])

    def ystart(b):
        dst = ytarget(b)
        for offset in range(1, nj):
            their = slot_rows(b, lax.rem(me_j + offset, nj))
            start_only(remote(results.at[their, :], dst.at[slot_rows(0, me_j), :], ysend.at[b], yrecv.at[b], jid(offset)))
        dst[slot_rows(0, me_j), :] = results[slot_rows(b, me_j), :]
        pending.append((dst.at[0:others, :], ysend.at[b]))

    def ywait(b):
        wait_bytes(ytarget(b).at[0:others, :], yrecv.at[b])

    def exchange(src, dst, d, cols, ssem, rsem):
        mine = slot_rows(0, me_j)
        for offset in range(1, nj):
            their = slot_rows(0, lax.rem(me_j + offset, nj))
            start_only(remote(src.at[d, their, cols], dst.at[d, mine, cols], ssem, rsem, jid(offset)))
        dst[d, mine, cols] = src[d, mine, cols]
        pending.append((src.at[d, 0:others, cols], ssem))

    def pack(b, offset, block):
        chosen = select(offset, z)
        for n in range(NC):
            cols = cols_of(n)
            packed[b, :, cols] = jnp.dot(chosen, block[:, cols], preferred_element_type=F32).astype(BF)

    fe = wg.shape[1]
    fw = fe // 2

    def experts(first, count):
        rows = count * grp
        base = first * grp

        def up(f, carry):
            cols = pl.ds(pl.multiple_of(f * fw, fw), fw)
            act = arrived[base : base + rows, :]
            g = jnp.dot(act, wg[:, cols], preferred_element_type=F32)
            u = jnp.dot(act, wu[:, cols], preferred_element_type=F32)
            hid[0:rows, cols] = (g * jax.nn.sigmoid(g) * u).astype(BF)
            return carry

        lax.fori_loop(0, 2, up, 0)

        def down(n, carry):
            cols = pl.ds(pl.multiple_of(n * cw, cw), cw)
            r = jnp.dot(hid[0:rows, :], wd[:, cols], preferred_element_type=F32)
            results[base : base + rows, cols] = r.astype(BF)
            return carry

        lax.fori_loop(0, NC, down, 0)

    with jax.named_scope("own"):
        pack(0, 0, rows_ref)
        xstart(0)
    for n, d in both:
        with jax.named_scope(f"hop1_{n}{d}"):
            zcopy(0, d, n).wait_recv()
        start(zcopy(1, d, n))
    with jax.named_scope("metas"):
        for offset in range(1, NZ):
            mcopy(offset).wait_recv()
    with jax.named_scope("pack1"):
        for d in (0, 1):
            pack(1 + d, near[d], hop1.at[d])
            xstart(1 + d)
    for copy in wcopies:
        copy.wait()
    for d in (0, 1):
        sel3[d] = select(far[d], zval(step[d]))
        sel4[d] = select(far[d], zval(2 * step[d]))
    xwait(0)
    with jax.named_scope("exp0"):
        experts(0, 1)

    def hop3_out(n):
        for d in (0, 1):
            with jax.named_scope(f"ex{n}{d}"):
                wait_bytes(gather3.at[d, 0:others, cols_of(n)], grecv.at[0, d, n])
                wait_bytes(gather4.at[d, 0:others, half_of(n)], grecv.at[1, d, n])
            start(zcopy(3, d, n))
            start(zcopy(2, d, n))

    for n in range(NC):
        for d in (0, 1):
            with jax.named_scope(f"hop2_{n}{d}"):
                zcopy(1, d, n).wait_recv()
            part = hop2[d, :, cols_of(n)]
            pack3[d, :, cols_of(n)] = jnp.dot(sel3[d], part, preferred_element_type=F32).astype(BF)
            part = hop2[d, :, part_of(n, d)]
            pack4[d, :, half_of(n)] = jnp.dot(sel4[d], part, preferred_element_type=F32).astype(BF)
            exchange(pack4, gather4, d, half_of(n), gsend.at[1, d, n], grecv.at[1, d, n])
            exchange(pack3, gather3, d, cols_of(n), gsend.at[0, d, n], grecv.at[0, d, n])
        if n > 0:
            hop3_out(n - 1)
    with jax.named_scope("pack2"):
        for d in (0, 1):
            pack(3 + d, far[d], hop2.at[d])
            xstart(3 + d)
    hop3_out(NC - 1)
    xwait(1)
    xwait(2)
    with jax.named_scope("exp12"):
        experts(1, 2)

    def rcopy(kind, d, n):
        cols = cols_of(n)
        if kind == 0:
            src, dst = results.at[block_rows(7), part_of(n, d)], back4.at[d, :, half_of(n)]
        elif kind == 1:
            src, dst = results.at[block_rows(5 + d), cols], got3.at[d, :, cols]
        elif kind == 2:
            src, dst = back4.at[d, :, half_of(n)], got4.at[d, :, half_of(n)]
        elif kind == 3:
            src, dst = send2.at[d, :, cols], part2.at[d, :, cols]
        else:
            src, dst = send1.at[d, :, cols], part1.at[d, :, cols]
        return remote(src, dst, rsend.at[kind, d, n], rrecv.at[kind, d, n], zid(-step[d]))

    for n, d in both:
        with jax.named_scope(f"hop3_{n}{d}"):
            zcopy(3, d, n).wait_recv()
        start(zcopy(4, d, n))
    xwait(3)
    xwait(4)
    with jax.named_scope("exp34"):
        experts(3, 2)
    ystart(3)
    ystart(4)
    with jax.named_scope("hop3w"):
        for n, d in both:
            zcopy(2, d, n).wait_recv()
    with jax.named_scope("exp56"):
        experts(5, 2)
    for n, d in both:
        start(rcopy(1, d, n))
    with jax.named_scope("hop4w"):
        for n, d in both:
            zcopy(4, d, n).wait_recv()
    with jax.named_scope("exp7"):
        experts(7, 1)
    for n, d in both:
        start(rcopy(0, d, n))
    for n, d in both:
        with jax.named_scope(f"r3_{n}{d}"):
            rcopy(1, d, n).wait_recv()
        exchange(got3, ret3, d, cols_of(n), bsend.at[0, d, n], brecv.at[0, d, n])
    for n, d in both:
        with jax.named_scope(f"r4_{n}{d}"):
            rcopy(0, d, n).wait_recv()
        start(rcopy(2, d, n))
    ywait(3)
    ywait(4)

    def sums2_out(n):
        for d in (0, 1):
            with jax.named_scope(f"ex{n}{d}"):
                wait_bytes(ret3.at[d, 0:others, cols_of(n)], brecv.at[0, d, n])
                wait_bytes(ret4.at[d, 0:others, half_of(n)], brecv.at[1, d, n])
            total = combine(spread(far[d], z), ret2[d, :, cols_of(n)])
            total = total + combine(spread(far[d], zval(step[d])), ret3[d, :, cols_of(n)])
            last = combine(spread(far[d], zval(2 * step[d])), ret4[d, :, half_of(n)])
            lo, hi = total[:, :hw], total[:, hw:]
            if d == 0:
                lo = lo + last
            else:
                hi = hi + last
            send2[d, :, part_of(n, 0)] = lo.astype(BF)
            send2[d, :, part_of(n, 1)] = hi.astype(BF)
            start(rcopy(3, d, n))

    for n in range(NC):
        for d in (0, 1):
            with jax.named_scope(f"r3b_{n}{d}"):
                rcopy(2, d, n).wait_recv()
            exchange(got4, ret4, d, half_of(n), bsend.at[1, d, n], brecv.at[1, d, n])
        if n > 0:
            sums2_out(n - 1)
    sums2_out(NC - 1)
    ystart(1)
    ystart(2)
    ystart(0)
    ywait(1)
    ywait(2)
    for n, d in both:
        with jax.named_scope(f"r2_{n}{d}"):
            rcopy(3, d, n).wait_recv()
        cols = cols_of(n)
        total = part2[d, :, cols].astype(F32) + combine(spread(near[d], z), ret1[d, :, cols])
        send1[d, :, cols] = total.astype(BF)
        start(rcopy(4, d, n))
    ywait(0)
    own = spread(0, z)
    for n in range(NC):
        with jax.named_scope(f"r1_{n}"):
            rcopy(4, 0, n).wait_recv()
            rcopy(4, 1, n).wait_recv()
        cols = cols_of(n)
        total = res_ref[:, cols].astype(F32) + combine(own, ret0[:, cols])
        total = total + part1[0, :, cols].astype(F32) + part1[1, :, cols].astype(F32)
        out_ref[:, cols] = total.astype(BF)
    for copy in sent:
        copy.wait_send()
    for ref, sem in pending:
        wait_bytes(ref, sem)


def moe(rows, res, meta, wg, wu, wd):
    tok, width = rows.shape
    fe = wg.shape[2]
    nj = lax.axis_size("sp") // NZ
    grp = nj * CAP
    vmem = pl.BlockSpec(memory_space=pltpu.VMEM)
    hbm = pl.BlockSpec(memory_space=pl.ANY)
    dma = pltpu.SemaphoreType.DMA
    shapes = [
        ((NZ,) + meta.shape, F32),
        ((2, tok, width), BF),
        ((2, tok, width), BF),
        ((2, grp, tok), BF),
        ((2, grp, tok), BF),
        ((2, grp, width), BF),
        ((2, grp, width // 2), BF),
        ((2, grp, width), BF),
        ((2, grp, width // 2), BF),
        ((2, grp, width // 2), BF),
        ((5, grp, width), BF),
        ((8 * grp, width), BF),
        ((8 * grp, width), BF),
        ((grp, width), BF),
        ((2, grp, width), BF),
        ((2, grp, width), BF),
        ((2, grp, width), BF),
        ((2, grp, width // 2), BF),
        ((2, grp, width // 2), BF),
        ((2, grp, width), BF),
        ((2, grp, width // 2), BF),
        ((2, tok, width), BF),
        ((2, tok, width), BF),
        ((2, tok, width), BF),
        ((2, tok, width), BF),
        ((2 * grp, fe), BF),
        (wg.shape[1:], BF),
        (wu.shape[1:], BF),
        (wd.shape[1:], BF),
    ]
    sems = [(3,), (NZ,), (NZ,), (5, 2, NC), (5, 2, NC), (5,), (5,), (5,), (5,)]
    sems += [(2, 2, NC), (2, 2, NC), (2, 2, NC), (2, 2, NC), (5, 2, NC), (5, 2, NC)]
    return pl.pallas_call(
        moe_kernel,
        out_shape=jax.ShapeDtypeStruct((tok, width), BF),
        in_specs=[vmem, vmem, vmem, hbm, hbm, hbm],
        out_specs=vmem,
        scratch_shapes=[pltpu.VMEM(s, t) for s, t in shapes] + [dma(s) for s in sems],
        compiler_params=pltpu.CompilerParams(
            collective_id=0, has_side_effects=True, vmem_limit_bytes=60 * 1024 * 1024
        ),
        name="moe",
    )(rows, res, meta, wg, wu, wd)


def from_behind(shard, axis, by):
    devices = lax.axis_size(axis)
    pairs = [(i, i + by) for i in range(devices) if 0 <= i + by < devices]
    return lax.ppermute(shard, axis, pairs)


def rms_norm(values, gain):
    floats = values.astype(F32)
    factor = lax.rsqrt(jnp.mean(floats * floats, axis=-1, keepdims=True) + EPSILON)
    return floats * factor * gain.astype(F32)


def slot_meta(expert_ids, group_prob, route_prob, experts_all):
    tok = expert_ids.shape[0]
    lane = jnp.arange(experts_all, dtype=jnp.int32)[None, :]
    hot0 = (expert_ids[:, 0:1] == lane).astype(BF)
    hot1 = (expert_ids[:, 1:2] == lane).astype(BF)
    row = jnp.arange(tok, dtype=jnp.int32)
    before = (row[:, None] > row[None, :]).astype(BF)
    ranks = jnp.dot(before, jnp.concatenate([hot0, hot1], axis=1), preferred_element_type=F32)
    count0 = jnp.sum(hot0.astype(F32), axis=0, keepdims=True)
    rank0 = jnp.sum(ranks[:, :experts_all] * hot0, axis=1)
    rank1 = jnp.sum((ranks[:, experts_all:] + count0) * hot1, axis=1)
    pos0 = expert_ids[:, 0].astype(F32) * CAP + rank0
    pos1 = expert_ids[:, 1].astype(F32) * CAP + rank1
    weights = group_prob[:, None] * route_prob / jnp.sum(route_prob, axis=1, keepdims=True)
    zero = jnp.zeros_like(pos0)
    return jnp.stack([pos0, pos1, weights[:, 0], weights[:, 1], zero, zero, zero, zero], axis=0)


def body(
    residual_in,
    gate_outer,
    gate_inner,
    conv_input,
    conv_taps,
    norm_gain,
    out_weight,
    moe_gain,
    expert_ids,
    group_prob,
    route_prob,
    expert_gate,
    expert_up,
    expert_down,
):
    seq_rows, channels = conv_input.shape
    taps_count = conv_taps.shape[0]
    inner = gate_inner.astype(F32) * conv_input.astype(F32)
    earlier = from_behind(inner[seq_rows - (taps_count - 1) :], "sp", 1)
    padded = jnp.concatenate([earlier, inner], axis=0)
    tap_f = conv_taps.astype(F32)
    filtered = jnp.zeros((seq_rows, channels), F32)
    for offset in range(taps_count):
        filtered = filtered + tap_f[offset][None, :] * padded[offset : offset + seq_rows]
    mixed_out = (gate_outer.astype(F32) * filtered).astype(BF)
    gathered = lax.all_to_all(mixed_out, "tp", split_axis=0, concat_axis=1, tiled=True)
    full_weight, full_gain = (
        lax.all_gather(out_weight, "tp", axis=0, tiled=True),
        lax.all_gather(norm_gain, "tp", axis=0, tiled=True),
    )
    normed = rms_norm(gathered, full_gain).astype(BF)
    projected = jnp.dot(normed, full_weight, preferred_element_type=F32)
    residual = (residual_in.astype(F32) + projected).astype(BF)
    routed_in = rms_norm(residual, moe_gain).astype(BF)
    experts_all = expert_gate.shape[0] * lax.axis_size("sp")
    meta = slot_meta(expert_ids, group_prob, route_prob, experts_all)
    return moe(routed_in, residual, meta, expert_gate, expert_up, expert_down)


def solution(mesh):
    in_specs = (
        P(("sp", "tp"), None),
        P("sp", "tp"),
        P("sp", "tp"),
        P("sp", "tp"),
        P(None, "tp"),
        P("tp"),
        P("tp", None),
        P(),
        P(("sp", "tp"), None),
        P(("sp", "tp")),
        P(("sp", "tp"), None),
        P("sp", None, None),
        P("sp", None, None),
        P("sp", None, None),
    )
    out_specs = P(("sp", "tp"), None)
    return jax.shard_map(body, mesh=mesh, in_specs=in_specs, out_specs=out_specs, check_vma=False)
```

```python
import jax
import jax.numpy as jnp
from jax import lax
from jax.experimental import pallas as pl
from jax.experimental.pallas import tpu as pltpu
from jax.sharding import PartitionSpec as P

EPSILON = 1e-06
NZ = 8
CAP = 16
NC = 4
MESH = pl.DeviceIdType.MESH
BF = jnp.bfloat16
F32 = jnp.float32


def layer_kernel(
    rin_hbm,
    go_hbm,
    gi_hbm,
    ci_hbm,
    ow_hbm,
    wg_hbm,
    wu_hbm,
    wd_hbm,
    taps_ref,
    gain_ref,
    mgain_ref,
    ids_ref,
    group_ref,
    route_ref,
    out_ref,
    rin,
    go,
    gi,
    ci,
    ow,
    halo,
    inner,
    mixed,
    mixrel,
    gainsrc,
    gainrel,
    normed,
    wrel,
    res_ref,
    meta_ref,
    act,
    metas,
    hop1,
    hop2,
    sel3,
    sel4,
    pack3,
    pack4,
    gather3,
    gather4,
    pass4,
    packed,
    arrived,
    results,
    ret0,
    ret1,
    ret2,
    got3,
    back4,
    got4,
    ret3,
    ret4,
    send2,
    part2,
    send1,
    part1,
    hid,
    wg,
    wu,
    wd,
    isem,
    wsem,
    hsend,
    hrecv,
    tsend,
    trecv,
    asend,
    arecv,
    msend,
    mrecv,
    zsend,
    zrecv,
    xsend,
    xrecv,
    ysend,
    yrecv,
    gsend,
    grecv,
    bsend,
    brecv,
    rsend,
    rrecv,
):
    tok, width = res_ref.shape
    nsp = lax.axis_size("sp")
    ntp = lax.axis_size("tp")
    nj = nsp // NZ
    grp = nj * CAP
    seq, chan = mixed.shape
    others = grp - CAP
    cw = width // NC
    hw = cw // 2
    sp = lax.axis_index("sp")
    tp = lax.axis_index("tp")
    z = sp // nj
    me_j = sp % nj
    step = (1, -1)
    near = (1, NZ - 1)
    far = (2, NZ - 2)
    both = [(n, d) for n in range(NC) for d in (0, 1)]

    def zval(offset):
        return lax.rem(z + offset + NZ, NZ)

    def zid(offset):
        return (zval(offset) * nj + me_j, tp)

    def jid(offset):
        return (z * nj + lax.rem(me_j + offset, nj), tp)

    def tid(offset):
        return (sp, lax.rem(tp + offset, ntp))

    after = (lax.rem(sp + 1, nsp), tp)
    before = (lax.rem(sp + nsp - 1, nsp), tp)
    core = lax.rem(me_j, 2)
    partner = (z * nj + me_j + 1 - 2 * core, tp)

    def cols_of(n):
        return slice(n * cw, (n + 1) * cw)

    def half_of(n):
        return slice(n * hw, (n + 1) * hw)

    def part_of(n, d):
        return slice(n * cw + d * hw, n * cw + (d + 1) * hw)

    def slot_rows(b, j):
        return pl.ds(pl.multiple_of(b * grp + j * CAP, CAP), CAP)

    def block_rows(b):
        return slice(b * grp, (b + 1) * grp)

    sent = []

    def remote(src, dst, send, recv, device):
        return pltpu.make_async_remote_copy(
            src_ref=src, dst_ref=dst, send_sem=send, recv_sem=recv, device_id=device, device_id_type=MESH
        )

    def start(copy):
        copy.start()
        sent.append(copy)

    def wait_bytes(ref, sem):
        pltpu.make_async_copy(ref, ref, sem).wait()

    icopies = [
        pltpu.make_async_copy(src, dst, isem.at[i])
        for i, (src, dst) in enumerate(((ow_hbm, ow), (gi_hbm, gi), (ci_hbm, ci), (go_hbm, go), (rin_hbm, rin)))
    ]
    for copy in icopies:
        copy.start()
    wcopies = [
        pltpu.make_async_copy(wg_hbm.at[0], wg, wsem.at[0]),
        pltpu.make_async_copy(wu_hbm.at[0], wu, wsem.at[1]),
        pltpu.make_async_copy(wd_hbm.at[0], wd, wsem.at[2]),
    ]
    barrier = pltpu.get_barrier_semaphore()
    for offset in range(1, NZ):
        pl.semaphore_signal(barrier, inc=1, device_id=zid(offset), device_id_type=MESH)
    for offset in range(1, nj):
        pl.semaphore_signal(barrier, inc=1, device_id=jid(offset), device_id_type=MESH)
    for offset in range(1, ntp):
        pl.semaphore_signal(barrier, inc=1, device_id=tid(offset), device_id_type=MESH)
    for ident in (after, before):
        pl.semaphore_signal(barrier, inc=1, device_id=ident, device_id_type=MESH)
    pl.semaphore_wait(barrier, NZ + nj + ntp - 1)

    def mcopy(offset):
        return remote(meta_ref, metas.at[offset], msend.at[offset], mrecv.at[offset], zid(offset))

    def zcopy(hop, d, n):
        cols = cols_of(n)
        if hop == 0:
            src, dst = res_ref.at[:, cols], hop1.at[d, :, cols]
        elif hop == 1:
            src, dst = hop1.at[d, :, cols], hop2.at[d, :, cols]
        elif hop == 2:
            src, dst = gather3.at[d, :, cols], arrived.at[block_rows(5 + d), cols]
        elif hop == 3:
            src, dst = gather4.at[d, :, half_of(n)], pass4.at[d, :, half_of(n)]
        else:
            src, dst = pass4.at[d, :, half_of(n)], arrived.at[block_rows(7), part_of(n, d)]
        return remote(src, dst, zsend.at[hop, d, n], zrecv.at[hop, d, n], zid(step[d]))

    def own_cols(n):
        return pl.ds(pl.multiple_of(n * cw + core * hw, hw), hw)

    def quarter_cols(n, d):
        return pl.ds(pl.multiple_of(n * cw + core * hw + d * (hw // 2), hw // 2), hw // 2)

    def acopy(kind, n):
        if kind == 0:
            src, dst, device = ow.at[:, own_cols(n)], wrel.at[3, :, own_cols(n)], tid(1)
        elif kind == 1:
            src, dst, device = ow.at[:, own_cols(n)], wrel.at[1, :, own_cols(n)], tid(ntp - 1)
        elif kind == 2:
            cols = quarter_cols(n, 0)
            src, dst, device = wrel.at[3, :, cols], wrel.at[2, :, cols], tid(1)
        elif kind == 3:
            cols = quarter_cols(n, 1)
            src, dst, device = wrel.at[1, :, cols], wrel.at[2, :, cols], tid(ntp - 1)
        else:
            cols = own_cols(n)
            block = (3, 1, 2)[kind - 4]
            src, dst, device = wrel.at[block, :, cols], wrel.at[block, :, cols], partner
        return remote(src, dst, asend.at[kind, n], arecv.at[kind, n], device)

    def tcopy(offset):
        rows = pl.ds(pl.multiple_of(lax.rem(tp + offset, ntp) * tok, tok), tok)
        return remote(mixed.at[rows, :], mixrel.at[ntp - offset], tsend.at[0, offset], trecv.at[0, offset], tid(offset))

    def gcopy(offset):
        return remote(gainsrc, gainrel.at[ntp - offset], tsend.at[1, offset], trecv.at[1, offset], tid(offset))

    def hcopy(i):
        src = (gi, ci)[i]
        return remote(src.at[seq - 16 : seq, :], halo.at[i], hsend.at[i], hrecv.at[i], after)

    icopies[0].wait()
    for kind in (0, 1):
        start(acopy(kind, 0))
    gainsrc[...] = jnp.broadcast_to(gain_ref[...].astype(F32), gainsrc.shape)
    for offset in range(1, ntp):
        start(gcopy(offset))
    icopies[1].wait()
    start(hcopy(0))
    icopies[2].wait()
    start(hcopy(1))
    icopies[3].wait()
    icopies[4].wait()
    for copy in wcopies:
        copy.start()
    taps = taps_ref[...].astype(F32)
    kw = taps_ref.shape[0]
    with jax.named_scope("conv"):
        inner[8 : 8 + seq, :] = gi[...].astype(F32) * ci[...].astype(F32)

        def mix(first, rows):
            filtered = taps[0:1, :] * inner[9 - kw + first : 9 - kw + first + rows, :]
            for k in range(1, kw):
                filtered = filtered + taps[k : k + 1, :] * inner[9 - kw + k + first : 9 - kw + k + first + rows, :]
            mixed[first : first + rows, :] = (go[first : first + rows, :].astype(F32) * filtered).astype(BF)

        mix(tok, seq - tok)
    with jax.named_scope("halo"):
        for i in (0, 1):
            hcopy(i).wait_recv()
    earlier = halo[0, 8:16, :].astype(F32) * halo[1, 8:16, :].astype(F32)
    inner[0:8, :] = jnp.where(sp > 0, earlier, 0.0)
    mix(0, tok)
    for offset in range(1, ntp):
        start(tcopy(offset))
    for kind in (0, 1):
        start(acopy(kind, 1))
    mixrel[0] = mixed[pl.ds(pl.multiple_of(tp * tok, tok), tok), :]

    with jax.named_scope("slots"):
        expert = lax.broadcasted_iota(jnp.int32, (nsp, tok), 0)
        hot = [jnp.where(expert == ids_ref[k : k + 1, :], 1.0, 0.0) for k in (0, 1)]
        earlier_tok = lax.broadcasted_iota(jnp.int32, (tok, tok), 0) < lax.broadcasted_iota(jnp.int32, (tok, tok), 1)
        upper = jnp.where(earlier_tok, 1.0, 0.0).astype(BF)
        rank = [jnp.dot(h.astype(BF), upper, preferred_element_type=F32) for h in hot]
        count = jnp.sum(hot[0], axis=1, keepdims=True)
        slot = expert.astype(F32) * CAP
        meta_ref[0:1, :] = jnp.sum((rank[0] + slot) * hot[0], axis=0, keepdims=True)
        meta_ref[1:2, :] = jnp.sum((rank[1] + count + slot) * hot[1], axis=0, keepdims=True)
        meta_ref[2:3, :] = group_ref[...] * route_ref[0:1, :] / (route_ref[0:1, :] + route_ref[1:2, :])
        meta_ref[3:4, :] = group_ref[...] * route_ref[1:2, :] / (route_ref[0:1, :] + route_ref[1:2, :])
        meta_ref[4:8, :] = jnp.zeros((4, tok), F32)
    for offset in range(1, NZ):
        start(mcopy(offset))

    def pass_on(n):
        acopy(0, n).wait_recv()
        start(acopy(2, n))
        start(acopy(4, n))
        acopy(1, n).wait_recv()
        start(acopy(3, n))
        start(acopy(5, n))

    with jax.named_scope("pass0"):
        pass_on(0)
    for kind in (0, 1):
        start(acopy(kind, 2))
    with jax.named_scope("rows"):
        for offset in range(1, ntp):
            tcopy(offset).wait_recv()
            gcopy(offset).wait_recv()
    gainrel[0] = gainsrc[...]
    with jax.named_scope("norm"):
        square = jnp.zeros((tok, 1), F32)
        for o in range(ntp):
            part = mixrel[o].astype(F32)
            square = square + jnp.sum(part * part, axis=1, keepdims=True)
        factor = lax.rsqrt(square / (chan * ntp) + EPSILON)
        for o in range(ntp):
            normed[o] = (mixrel[o].astype(F32) * factor * gainrel[o, 0:1, :]).astype(BF)
    for n in range(NC):
        if n > 0:
            with jax.named_scope(f"pass{n}"):
                pass_on(n)
            if n + 2 < NC:
                for kind in (0, 1):
                    start(acopy(kind, n + 2))
        with jax.named_scope(f"ring{n}"):
            acopy(2, n).wait_recv()
            acopy(3, n).wait_recv()
            start(acopy(6, n))
            for kind in (4, 5, 6):
                acopy(kind, n).wait_recv()
        with jax.named_scope(f"proj{n}"):
            cols = cols_of(n)
            total = rin[:, cols].astype(F32) + jnp.dot(normed[0], ow[:, cols], preferred_element_type=F32)
            for o in range(1, ntp):
                total = total + jnp.dot(normed[o], wrel[o, :, cols], preferred_element_type=F32)
            res_ref[:, cols] = total.astype(BF)
        for d in (0, 1):
            start(zcopy(0, d, n))

    def meta_of(offset):
        return meta_ref if offset == 0 else metas.at[offset]

    def slots_of(target):
        return (lax.broadcasted_iota(jnp.int32, (grp, tok), 0) + target * grp).astype(F32)

    def select(offset, target):
        ref = meta_of(offset)
        slot = slots_of(target)
        hit = jnp.where(slot == ref[0:1, :], 1.0, 0.0) + jnp.where(slot == ref[1:2, :], 1.0, 0.0)
        return hit.astype(BF)

    def spread(offset, target):
        ref = meta_of(offset)
        slot = slots_of(target)
        hit = jnp.where(slot == ref[0:1, :], ref[2:3, :], 0.0) + jnp.where(slot == ref[1:2, :], ref[3:4, :], 0.0)
        return hit.astype(BF)

    def combine(weights, rows):
        return lax.dot_general(weights, rows, (((0,), (0,)), ((), ())), preferred_element_type=F32)

    def ytarget(b):
        return ret0 if b == 0 else ret1.at[b - 1] if b < 3 else ret2.at[b - 3]

    def xstart(b):
        for offset in range(1, nj):
            their = slot_rows(0, lax.rem(me_j + offset, nj))
            start_only(remote(packed.at[b, their, :], arrived.at[slot_rows(b, me_j), :], xsend.at[b], xrecv.at[b], jid(offset)))
        arrived[slot_rows(b, me_j), :] = packed[b, slot_rows(0, me_j), :]
        pending.append((packed.at[b, 0:others, :], xsend.at[b]))

    pending = []

    def start_only(copy):
        copy.start()

    def xwait(b):
        wait_bytes(arrived.at[b * grp : b * grp + others, :], xrecv.at[b])

    def ystart(b):
        dst = ytarget(b)
        for offset in range(1, nj):
            their = slot_rows(b, lax.rem(me_j + offset, nj))
            start_only(remote(results.at[their, :], dst.at[slot_rows(0, me_j), :], ysend.at[b], yrecv.at[b], jid(offset)))
        dst[slot_rows(0, me_j), :] = results[slot_rows(b, me_j), :]
        pending.append((dst.at[0:others, :], ysend.at[b]))

    def ywait(b):
        wait_bytes(ytarget(b).at[0:others, :], yrecv.at[b])

    def exchange(src, dst, d, cols, ssem, rsem):
        mine = slot_rows(0, me_j)
        for offset in range(1, nj):
            their = slot_rows(0, lax.rem(me_j + offset, nj))
            start_only(remote(src.at[d, their, cols], dst.at[d, mine, cols], ssem, rsem, jid(offset)))
        dst[d, mine, cols] = src[d, mine, cols]
        pending.append((src.at[d, 0:others, cols], ssem))

    def pack(b, offset, block):
        chosen = select(offset, z)
        for n in range(NC):
            cols = cols_of(n)
            packed[b, :, cols] = jnp.dot(chosen, block[:, cols], preferred_element_type=F32).astype(BF)

    fe = wg.shape[1]
    fw = fe // 2

    def experts(first, count):
        rows = count * grp
        base = first * grp

        def norm(i, carry):
            from_rows = pl.ds(pl.multiple_of(base + i * 32, 32), 32)
            vals = arrived[from_rows, :].astype(F32)
            factor = lax.rsqrt(jnp.mean(vals * vals, axis=1, keepdims=True) + EPSILON)
            act[pl.ds(pl.multiple_of(i * 32, 32), 32), :] = (vals * factor * mgain_ref[...].astype(F32)).astype(BF)
            return carry

        lax.fori_loop(0, rows // 32, norm, 0)

        def up(f, carry):
            cols = pl.ds(pl.multiple_of(f * fw, fw), fw)
            x = act[0:rows, :]
            g = jnp.dot(x, wg[:, cols], preferred_element_type=F32)
            u = jnp.dot(x, wu[:, cols], preferred_element_type=F32)
            hid[0:rows, cols] = (g * jax.nn.sigmoid(g) * u).astype(BF)
            return carry

        lax.fori_loop(0, 2, up, 0)

        def down(n, carry):
            cols = pl.ds(pl.multiple_of(n * cw, cw), cw)
            r = jnp.dot(hid[0:rows, :], wd[:, cols], preferred_element_type=F32)
            results[base : base + rows, cols] = r.astype(BF)
            return carry

        lax.fori_loop(0, NC, down, 0)

    with jax.named_scope("own"):
        pack(0, 0, res_ref)
        xstart(0)
    for n, d in both:
        with jax.named_scope(f"hop1_{n}{d}"):
            zcopy(0, d, n).wait_recv()
        start(zcopy(1, d, n))
    with jax.named_scope("metas"):
        for offset in range(1, NZ):
            mcopy(offset).wait_recv()
    with jax.named_scope("pack1"):
        for d in (0, 1):
            pack(1 + d, near[d], hop1.at[d])
            xstart(1 + d)
    for copy in wcopies:
        copy.wait()
    for d in (0, 1):
        sel3[d] = select(far[d], zval(step[d]))
        sel4[d] = select(far[d], zval(2 * step[d]))
    xwait(0)
    with jax.named_scope("exp0"):
        experts(0, 1)

    def hop3_out(n):
        for d in (0, 1):
            with jax.named_scope(f"ex{n}{d}"):
                wait_bytes(gather3.at[d, 0:others, cols_of(n)], grecv.at[0, d, n])
                wait_bytes(gather4.at[d, 0:others, half_of(n)], grecv.at[1, d, n])
            start(zcopy(3, d, n))
            start(zcopy(2, d, n))

    for n in range(NC):
        for d in (0, 1):
            with jax.named_scope(f"hop2_{n}{d}"):
                zcopy(1, d, n).wait_recv()
            part = hop2[d, :, cols_of(n)]
            pack3[d, :, cols_of(n)] = jnp.dot(sel3[d], part, preferred_element_type=F32).astype(BF)
            part = hop2[d, :, part_of(n, d)]
            pack4[d, :, half_of(n)] = jnp.dot(sel4[d], part, preferred_element_type=F32).astype(BF)
            exchange(pack4, gather4, d, half_of(n), gsend.at[1, d, n], grecv.at[1, d, n])
            exchange(pack3, gather3, d, cols_of(n), gsend.at[0, d, n], grecv.at[0, d, n])
        if n > 0:
            hop3_out(n - 1)
    with jax.named_scope("pack2"):
        for d in (0, 1):
            pack(3 + d, far[d], hop2.at[d])
            xstart(3 + d)
    hop3_out(NC - 1)
    xwait(1)
    xwait(2)
    with jax.named_scope("exp12"):
        experts(1, 2)

    def rcopy(kind, d, n):
        cols = cols_of(n)
        if kind == 0:
            src, dst = results.at[block_rows(7), part_of(n, d)], back4.at[d, :, half_of(n)]
        elif kind == 1:
            src, dst = results.at[block_rows(5 + d), cols], got3.at[d, :, cols]
        elif kind == 2:
            src, dst = back4.at[d, :, half_of(n)], got4.at[d, :, half_of(n)]
        elif kind == 3:
            src, dst = send2.at[d, :, cols], part2.at[d, :, cols]
        else:
            src, dst = send1.at[d, :, cols], part1.at[d, :, cols]
        return remote(src, dst, rsend.at[kind, d, n], rrecv.at[kind, d, n], zid(-step[d]))

    for n, d in both:
        with jax.named_scope(f"hop3_{n}{d}"):
            zcopy(3, d, n).wait_recv()
        start(zcopy(4, d, n))
    xwait(3)
    xwait(4)
    with jax.named_scope("exp34"):
        experts(3, 2)
    ystart(3)
    ystart(4)
    with jax.named_scope("hop3w"):
        for n, d in both:
            zcopy(2, d, n).wait_recv()
    with jax.named_scope("exp56"):
        experts(5, 2)
    for n, d in both:
        start(rcopy(1, d, n))
    with jax.named_scope("hop4w"):
        for n, d in both:
            zcopy(4, d, n).wait_recv()
    with jax.named_scope("exp7"):
        experts(7, 1)
    for n, d in both:
        start(rcopy(0, d, n))
    for n, d in both:
        with jax.named_scope(f"r3_{n}{d}"):
            rcopy(1, d, n).wait_recv()
        exchange(got3, ret3, d, cols_of(n), bsend.at[0, d, n], brecv.at[0, d, n])
    for n, d in both:
        with jax.named_scope(f"r4_{n}{d}"):
            rcopy(0, d, n).wait_recv()
        start(rcopy(2, d, n))
    ywait(3)
    ywait(4)

    def sums2_out(n):
        for d in (0, 1):
            with jax.named_scope(f"ex{n}{d}"):
                wait_bytes(ret3.at[d, 0:others, cols_of(n)], brecv.at[0, d, n])
                wait_bytes(ret4.at[d, 0:others, half_of(n)], brecv.at[1, d, n])
            total = combine(spread(far[d], z), ret2[d, :, cols_of(n)])
            total = total + combine(spread(far[d], zval(step[d])), ret3[d, :, cols_of(n)])
            last = combine(spread(far[d], zval(2 * step[d])), ret4[d, :, half_of(n)])
            lo, hi = total[:, :hw], total[:, hw:]
            if d == 0:
                lo = lo + last
            else:
                hi = hi + last
            send2[d, :, part_of(n, 0)] = lo.astype(BF)
            send2[d, :, part_of(n, 1)] = hi.astype(BF)
            start(rcopy(3, d, n))

    for n in range(NC):
        for d in (0, 1):
            with jax.named_scope(f"r3b_{n}{d}"):
                rcopy(2, d, n).wait_recv()
            exchange(got4, ret4, d, half_of(n), bsend.at[1, d, n], brecv.at[1, d, n])
        if n > 0:
            sums2_out(n - 1)
    sums2_out(NC - 1)
    ystart(1)
    ystart(2)
    ystart(0)
    ywait(1)
    ywait(2)
    for n, d in both:
        with jax.named_scope(f"r2_{n}{d}"):
            rcopy(3, d, n).wait_recv()
        cols = cols_of(n)
        total = part2[d, :, cols].astype(F32) + combine(spread(near[d], z), ret1[d, :, cols])
        send1[d, :, cols] = total.astype(BF)
        start(rcopy(4, d, n))
    ywait(0)
    own = spread(0, z)
    for n in range(NC):
        with jax.named_scope(f"r1_{n}"):
            rcopy(4, 0, n).wait_recv()
            rcopy(4, 1, n).wait_recv()
        cols = cols_of(n)
        total = res_ref[:, cols].astype(F32) + combine(own, ret0[:, cols])
        total = total + part1[0, :, cols].astype(F32) + part1[1, :, cols].astype(F32)
        out_ref[:, cols] = total.astype(BF)
    for copy in sent:
        copy.wait_send()
    for ref, sem in pending:
        wait_bytes(ref, sem)


def body(
    residual_in,
    gate_outer,
    gate_inner,
    conv_input,
    conv_taps,
    norm_gain,
    out_weight,
    moe_gain,
    expert_ids,
    group_prob,
    route_prob,
    expert_gate,
    expert_up,
    expert_down,
):
    tok, width = residual_in.shape
    seq, chan = conv_input.shape
    fe = expert_gate.shape[2]
    ntp = lax.axis_size("tp")
    nj = lax.axis_size("sp") // NZ
    grp = nj * CAP
    vmem = pl.BlockSpec(memory_space=pltpu.VMEM)
    hbm = pl.BlockSpec(memory_space=pl.ANY)
    dma = pltpu.SemaphoreType.DMA
    shapes = [
        ((tok, width), BF),
        ((seq, chan), BF),
        ((seq, chan), BF),
        ((seq, chan), BF),
        ((chan, width), BF),
        ((2, 16, chan), BF),
        ((seq + 8, chan), F32),
        ((seq, chan), BF),
        ((ntp, tok, chan), BF),
        ((8, chan), F32),
        ((ntp, 8, chan), F32),
        ((ntp, tok, chan), BF),
        ((ntp, chan, width), BF),
        ((tok, width), BF),
        ((8, tok), F32),
        ((2 * grp, width), BF),
        ((NZ, 8, tok), F32),
        ((2, tok, width), BF),
        ((2, tok, width), BF),
        ((2, grp, tok), BF),
        ((2, grp, tok), BF),
        ((2, grp, width), BF),
        ((2, grp, width // 2), BF),
        ((2, grp, width), BF),
        ((2, grp, width // 2), BF),
        ((2, grp, width // 2), BF),
        ((5, grp, width), BF),
        ((8 * grp, width), BF),
        ((8 * grp, width), BF),
        ((grp, width), BF),
        ((2, grp, width), BF),
        ((2, grp, width), BF),
        ((2, grp, width), BF),
        ((2, grp, width // 2), BF),
        ((2, grp, width // 2), BF),
        ((2, grp, width), BF),
        ((2, grp, width // 2), BF),
        ((2, tok, width), BF),
        ((2, tok, width), BF),
        ((2, tok, width), BF),
        ((2, tok, width), BF),
        ((2 * grp, fe), BF),
        ((width, fe), BF),
        ((width, fe), BF),
        ((fe, width), BF),
    ]
    sems = [(5,), (3,), (2,), (2,), (2, ntp), (2, ntp), (7, NC), (7, NC)]
    sems += [(NZ,), (NZ,), (5, 2, NC), (5, 2, NC), (5,), (5,), (5,), (5,)]
    sems += [(2, 2, NC), (2, 2, NC), (2, 2, NC), (2, 2, NC), (5, 2, NC), (5, 2, NC)]
    return pl.pallas_call(
        layer_kernel,
        out_shape=jax.ShapeDtypeStruct((tok, width), BF),
        in_specs=[hbm] * 8 + [vmem] * 6,
        out_specs=vmem,
        scratch_shapes=[pltpu.VMEM(s, t) for s, t in shapes] + [dma(s) for s in sems],
        compiler_params=pltpu.CompilerParams(
            collective_id=0, has_side_effects=True, vmem_limit_bytes=61 * 1024 * 1024
        ),
        name="layer",
    )(
        residual_in,
        gate_outer,
        gate_inner,
        conv_input,
        out_weight,
        expert_gate,
        expert_up,
        expert_down,
        conv_taps,
        norm_gain.reshape(1, chan),
        moe_gain.reshape(1, width),
        expert_ids.T,
        group_prob.reshape(1, tok),
        route_prob.T,
    )


def solution(mesh):
    in_specs = (
        P(("sp", "tp"), None),
        P("sp", "tp"),
        P("sp", "tp"),
        P("sp", "tp"),
        P(None, "tp"),
        P("tp"),
        P("tp", None),
        P(),
        P(("sp", "tp"), None),
        P(("sp", "tp")),
        P(("sp", "tp"), None),
        P("sp", None, None),
        P("sp", None, None),
        P("sp", None, None),
    )
    out_specs = P(("sp", "tp"), None)
    return jax.shard_map(body, mesh=mesh, in_specs=in_specs, out_specs=out_specs, check_vma=False)
```

```python
import jax
import jax.numpy as jnp
from jax import lax
from jax.experimental import pallas as pl
from jax.experimental.pallas import tpu as pltpu
from jax.sharding import PartitionSpec as P

EPSILON = 1e-06
NZ = 8
CAP = 16
NC = 4
MESH = pl.DeviceIdType.MESH
BF = jnp.bfloat16
F32 = jnp.float32


def layer_kernel(
    rin_hbm,
    go_hbm,
    gi_hbm,
    ci_hbm,
    ow_hbm,
    wg_hbm,
    wu_hbm,
    wd_hbm,
    taps_ref,
    gain_ref,
    mgain_ref,
    ids_ref,
    group_ref,
    route_ref,
    out_ref,
    rin,
    go,
    gi,
    ci,
    ow,
    halo,
    inner,
    mixed,
    mixrel,
    gainsrc,
    gainrel,
    normed,
    normed_near,
    wrel,
    res_ref,
    meta_ref,
    squares,
    gate,
    value,
    mgain,
    out,
    sel,
    metas,
    hop1,
    hop2,
    sel3,
    sel4,
    pack3,
    pack4,
    gather3,
    gather4,
    pass4,
    packed,
    arrived,
    results,
    ret0,
    ret1,
    ret2,
    got3,
    back4,
    got4,
    ret3,
    ret4,
    send2,
    part2,
    send1,
    part1,
    hid,
    wg,
    wu,
    wd,
    isem,
    osem,
    wsem,
    ssem,
    trecv,
    arecv,
    nrecv,
    mrecv,
    zrecv,
    xrecv,
    yrecv,
    grecv,
    brecv,
    rrecv,
):
    tok, width = res_ref.shape
    nsp = lax.axis_size("sp")
    ntp = lax.axis_size("tp")
    nj = nsp // NZ
    grp = nj * CAP
    seq, chan = mixed.shape
    others = grp - CAP
    cw = width // NC
    hw = cw // 2
    sp = lax.axis_index("sp")
    tp = lax.axis_index("tp")
    z = sp // nj
    me_j = sp % nj
    step = (1, -1)
    near = (1, NZ - 1)
    far = (2, NZ - 2)
    both = [(n, d) for n in range(NC) for d in (0, 1)]

    def zval(offset):
        return lax.rem(z + offset + NZ, NZ)

    def zid(offset):
        return (zval(offset) * nj + me_j, tp)

    def jid(offset):
        return (z * nj + lax.rem(me_j + offset, nj), tp)

    def tid(offset):
        return (sp, lax.rem(tp + offset, ntp))

    after = (lax.rem(sp + 1, nsp), tp)
    before = (lax.rem(sp + nsp - 1, nsp), tp)
    core = lax.rem(me_j, 2)
    partner = (z * nj + me_j + 1 - 2 * core, tp)

    def cols_of(n):
        return slice(n * cw, (n + 1) * cw)

    def half_of(n):
        return slice(n * hw, (n + 1) * hw)

    def part_of(n, d):
        return slice(n * cw + d * hw, n * cw + (d + 1) * hw)

    def slot_rows(b, j):
        return pl.ds(pl.multiple_of(b * grp + j * CAP, CAP), CAP)

    def block_rows(b):
        return slice(b * grp, (b + 1) * grp)

    near_z, far_z, back_near, back_far, xs, ys, gs, bs, ring, rows_t, gains_t, halo_t, metas_z, normed_z = range(14)

    def remote(src, dst, send, recv, device):
        return pltpu.make_async_remote_copy(
            src_ref=src, dst_ref=dst, send_sem=send, recv_sem=recv, device_id=device, device_id_type=MESH
        )

    def wait_bytes(ref, sem):
        pltpu.make_async_copy(ref, ref, sem).wait()

    def make_slots():
        expert = lax.broadcasted_iota(jnp.int32, (nsp, tok), 0)
        hot = [jnp.where(expert == ids_ref[k : k + 1, :], 1.0, 0.0) for k in (0, 1)]
        earlier_tok = lax.broadcasted_iota(jnp.int32, (tok, tok), 0) < lax.broadcasted_iota(jnp.int32, (tok, tok), 1)
        upper = jnp.where(earlier_tok, 1.0, 0.0).astype(BF)
        rank = [jnp.dot(h.astype(BF), upper, preferred_element_type=F32) for h in hot]
        count = jnp.sum(hot[0], axis=1, keepdims=True)
        slot = expert.astype(F32) * CAP
        meta_ref[0:1, :] = jnp.sum((rank[0] + slot) * hot[0], axis=0, keepdims=True)
        meta_ref[1:2, :] = jnp.sum((rank[1] + count + slot) * hot[1], axis=0, keepdims=True)
        meta_ref[2:3, :] = group_ref[...] * route_ref[0:1, :] / (route_ref[0:1, :] + route_ref[1:2, :])
        meta_ref[3:4, :] = group_ref[...] * route_ref[1:2, :] / (route_ref[0:1, :] + route_ref[1:2, :])
        meta_ref[4:8, :] = jnp.zeros((4, tok), F32)

    icopies = [
        pltpu.make_async_copy(src, dst, isem.at[i])
        for i, (src, dst) in enumerate(((ow_hbm, ow), (rin_hbm, rin), (gi_hbm, gi), (ci_hbm, ci), (go_hbm, go)))
    ]
    wcopies = [
        pltpu.make_async_copy(wg_hbm.at[0], wg, wsem.at[0]),
        pltpu.make_async_copy(wu_hbm.at[0], wu, wsem.at[1]),
        pltpu.make_async_copy(wd_hbm.at[0], wd, wsem.at[2]),
    ]
    barrier = pltpu.get_barrier_semaphore()
    for offset in (1, -1):
        pl.semaphore_signal(barrier, inc=1, device_id=zid(offset), device_id_type=MESH)
    for offset in range(1, nj):
        pl.semaphore_signal(barrier, inc=1, device_id=jid(offset), device_id_type=MESH)
    for offset in range(1, ntp):
        pl.semaphore_signal(barrier, inc=1, device_id=tid(offset), device_id_type=MESH)
    for ident in (after, before):
        pl.semaphore_signal(barrier, inc=1, device_id=ident, device_id_type=MESH)
    for copy in icopies:
        copy.start()
    make_slots()
    with jax.named_scope("barrier"):
        pl.semaphore_wait(barrier, nj + ntp + 2)

    def mcopy(hop, d):
        src = metas.at[near[d]] if hop else meta_ref
        dst = metas.at[far[d] if hop else near[d]]
        return remote(src, dst, ssem.at[metas_z], mrecv.at[hop, d], zid(step[d]))

    def zcopy(hop, d, n):
        cols = cols_of(n)
        if hop == 0:
            src, dst = rin.at[:, cols], hop1.at[d, :, cols]
        elif hop == 1:
            src, dst = hop1.at[d, :, cols], hop2.at[d, :, cols]
        elif hop == 2:
            src, dst = gather3.at[d, :, cols], arrived.at[block_rows(5 + d), cols]
        elif hop == 3:
            src, dst = gather4.at[d, :, half_of(n)], pass4.at[d, :, half_of(n)]
        else:
            src, dst = pass4.at[d, :, half_of(n)], arrived.at[block_rows(7), part_of(n, d)]
        return remote(src, dst, ssem.at[near_z if hop < 2 else far_z], zrecv.at[hop, d, n], zid(step[d]))

    def meta_of(offset):
        return meta_ref if offset == 0 else metas.at[offset]

    def slots_of(target):
        return (lax.broadcasted_iota(jnp.int32, (grp, tok), 0) + target * grp).astype(F32)

    def select(offset, target):
        ref = meta_of(offset)
        slot = slots_of(target)
        hit = jnp.where(slot == ref[0:1, :], 1.0, 0.0) + jnp.where(slot == ref[1:2, :], 1.0, 0.0)
        return hit.astype(BF)

    def spread(offset, target):
        ref = meta_of(offset)
        slot = slots_of(target)
        hit = jnp.where(slot == ref[0:1, :], ref[2:3, :], 0.0) + jnp.where(slot == ref[1:2, :], ref[3:4, :], 0.0)
        return hit.astype(BF)

    def combine(weights, rows):
        return lax.dot_general(weights, rows, (((0,), (0,)), ((), ())), preferred_element_type=F32)

    def ytarget(b):
        return ret0 if b == 0 else ret1.at[b - 1] if b < 3 else ret2.at[b - 3]

    def xstart(b, n):
        cols = cols_of(n)
        for offset in range(1, nj):
            their = slot_rows(0, lax.rem(me_j + offset, nj))
            src, dst = packed.at[b, their, cols], arrived.at[slot_rows(b, me_j), cols]
            remote(src, dst, ssem.at[xs], xrecv.at[b], jid(offset)).start()
        arrived[slot_rows(b, me_j), cols] = packed[b, slot_rows(0, me_j), cols]

    def xwait(b):
        wait_bytes(arrived.at[b * grp : b * grp + others, :], xrecv.at[b])

    def ystart(b):
        dst = ytarget(b)
        for offset in range(1, nj):
            their = slot_rows(b, lax.rem(me_j + offset, nj))
            remote(results.at[their, :], dst.at[slot_rows(0, me_j), :], ssem.at[ys], yrecv.at[b], jid(offset)).start()
        dst[slot_rows(0, me_j), :] = results[slot_rows(b, me_j), :]

    def ywait(b):
        wait_bytes(ytarget(b).at[0:others, :], yrecv.at[b])

    def exchange(src, dst, d, cols, send, recv):
        mine = slot_rows(0, me_j)
        for offset in range(1, nj):
            their = slot_rows(0, lax.rem(me_j + offset, nj))
            remote(src.at[d, their, cols], dst.at[d, mine, cols], send, recv, jid(offset)).start()
        dst[d, mine, cols] = src[d, mine, cols]

    def pack(b, block, n, go_now=True):
        cols = cols_of(n)
        packed[b, :, cols] = jnp.dot(sel[b], block[:, cols], preferred_element_type=F32).astype(BF)
        if go_now:
            xstart(b, n)

    def own_cols(n):
        return pl.ds(pl.multiple_of(n * cw + core * hw, hw), hw)

    def quarter_cols(n, d):
        return pl.ds(pl.multiple_of(n * cw + core * hw + d * (hw // 2), hw // 2), hw // 2)

    def acopy(kind, n):
        if kind == 0:
            src, dst, device = ow.at[:, own_cols(n)], wrel.at[3, :, own_cols(n)], tid(1)
        elif kind == 1:
            src, dst, device = ow.at[:, own_cols(n)], wrel.at[1, :, own_cols(n)], tid(ntp - 1)
        elif kind == 2:
            cols = quarter_cols(n, 0)
            src, dst, device = wrel.at[3, :, cols], wrel.at[2, :, cols], tid(1)
        elif kind == 3:
            cols = quarter_cols(n, 1)
            src, dst, device = wrel.at[1, :, cols], wrel.at[2, :, cols], tid(ntp - 1)
        else:
            cols = own_cols(n)
            block = (3, 1, 2)[kind - 4]
            src, dst, device = wrel.at[block, :, cols], wrel.at[block, :, cols], partner
        return remote(src, dst, ssem.at[ring], arecv.at[(0, 1, 2, 2, 3, 3, 3)[kind], n], device)

    def tcopy(offset):
        rows = pl.ds(pl.multiple_of(lax.rem(tp + offset, ntp) * tok, tok), tok)
        return remote(mixed.at[rows, :], mixrel.at[ntp - offset], ssem.at[rows_t], trecv.at[0], tid(offset))

    def gcopy(offset):
        return remote(gainsrc, gainrel.at[ntp - offset], ssem.at[gains_t], trecv.at[1], tid(offset))

    def hcopy(i):
        src = (gi_hbm, ci_hbm)[i]
        return remote(src.at[seq - 16 : seq, :], halo.at[i], ssem.at[halo_t], trecv.at[2], after)

    def pass_on(n):
        acopy(0, n).wait_recv()
        acopy(2, n).start()
        acopy(4, n).start()
        acopy(1, n).wait_recv()
        acopy(3, n).start()
        acopy(5, n).start()

    for i in (0, 1):
        hcopy(i).start()
    for d in (0, 1):
        mcopy(0, d).start()
    with jax.named_scope("inputs"):
        icopies[0].wait()
    for kind in (0, 1):
        acopy(kind, 0).start()
    with jax.named_scope("rin"):
        icopies[1].wait()
    for n in range(NC - 1):
        for d in (0, 1):
            zcopy(0, d, n).start()
    mgain[...] = jnp.broadcast_to(mgain_ref[...].astype(F32)[None, :], mgain.shape)
    gainsrc[...] = jnp.broadcast_to(gain_ref[...].astype(F32)[None, :], gainsrc.shape)
    for offset in range(1, ntp):
        gcopy(offset).start()
    for i in (2, 3, 4):
        icopies[i].wait()
    for copy in wcopies:
        copy.start()
    taps = taps_ref[...].astype(F32)
    kw = taps_ref.shape[0]
    with jax.named_scope("conv"):
        inner[8 : 8 + seq, :] = gi[...].astype(F32) * ci[...].astype(F32)

        def mix(first, rows):
            filtered = taps[0:1, :] * inner[9 - kw + first : 9 - kw + first + rows, :]
            for k in range(1, kw):
                filtered = filtered + taps[k : k + 1, :] * inner[9 - kw + k + first : 9 - kw + k + first + rows, :]
            mixed[first : first + rows, :] = (go[first : first + rows, :].astype(F32) * filtered).astype(BF)

        mix(tok, seq - tok)
    for offset in range(1, ntp):
        pl.when(lax.rem(tp + offset, ntp) != 0)(tcopy(offset).start)
    with jax.named_scope("pass0"):
        pass_on(0)
    with jax.named_scope("halo"):
        wait_bytes(halo, trecv.at[2])
    earlier = halo[0, 8:16, :].astype(F32) * halo[1, 8:16, :].astype(F32)
    inner[0:8, :] = jnp.where(sp > 0, earlier, 0.0)
    mix(0, tok)
    for offset in range(1, ntp):
        pl.when(lax.rem(tp + offset, ntp) == 0)(tcopy(offset).start)
    mixrel[0] = mixed[pl.ds(pl.multiple_of(tp * tok, tok), tok), :]

    with jax.named_scope("rows"):
        wait_bytes(mixrel.at[1:ntp], trecv.at[0])
        wait_bytes(gainrel.at[1:ntp], trecv.at[1])
    gainrel[0] = gainsrc[...]
    for n in (1, 2):
        for kind in (0, 1):
            acopy(kind, n).start()
    with jax.named_scope("norm"):
        square = jnp.zeros((tok, 1), F32)
        for o in range(ntp):
            part = mixrel[o].astype(F32)
            square = square + jnp.sum(part * part, axis=1, keepdims=True)
        factor = lax.rsqrt(square / (chan * ntp) + EPSILON)
        for o in range(ntp):
            normed[o] = (mixrel[o].astype(F32) * factor * gainrel[o, 0:1, :]).astype(BF)

    def ncopy(d):
        return remote(normed, normed_near.at[d], ssem.at[normed_z], nrecv.at[d], zid(step[d]))

    for d in (0, 1):
        ncopy(d).start()
    for d in (0, 1):
        zcopy(0, d, NC - 1).start()

    def selections():
        sel[0] = select(0, z)
        for d in (0, 1):
            mcopy(0, d).wait_recv()
            mcopy(1, d).start()
            sel[1 + d] = select(near[d], z)

    def far_selections():
        for d in (0, 1):
            mcopy(1, d).wait_recv()
            sel[3 + d] = select(far[d], z)
            sel3[d] = select(far[d], zval(step[d]))
            sel4[d] = select(far[d], zval(2 * step[d]))

    def project(values, rows, n):
        cols = cols_of(n)
        total = values[:, cols].astype(F32) + jnp.dot(rows[0], ow[:, cols], preferred_element_type=F32)
        for o in range(1, ntp):
            total = total + jnp.dot(rows[o], wrel[o, :, cols], preferred_element_type=F32)
        return total.astype(BF)

    for n in range(NC):
        with jax.named_scope(f"ring{n}"):
            wait_bytes(wrel.at[2, :, 0:hw], arecv.at[2, n])
            acopy(6, n).start()
            wait_bytes(wrel.at[1:4, :, 0:hw], arecv.at[3, n])
        with jax.named_scope(f"proj{n}"):
            res_ref[:, cols_of(n)] = project(rin, normed, n)
        if n == 0:
            with jax.named_scope("selections"):
                selections()
        with jax.named_scope(f"own{n}"):
            pack(0, res_ref, n)
        for later in ((1, 2), (3,), (), ())[n]:
            with jax.named_scope(f"pass{later}"):
                pass_on(later)
            if later == 1:
                for kind in (0, 1):
                    acopy(kind, 3).start()

    def expert_in(first, count, n, fresh):
        rows = count * grp
        base = first * grp
        cols = pl.ds(pl.multiple_of(n * cw, cw), cw)
        vals = arrived[base : base + rows, cols].astype(F32)
        x = (vals * mgain[0:1, cols]).astype(BF)
        parts = jnp.sum(vals * vals, axis=1, keepdims=True)
        g = jnp.dot(x, wg[cols, :], preferred_element_type=F32)
        u = jnp.dot(x, wu[cols, :], preferred_element_type=F32)
        if fresh:
            squares[0:rows, :] = jnp.broadcast_to(parts, (rows, 128))
            gate[0:rows, :] = g
            value[0:rows, :] = u
        else:
            squares[0:rows, :] += jnp.broadcast_to(parts, (rows, 128))
            gate[0:rows, :] += g
            value[0:rows, :] += u

    def expert_mid(count):
        rows = count * grp
        factor = lax.rsqrt(squares[0:rows, 0:1] / width + EPSILON)
        g = gate[0:rows, :] * factor
        hid[0:rows, :] = (g * jax.nn.sigmoid(g) * (value[0:rows, :] * factor)).astype(BF)

    def expert_out(first, count, n):
        rows = count * grp
        cols = pl.ds(pl.multiple_of(n * cw, cw), cw)
        r = jnp.dot(hid[0:rows, :], wd[:, cols], preferred_element_type=F32)
        results[first * grp : first * grp + rows, cols] = r.astype(BF)

    def experts(first, count):
        expert_in(first, count, 0, True)

        def more(n, carry):
            expert_in(first, count, n, False)
            return carry

        lax.fori_loop(1, NC, more, 0)
        expert_mid(count)

        def out_cols(n, carry):
            expert_out(first, count, n)
            return carry

        lax.fori_loop(0, NC, out_cols, 0)

    with jax.named_scope("normed"):
        for d in (0, 1):
            ncopy(d).wait_recv()
    for n, d in both:
        with jax.named_scope(f"hop1_{n}{d}"):
            zcopy(0, d, n).wait_recv()
        hop1[d, :, cols_of(n)] = project(hop1.at[d], normed_near.at[d], n)
        zcopy(1, d, n).start()
        pack(1 + d, hop1.at[d], n)
    with jax.named_scope("far_selections"):
        far_selections()
    for copy in wcopies:
        copy.wait()
    xwait(0)
    with jax.named_scope("exp0"):
        experts(0, 1)

    def hop3_out(n):
        for d in (0, 1):
            with jax.named_scope(f"ex{n}{d}"):
                wait_bytes(gather3.at[d, 0:others, 0 : cw + hw], grecv.at[d, n])
            zcopy(3, d, n).start()
            zcopy(2, d, n).start()

    for n in range(NC):
        for d in (0, 1):
            with jax.named_scope(f"hop2_{n}{d}"):
                zcopy(1, d, n).wait_recv()
            part = hop2[d, :, cols_of(n)]
            pack3[d, :, cols_of(n)] = jnp.dot(sel3[d], part, preferred_element_type=F32).astype(BF)
            part = hop2[d, :, part_of(n, d)]
            pack4[d, :, half_of(n)] = jnp.dot(sel4[d], part, preferred_element_type=F32).astype(BF)
            exchange(pack4, gather4, d, half_of(n), ssem.at[gs], grecv.at[d, n])
            exchange(pack3, gather3, d, cols_of(n), ssem.at[gs], grecv.at[d, n])
            pack(3 + d, hop2.at[d], n, False)
        if n > 0:
            hop3_out(n - 1)
            xstart(3, n - 1)
            xstart(4, n - 1)
        if n == 1:
            xwait(1)
            xwait(2)
            with jax.named_scope("exp12"):
                experts(1, 2)
    hop3_out(NC - 1)
    xstart(3, NC - 1)
    xstart(4, NC - 1)

    def rcopy(kind, d, n):
        cols = cols_of(n)
        if kind == 0:
            src, dst = results.at[block_rows(7), part_of(n, d)], back4.at[d, :, half_of(n)]
        elif kind == 1:
            src, dst = results.at[block_rows(5 + d), cols], got3.at[d, :, cols]
        elif kind == 2:
            src, dst = back4.at[d, :, half_of(n)], got4.at[d, :, half_of(n)]
        elif kind == 3:
            src, dst = send2.at[d, :, cols], part2.at[d, :, cols]
        else:
            src, dst = send1.at[d, :, cols], part1.at[d, :, cols]
        return remote(src, dst, ssem.at[back_near if kind > 2 else back_far], rrecv.at[kind, d, n], zid(-step[d]))

    for n in range(NC):
        for d in (0, 1):
            with jax.named_scope(f"hop3_{n}{d}"):
                zcopy(3, d, n).wait_recv()
            zcopy(4, d, n).start()
        with jax.named_scope(f"hop3w{n}"):
            for d in (0, 1):
                zcopy(2, d, n).wait_recv()
        with jax.named_scope(f"in56_{n}"):
            expert_in(5, 2, n, n == 0)
    with jax.named_scope("out56"):
        expert_mid(2)
        for n in range(NC):
            expert_out(5, 2, n)
            for d in (0, 1):
                rcopy(1, d, n).start()
    with jax.named_scope("xw34"):
        xwait(3)
        xwait(4)
    with jax.named_scope("exp34"):
        experts(3, 2)
    ystart(3)
    ystart(4)
    for n in range(NC):
        with jax.named_scope(f"hop4w{n}"):
            for d in (0, 1):
                zcopy(4, d, n).wait_recv()
        with jax.named_scope(f"in7_{n}"):
            expert_in(7, 1, n, n == 0)
    with jax.named_scope("out7"):
        expert_mid(1)
        for n in range(NC):
            expert_out(7, 1, n)
            for d in (0, 1):
                rcopy(0, d, n).start()
    for n, d in both:
        with jax.named_scope(f"r3_{n}{d}"):
            rcopy(1, d, n).wait_recv()
        exchange(got3, ret3, d, cols_of(n), ssem.at[bs], brecv.at[d, n])
    for n, d in both:
        with jax.named_scope(f"r4_{n}{d}"):
            rcopy(0, d, n).wait_recv()
        rcopy(2, d, n).start()
    ywait(3)
    ywait(4)

    def sums2_out(n):
        for d in (0, 1):
            with jax.named_scope(f"ex{n}{d}"):
                wait_bytes(ret3.at[d, 0:others, 0 : cw + hw], brecv.at[d, n])
            total = combine(spread(far[d], z), ret2[d, :, cols_of(n)])
            total = total + combine(spread(far[d], zval(step[d])), ret3[d, :, cols_of(n)])
            last = combine(spread(far[d], zval(2 * step[d])), ret4[d, :, half_of(n)])
            lo, hi = total[:, :hw], total[:, hw:]
            if d == 0:
                lo = lo + last
            else:
                hi = hi + last
            send2[d, :, part_of(n, 0)] = lo.astype(BF)
            send2[d, :, part_of(n, 1)] = hi.astype(BF)
            rcopy(3, d, n).start()

    for n in range(NC):
        for d in (0, 1):
            with jax.named_scope(f"r3b_{n}{d}"):
                rcopy(2, d, n).wait_recv()
            exchange(got4, ret4, d, half_of(n), ssem.at[bs], brecv.at[d, n])
        if n > 0:
            sums2_out(n - 1)
    sums2_out(NC - 1)
    ystart(1)
    ystart(2)
    ystart(0)
    ywait(1)
    ywait(2)
    for n, d in both:
        with jax.named_scope(f"r2_{n}{d}"):
            rcopy(3, d, n).wait_recv()
        cols = cols_of(n)
        total = part2[d, :, cols].astype(F32) + combine(spread(near[d], z), ret1[d, :, cols])
        send1[d, :, cols] = total.astype(BF)
        rcopy(4, d, n).start()
    ywait(0)
    own = spread(0, z)
    ocopies = []
    for n in range(NC):
        with jax.named_scope(f"r1_{n}"):
            rcopy(4, 0, n).wait_recv()
            rcopy(4, 1, n).wait_recv()
        cols = cols_of(n)
        total = res_ref[:, cols].astype(F32) + combine(own, ret0[:, cols])
        total = total + part1[0, :, cols].astype(F32) + part1[1, :, cols].astype(F32)
        out[:, cols] = total.astype(BF)
        copy = pltpu.make_async_copy(out.at[:, cols], out_ref.at[:, cols], osem.at[n])
        copy.start()
        ocopies.append(copy)
    with jax.named_scope("ends"):
        for copy in ocopies:
            copy.wait()
        flat = ((near_z, 4 * tok), (far_z, 4 * grp), (back_near, 4 * tok), (back_far, 4 * grp), (xs, 5 * others), (ys, 5 * others))
        flat += ((gs, 3 * others), (bs, 3 * others), (ring, 3 * chan), (rows_t, 3 * tok * chan // width), (normed_z, 2 * ntp * tok * chan // width))
        for kind, rows in flat:
            wait_bytes(arrived.at[0:rows, :], ssem.at[kind])
        wait_bytes(gainrel.at[1:ntp], ssem.at[gains_t])
        wait_bytes(halo, ssem.at[halo_t])
        wait_bytes(metas.at[0:4], ssem.at[metas_z])


def body(
    residual_in,
    gate_outer,
    gate_inner,
    conv_input,
    conv_taps,
    norm_gain,
    out_weight,
    moe_gain,
    expert_ids,
    group_prob,
    route_prob,
    expert_gate,
    expert_up,
    expert_down,
):
    tok, width = residual_in.shape
    seq, chan = conv_input.shape
    fe = expert_gate.shape[2]
    ntp = lax.axis_size("tp")
    nj = lax.axis_size("sp") // NZ
    grp = nj * CAP
    vmem = pl.BlockSpec(memory_space=pltpu.VMEM)
    hbm = pl.BlockSpec(memory_space=pl.ANY)
    dma = pltpu.SemaphoreType.DMA
    shapes = [
        ((tok, width), BF),
        ((seq, chan), BF),
        ((seq, chan), BF),
        ((seq, chan), BF),
        ((chan, width), BF),
        ((2, 16, chan), BF),
        ((seq + 8, chan), F32),
        ((seq, chan), BF),
        ((ntp, tok, chan), BF),
        ((8, chan), F32),
        ((ntp, 8, chan), F32),
        ((ntp, tok, chan), BF),
        ((2, ntp, tok, chan), BF),
        ((ntp, chan, width), BF),
        ((tok, width), BF),
        ((8, tok), F32),
        ((2 * grp, 128), F32),
        ((2 * grp, fe), F32),
        ((2 * grp, fe), F32),
        ((8, width), F32),
        ((tok, width), BF),
        ((5, grp, tok), BF),
        ((NZ, 8, tok), F32),
        ((2, tok, width), BF),
        ((2, tok, width), BF),
        ((2, grp, tok), BF),
        ((2, grp, tok), BF),
        ((2, grp, width), BF),
        ((2, grp, width // 2), BF),
        ((2, grp, width), BF),
        ((2, grp, width // 2), BF),
        ((2, grp, width // 2), BF),
        ((5, grp, width), BF),
        ((8 * grp, width), BF),
        ((8 * grp, width), BF),
        ((grp, width), BF),
        ((2, grp, width), BF),
        ((2, grp, width), BF),
        ((2, grp, width), BF),
        ((2, grp, width // 2), BF),
        ((2, grp, width // 2), BF),
        ((2, grp, width), BF),
        ((2, grp, width // 2), BF),
        ((2, tok, width), BF),
        ((2, tok, width), BF),
        ((2, tok, width), BF),
        ((2, tok, width), BF),
        ((2 * grp, fe), BF),
        ((width, fe), BF),
        ((width, fe), BF),
        ((fe, width), BF),
    ]
    sems = [(5,), (NC,), (3,), (14,), (3,), (4, NC), (2,), (2, 2), (5, 2, NC), (5,), (5,), (2, NC), (2, NC), (5, 2, NC)]
    return pl.pallas_call(
        layer_kernel,
        out_shape=jax.ShapeDtypeStruct((tok, width), BF),
        in_specs=[hbm] * 8 + [vmem] * 6,
        out_specs=hbm,
        scratch_shapes=[pltpu.VMEM(s, t) for s, t in shapes] + [dma(s) for s in sems],
        compiler_params=pltpu.CompilerParams(
            collective_id=0, has_side_effects=True, vmem_limit_bytes=61 * 1024 * 1024
        ),
        name="layer",
    )(
        residual_in,
        gate_outer,
        gate_inner,
        conv_input,
        out_weight,
        expert_gate,
        expert_up,
        expert_down,
        conv_taps,
        norm_gain,
        moe_gain,
        expert_ids.T,
        group_prob.reshape(1, tok),
        route_prob.T,
    )


def solution(mesh):
    in_specs = (
        P(("sp", "tp"), None),
        P("sp", "tp"),
        P("sp", "tp"),
        P("sp", "tp"),
        P(None, "tp"),
        P("tp"),
        P("tp", None),
        P(),
        P(("sp", "tp"), None),
        P(("sp", "tp")),
        P(("sp", "tp"), None),
        P("sp", None, None),
        P("sp", None, None),
        P("sp", None, None),
    )
    out_specs = P(("sp", "tp"), None)
    return jax.shard_map(body, mesh=mesh, in_specs=in_specs, out_specs=out_specs, check_vma=False)
```

```python
import jax
import jax.numpy as jnp
from jax import lax
from jax.experimental import pallas as pl
from jax.experimental.pallas import tpu as pltpu
from jax.sharding import PartitionSpec as P

EPSILON = 1e-06
NZ = 8
CAP = 16
NC = 4
MESH = pl.DeviceIdType.MESH
BF = jnp.bfloat16
F32 = jnp.float32


def layer_kernel(
    rin_hbm,
    go_hbm,
    gi_hbm,
    ci_hbm,
    ow_hbm,
    wg_hbm,
    wu_hbm,
    wd_hbm,
    taps_ref,
    gain_ref,
    mgain_ref,
    ids_ref,
    group_ref,
    route_ref,
    out_ref,
    rin,
    go,
    gi,
    ci,
    ow,
    halo,
    inner,
    mixed,
    mixrel,
    gainsrc,
    gainrel,
    normed,
    normed_near,
    wrel,
    res_ref,
    meta_ref,
    squares,
    gate,
    value,
    mgain,
    out,
    sel,
    metas,
    hop1,
    hop2,
    sel3,
    sel4,
    pack3,
    pack4,
    gather3,
    gather4,
    pass4,
    packed,
    arrived,
    results,
    ret0,
    ret1,
    ret2,
    got3,
    back4,
    got4,
    ret3,
    ret4,
    send2,
    part2,
    send1,
    part1,
    hid,
    wg,
    wu,
    wd,
    isem,
    osem,
    wsem,
    ssem,
    trecv,
    arecv,
    nrecv,
    mrecv,
    zrecv,
    xrecv,
    yrecv,
    grecv,
    brecv,
    rrecv,
):
    tok, width = res_ref.shape
    nsp = lax.axis_size("sp")
    ntp = lax.axis_size("tp")
    nj = nsp // NZ
    grp = nj * CAP
    seq, chan = mixed.shape
    others = grp - CAP
    cw = width // NC
    hw = cw // 2
    sp = lax.axis_index("sp")
    tp = lax.axis_index("tp")
    z = sp // nj
    me_j = sp % nj
    step = (1, -1)
    near = (1, NZ - 1)
    far = (2, NZ - 2)
    both = [(n, d) for n in range(NC) for d in (0, 1)]

    def zval(offset):
        return lax.rem(z + offset + NZ, NZ)

    def zid(offset):
        return (zval(offset) * nj + me_j, tp)

    def jid(offset):
        return (z * nj + lax.rem(me_j + offset, nj), tp)

    def tid(offset):
        return (sp, lax.rem(tp + offset, ntp))

    after = (lax.rem(sp + 1, nsp), tp)
    before = (lax.rem(sp + nsp - 1, nsp), tp)
    core = lax.rem(me_j, 2)
    partner = (z * nj + me_j + 1 - 2 * core, tp)

    def cols_of(n):
        return slice(n * cw, (n + 1) * cw)

    def half_of(n):
        return slice(n * hw, (n + 1) * hw)

    def part_of(n, d):
        return slice(n * cw + d * hw, n * cw + (d + 1) * hw)

    def slot_rows(b, j):
        return pl.ds(pl.multiple_of(b * grp + j * CAP, CAP), CAP)

    def block_rows(b):
        return slice(b * grp, (b + 1) * grp)

    near_z, far_z, back_near, back_far, xs, ys, gs, bs, ring, rows_t, gains_t, halo_t, metas_z, normed_z = range(14)

    def remote(src, dst, send, recv, device):
        return pltpu.make_async_remote_copy(
            src_ref=src, dst_ref=dst, send_sem=send, recv_sem=recv, device_id=device, device_id_type=MESH
        )

    def wait_bytes(ref, sem):
        pltpu.make_async_copy(ref, ref, sem).wait()

    def make_slots():
        expert = lax.broadcasted_iota(jnp.int32, (nsp, tok), 0)
        hot = [jnp.where(expert == ids_ref[k : k + 1, :], 1.0, 0.0) for k in (0, 1)]
        earlier_tok = lax.broadcasted_iota(jnp.int32, (tok, tok), 0) < lax.broadcasted_iota(jnp.int32, (tok, tok), 1)
        upper = jnp.where(earlier_tok, 1.0, 0.0).astype(BF)
        rank = [jnp.dot(h.astype(BF), upper, preferred_element_type=F32) for h in hot]
        count = jnp.sum(hot[0], axis=1, keepdims=True)
        slot = expert.astype(F32) * CAP
        meta_ref[0:1, :] = jnp.sum((rank[0] + slot) * hot[0], axis=0, keepdims=True)
        meta_ref[1:2, :] = jnp.sum((rank[1] + count + slot) * hot[1], axis=0, keepdims=True)
        meta_ref[2:3, :] = group_ref[...] * route_ref[0:1, :] / (route_ref[0:1, :] + route_ref[1:2, :])
        meta_ref[3:4, :] = group_ref[...] * route_ref[1:2, :] / (route_ref[0:1, :] + route_ref[1:2, :])
        meta_ref[4:8, :] = jnp.zeros((4, tok), F32)

    icopies = [
        pltpu.make_async_copy(src, dst, isem.at[i])
        for i, (src, dst) in enumerate(((ow_hbm, ow), (rin_hbm, rin), (gi_hbm, gi), (ci_hbm, ci), (go_hbm, go)))
    ]
    wcopies = [
        pltpu.make_async_copy(wg_hbm.at[0], wg, wsem.at[0]),
        pltpu.make_async_copy(wu_hbm.at[0], wu, wsem.at[1]),
        pltpu.make_async_copy(wd_hbm.at[0], wd, wsem.at[2]),
    ]
    barrier = pltpu.get_barrier_semaphore()
    for offset in (1, -1):
        pl.semaphore_signal(barrier, inc=1, device_id=zid(offset), device_id_type=MESH)
    for offset in range(1, nj):
        pl.semaphore_signal(barrier, inc=1, device_id=jid(offset), device_id_type=MESH)
    for offset in range(1, ntp):
        pl.semaphore_signal(barrier, inc=1, device_id=tid(offset), device_id_type=MESH)
    for ident in (after, before):
        pl.semaphore_signal(barrier, inc=1, device_id=ident, device_id_type=MESH)
    for copy in icopies:
        copy.start()
    make_slots()
    with jax.named_scope("barrier"):
        pl.semaphore_wait(barrier, nj + ntp + 2)

    def mcopy(hop, d):
        src = metas.at[near[d]] if hop else meta_ref
        dst = metas.at[far[d] if hop else near[d]]
        return remote(src, dst, ssem.at[metas_z], mrecv.at[hop, d], zid(step[d]))

    def zcopy(hop, d, n):
        cols = cols_of(n)
        if hop == 0:
            src, dst = rin.at[:, cols], hop1.at[d, :, cols]
        elif hop == 1:
            src, dst = hop1.at[d, :, cols], hop2.at[d, :, cols]
        elif hop == 2:
            src, dst = gather3.at[d, :, cols], arrived.at[block_rows(5 + d), cols]
        elif hop == 3:
            src, dst = gather4.at[d, :, half_of(n)], pass4.at[d, :, half_of(n)]
        else:
            src, dst = pass4.at[d, :, half_of(n)], arrived.at[block_rows(7), part_of(n, d)]
        return remote(src, dst, ssem.at[near_z if hop < 2 else far_z], zrecv.at[hop, d, n], zid(step[d]))

    def meta_of(offset):
        return meta_ref if offset == 0 else metas.at[offset]

    def slots_of(target):
        return (lax.broadcasted_iota(jnp.int32, (grp, tok), 0) + target * grp).astype(F32)

    def select(offset, target):
        ref = meta_of(offset)
        slot = slots_of(target)
        hit = jnp.where(slot == ref[0:1, :], 1.0, 0.0) + jnp.where(slot == ref[1:2, :], 1.0, 0.0)
        return hit.astype(BF)

    def spread(offset, target):
        ref = meta_of(offset)
        slot = slots_of(target)
        hit = jnp.where(slot == ref[0:1, :], ref[2:3, :], 0.0) + jnp.where(slot == ref[1:2, :], ref[3:4, :], 0.0)
        return hit.astype(BF)

    def combine(weights, rows):
        return lax.dot_general(weights, rows, (((0,), (0,)), ((), ())), preferred_element_type=F32)

    def ytarget(b):
        return ret0 if b == 0 else ret1.at[b - 1] if b < 3 else ret2.at[b - 3]

    def xstart(b, n):
        cols = cols_of(n)
        for offset in range(1, nj):
            their = slot_rows(0, lax.rem(me_j + offset, nj))
            src, dst = packed.at[b, their, cols], arrived.at[slot_rows(b, me_j), cols]
            remote(src, dst, ssem.at[xs], xrecv.at[b], jid(offset)).start()
        arrived[slot_rows(b, me_j), cols] = packed[b, slot_rows(0, me_j), cols]

    def xwait(b):
        wait_bytes(arrived.at[b * grp : b * grp + others, :], xrecv.at[b])

    def ypart(b, part):
        return (slice(0, width), b) if b < 3 else (slice(part * (width // 2), (part + 1) * (width // 2)), 3 + 2 * (b - 3) + part)

    def ystart(b, part=0):
        dst = ytarget(b)
        cols, index = ypart(b, part)
        for offset in range(1, nj):
            their = slot_rows(b, lax.rem(me_j + offset, nj))
            src = results.at[their, cols]
            remote(src, dst.at[slot_rows(0, me_j), cols], ssem.at[ys], yrecv.at[index], jid(offset)).start()
        dst[slot_rows(0, me_j), cols] = results[slot_rows(b, me_j), cols]

    def ywait(b, part=0):
        cols, index = ypart(b, part)
        wait_bytes(ytarget(b).at[0:others, cols], yrecv.at[index])

    def exchange(src, dst, d, cols, send, recv):
        mine = slot_rows(0, me_j)
        for offset in range(1, nj):
            their = slot_rows(0, lax.rem(me_j + offset, nj))
            remote(src.at[d, their, cols], dst.at[d, mine, cols], send, recv, jid(offset)).start()
        dst[d, mine, cols] = src[d, mine, cols]

    def pack(b, block, n, go_now=True):
        cols = cols_of(n)
        packed[b, :, cols] = jnp.dot(sel[b], block[:, cols], preferred_element_type=F32).astype(BF)
        if go_now:
            xstart(b, n)

    def own_cols(n):
        return pl.ds(pl.multiple_of(n * cw + core * hw, hw), hw)

    def quarter_cols(n, d):
        return pl.ds(pl.multiple_of(n * cw + core * hw + d * (hw // 2), hw // 2), hw // 2)

    def acopy(kind, n):
        if kind == 0:
            src, dst, device = ow.at[:, own_cols(n)], wrel.at[3, :, own_cols(n)], tid(1)
        elif kind == 1:
            src, dst, device = ow.at[:, own_cols(n)], wrel.at[1, :, own_cols(n)], tid(ntp - 1)
        elif kind == 2:
            cols = quarter_cols(n, 0)
            src, dst, device = wrel.at[3, :, cols], wrel.at[2, :, cols], tid(1)
        elif kind == 3:
            cols = quarter_cols(n, 1)
            src, dst, device = wrel.at[1, :, cols], wrel.at[2, :, cols], tid(ntp - 1)
        else:
            cols = own_cols(n)
            block = (3, 1, 2)[kind - 4]
            src, dst, device = wrel.at[block, :, cols], wrel.at[block, :, cols], partner
        return remote(src, dst, ssem.at[ring], arecv.at[(0, 1, 2, 2, 3, 3, 3)[kind], n], device)

    def tcopy(offset):
        rows = pl.ds(pl.multiple_of(lax.rem(tp + offset, ntp) * tok, tok), tok)
        return remote(mixed.at[rows, :], mixrel.at[ntp - offset], ssem.at[rows_t], trecv.at[0], tid(offset))

    def gcopy(offset):
        return remote(gainsrc, gainrel.at[ntp - offset], ssem.at[gains_t], trecv.at[1], tid(offset))

    def hcopy(i):
        src = (gi_hbm, ci_hbm)[i]
        return remote(src.at[seq - 16 : seq, :], halo.at[i], ssem.at[halo_t], trecv.at[2], after)

    def pass_on(n):
        acopy(0, n).wait_recv()
        acopy(2, n).start()
        acopy(4, n).start()
        acopy(1, n).wait_recv()
        acopy(3, n).start()
        acopy(5, n).start()

    for i in (0, 1):
        hcopy(i).start()
    for d in (0, 1):
        mcopy(0, d).start()
    with jax.named_scope("inputs"):
        icopies[0].wait()
    for kind in (0, 1):
        acopy(kind, 0).start()
    with jax.named_scope("rin"):
        icopies[1].wait()
    for n in range(NC - 1):
        for d in (0, 1):
            zcopy(0, d, n).start()
    mgain[...] = jnp.broadcast_to(mgain_ref[...].astype(F32)[None, :], mgain.shape)
    gainsrc[...] = jnp.broadcast_to(gain_ref[...].astype(F32)[None, :], gainsrc.shape)
    for offset in range(1, ntp):
        gcopy(offset).start()
    for i in (2, 3, 4):
        icopies[i].wait()
    for copy in wcopies:
        copy.start()
    taps = taps_ref[...].astype(F32)
    kw = taps_ref.shape[0]
    with jax.named_scope("conv"):
        inner[8 : 8 + seq, :] = gi[...].astype(F32) * ci[...].astype(F32)

        def mix(first, rows):
            filtered = taps[0:1, :] * inner[9 - kw + first : 9 - kw + first + rows, :]
            for k in range(1, kw):
                filtered = filtered + taps[k : k + 1, :] * inner[9 - kw + k + first : 9 - kw + k + first + rows, :]
            mixed[first : first + rows, :] = (go[first : first + rows, :].astype(F32) * filtered).astype(BF)

        mix(tok, seq - tok)
    for offset in range(1, ntp):
        pl.when(lax.rem(tp + offset, ntp) != 0)(tcopy(offset).start)
    with jax.named_scope("pass0"):
        pass_on(0)
    with jax.named_scope("halo"):
        wait_bytes(halo, trecv.at[2])
    earlier = halo[0, 8:16, :].astype(F32) * halo[1, 8:16, :].astype(F32)
    inner[0:8, :] = jnp.where(sp > 0, earlier, 0.0)
    mix(0, tok)
    for offset in range(1, ntp):
        pl.when(lax.rem(tp + offset, ntp) == 0)(tcopy(offset).start)
    mixrel[0] = mixed[pl.ds(pl.multiple_of(tp * tok, tok), tok), :]

    with jax.named_scope("rows"):
        wait_bytes(mixrel.at[1:ntp], trecv.at[0])
        wait_bytes(gainrel.at[1:ntp], trecv.at[1])
    gainrel[0] = gainsrc[...]
    for n in (1, 2):
        for kind in (0, 1):
            acopy(kind, n).start()
    with jax.named_scope("norm"):
        square = jnp.zeros((tok, 1), F32)
        for o in range(ntp):
            part = mixrel[o].astype(F32)
            square = square + jnp.sum(part * part, axis=1, keepdims=True)
        factor = lax.rsqrt(square / (chan * ntp) + EPSILON)
        for o in range(ntp):
            normed[o] = (mixrel[o].astype(F32) * factor * gainrel[o, 0:1, :]).astype(BF)

    def ncopy(d):
        return remote(normed, normed_near.at[d], ssem.at[normed_z], nrecv.at[d], zid(step[d]))

    for d in (0, 1):
        ncopy(d).start()
    for d in (0, 1):
        zcopy(0, d, NC - 1).start()

    def selections():
        sel[0] = select(0, z)
        for d in (0, 1):
            mcopy(0, d).wait_recv()
            mcopy(1, d).start()
            sel[1 + d] = select(near[d], z)

    def far_selections():
        for d in (0, 1):
            mcopy(1, d).wait_recv()
            sel[3 + d] = select(far[d], z)
            sel3[d] = select(far[d], zval(step[d]))
            sel4[d] = select(far[d], zval(2 * step[d]))

    def project(values, rows, n):
        cols = cols_of(n)
        total = values[:, cols].astype(F32) + jnp.dot(rows[0], ow[:, cols], preferred_element_type=F32)
        for o in range(1, ntp):
            total = total + jnp.dot(rows[o], wrel[o, :, cols], preferred_element_type=F32)
        return total.astype(BF)

    for n in range(NC):
        with jax.named_scope(f"ring{n}"):
            wait_bytes(wrel.at[2, :, 0:hw], arecv.at[2, n])
            acopy(6, n).start()
            wait_bytes(wrel.at[1:4, :, 0:hw], arecv.at[3, n])
        with jax.named_scope(f"proj{n}"):
            res_ref[:, cols_of(n)] = project(rin, normed, n)
        if n == 0:
            with jax.named_scope("selections"):
                selections()
        with jax.named_scope(f"own{n}"):
            pack(0, res_ref, n)
        for later in ((1, 2), (3,), (), ())[n]:
            with jax.named_scope(f"pass{later}"):
                pass_on(later)
            if later == 1:
                for kind in (0, 1):
                    acopy(kind, 3).start()

    def expert_in(first, count, n, fresh):
        rows = count * grp
        base = first * grp
        cols = pl.ds(pl.multiple_of(n * cw, cw), cw)
        vals = arrived[base : base + rows, cols].astype(F32)
        x = (vals * mgain[0:1, cols]).astype(BF)
        parts = jnp.sum(vals * vals, axis=1, keepdims=True)
        g = jnp.dot(x, wg[cols, :], preferred_element_type=F32)
        u = jnp.dot(x, wu[cols, :], preferred_element_type=F32)
        if fresh:
            squares[0:rows, :] = jnp.broadcast_to(parts, (rows, 128))
            gate[0:rows, :] = g
            value[0:rows, :] = u
        else:
            squares[0:rows, :] += jnp.broadcast_to(parts, (rows, 128))
            gate[0:rows, :] += g
            value[0:rows, :] += u

    def expert_mid(count):
        rows = count * grp
        factor = lax.rsqrt(squares[0:rows, 0:1] / width + EPSILON)
        g = gate[0:rows, :] * factor
        hid[0:rows, :] = (g * jax.nn.sigmoid(g) * (value[0:rows, :] * factor)).astype(BF)

    def expert_out(first, count, n):
        rows = count * grp
        cols = pl.ds(pl.multiple_of(n * cw, cw), cw)
        r = jnp.dot(hid[0:rows, :], wd[:, cols], preferred_element_type=F32)
        results[first * grp : first * grp + rows, cols] = r.astype(BF)

    def experts(first, count):
        expert_in(first, count, 0, True)

        def more(n, carry):
            expert_in(first, count, n, False)
            return carry

        lax.fori_loop(1, NC, more, 0)
        expert_mid(count)

        def out_cols(n, carry):
            expert_out(first, count, n)
            return carry

        lax.fori_loop(0, NC, out_cols, 0)

    with jax.named_scope("normed"):
        for d in (0, 1):
            ncopy(d).wait_recv()
    for n, d in both:
        with jax.named_scope(f"hop1_{n}{d}"):
            zcopy(0, d, n).wait_recv()
        hop1[d, :, cols_of(n)] = project(hop1.at[d], normed_near.at[d], n)
        zcopy(1, d, n).start()
        pack(1 + d, hop1.at[d], n)
    with jax.named_scope("far_selections"):
        far_selections()
    for copy in wcopies:
        copy.wait()
    xwait(0)
    with jax.named_scope("exp0"):
        experts(0, 1)

    def hop3_out(n):
        for d in (0, 1):
            with jax.named_scope(f"ex{n}{d}"):
                wait_bytes(gather3.at[d, 0:others, 0 : cw + hw], grecv.at[d, n])
            zcopy(3, d, n).start()
            zcopy(2, d, n).start()

    for n in range(NC):
        for d in (0, 1):
            with jax.named_scope(f"hop2_{n}{d}"):
                zcopy(1, d, n).wait_recv()
            part = hop2[d, :, cols_of(n)]
            pack3[d, :, cols_of(n)] = jnp.dot(sel3[d], part, preferred_element_type=F32).astype(BF)
            part = hop2[d, :, part_of(n, d)]
            pack4[d, :, half_of(n)] = jnp.dot(sel4[d], part, preferred_element_type=F32).astype(BF)
            exchange(pack4, gather4, d, half_of(n), ssem.at[gs], grecv.at[d, n])
            exchange(pack3, gather3, d, cols_of(n), ssem.at[gs], grecv.at[d, n])
            pack(3 + d, hop2.at[d], n, False)
        if n > 0:
            hop3_out(n - 1)
            if n < 3:
                xstart(3, n - 1)
                xstart(4, n - 1)
        if n == 1:
            xwait(1)
            xwait(2)
            with jax.named_scope("exp12"):
                experts(1, 2)
    hop3_out(NC - 1)
    for n in (2, 3):
        xstart(3, n)
        xstart(4, n)

    def rcopy(kind, d, n):
        cols = cols_of(n)
        if kind == 0:
            src, dst = results.at[block_rows(7), part_of(n, d)], back4.at[d, :, half_of(n)]
        elif kind == 1:
            src, dst = results.at[block_rows(5 + d), cols], got3.at[d, :, cols]
        elif kind == 2:
            src, dst = back4.at[d, :, half_of(n)], got4.at[d, :, half_of(n)]
        elif kind == 3:
            src, dst = send2.at[d, :, cols], part2.at[d, :, cols]
        else:
            src, dst = send1.at[d, :, cols], part1.at[d, :, cols]
        return remote(src, dst, ssem.at[back_near if kind > 2 else back_far], rrecv.at[kind, d, n], zid(-step[d]))

    for n in range(NC):
        for d in (0, 1):
            with jax.named_scope(f"hop3_{n}{d}"):
                zcopy(3, d, n).wait_recv()
            zcopy(4, d, n).start()
        if n == NC - 1:
            ystart(1)
        with jax.named_scope(f"hop3w{n}"):
            for d in (0, 1):
                zcopy(2, d, n).wait_recv()
        with jax.named_scope(f"in56_{n}"):
            expert_in(5, 2, n, n == 0)
    with jax.named_scope("out56"):
        expert_mid(2)
        for n in range(NC):
            expert_out(5, 2, n)
            if n < 2:
                for d in (0, 1):
                    rcopy(1, d, n).start()
    with jax.named_scope("xw34"):
        xwait(3)
        xwait(4)
    with jax.named_scope("exp34"):
        experts(3, 2)
    ystart(3)
    ystart(4)
    for n in range(NC):
        with jax.named_scope(f"hop4w{n}"):
            for d in (0, 1):
                zcopy(4, d, n).wait_recv()
        with jax.named_scope(f"in7_{n}"):
            expert_in(7, 1, n, n == 0)
    with jax.named_scope("out7"):
        expert_mid(1)
        for n in range(NC):
            expert_out(7, 1, n)
            for d in (0, 1):
                rcopy(0, d, n).start()
    def slots3_in(n):
        for d in (0, 1):
            with jax.named_scope(f"r3_{n}{d}"):
                rcopy(1, d, n).wait_recv()
            exchange(got3, ret3, d, cols_of(n), ssem.at[bs], brecv.at[d, n])

    slots3_in(0)
    slots3_in(1)
    for n, d in both:
        with jax.named_scope(f"r4_{n}{d}"):
            rcopy(0, d, n).wait_recv()
        rcopy(2, d, n).start()
        if n < 2:
            rcopy(1, d, n + 2).start()

    def sums2_out(n):
        if n % 2 == 0:
            ywait(3, n // 2)
            ywait(4, n // 2)
        for d in (0, 1):
            with jax.named_scope(f"ex{n}{d}"):
                wait_bytes(ret3.at[d, 0:others, 0 : cw + hw], brecv.at[d, n])
            total = combine(spread(far[d], z), ret2[d, :, cols_of(n)])
            total = total + combine(spread(far[d], zval(step[d])), ret3[d, :, cols_of(n)])
            last = combine(spread(far[d], zval(2 * step[d])), ret4[d, :, half_of(n)])
            lo, hi = total[:, :hw], total[:, hw:]
            if d == 0:
                lo = lo + last
            else:
                hi = hi + last
            send2[d, :, part_of(n, 0)] = lo.astype(BF)
            send2[d, :, part_of(n, 1)] = hi.astype(BF)
            rcopy(3, d, n).start()

    def slots4_in(n):
        for d in (0, 1):
            with jax.named_scope(f"r3b_{n}{d}"):
                rcopy(2, d, n).wait_recv()
            exchange(got4, ret4, d, half_of(n), ssem.at[bs], brecv.at[d, n])

    slots4_in(0)
    slots3_in(2)
    slots4_in(1)
    ystart(3, 1)
    ystart(4, 1)
    sums2_out(0)
    slots3_in(3)
    slots4_in(2)
    sums2_out(1)
    slots4_in(3)
    sums2_out(2)
    sums2_out(3)
    ystart(2)
    with jax.named_scope("yw12"):
        ywait(1)
        ywait(2)
    ystart(0)
    for n, d in both:
        with jax.named_scope(f"r2_{n}{d}"):
            rcopy(3, d, n).wait_recv()
        cols = cols_of(n)
        total = part2[d, :, cols].astype(F32) + combine(spread(near[d], z), ret1[d, :, cols])
        send1[d, :, cols] = total.astype(BF)
        rcopy(4, d, n).start()
    ywait(0)
    own = spread(0, z)
    ocopies = []
    for n in range(NC):
        with jax.named_scope(f"r1_{n}"):
            rcopy(4, 0, n).wait_recv()
            rcopy(4, 1, n).wait_recv()
        cols = cols_of(n)
        total = res_ref[:, cols].astype(F32) + combine(own, ret0[:, cols])
        total = total + part1[0, :, cols].astype(F32) + part1[1, :, cols].astype(F32)
        out[:, cols] = total.astype(BF)
        copy = pltpu.make_async_copy(out.at[:, cols], out_ref.at[:, cols], osem.at[n])
        copy.start()
        ocopies.append(copy)
    with jax.named_scope("ends"):
        for copy in ocopies:
            copy.wait()
        flat = ((near_z, 4 * tok), (far_z, 4 * grp), (back_near, 4 * tok), (back_far, 4 * grp), (xs, 5 * others), (ys, 5 * others))
        flat += ((gs, 3 * others), (bs, 3 * others), (ring, 3 * chan), (rows_t, 3 * tok * chan // width), (normed_z, 2 * ntp * tok * chan // width))
        for kind, rows in flat:
            wait_bytes(arrived.at[0:rows, :], ssem.at[kind])
        wait_bytes(gainrel.at[1:ntp], ssem.at[gains_t])
        wait_bytes(halo, ssem.at[halo_t])
        wait_bytes(metas.at[0:4], ssem.at[metas_z])


def body(
    residual_in,
    gate_outer,
    gate_inner,
    conv_input,
    conv_taps,
    norm_gain,
    out_weight,
    moe_gain,
    expert_ids,
    group_prob,
    route_prob,
    expert_gate,
    expert_up,
    expert_down,
):
    tok, width = residual_in.shape
    seq, chan = conv_input.shape
    fe = expert_gate.shape[2]
    ntp = lax.axis_size("tp")
    nj = lax.axis_size("sp") // NZ
    grp = nj * CAP
    vmem = pl.BlockSpec(memory_space=pltpu.VMEM)
    hbm = pl.BlockSpec(memory_space=pl.ANY)
    dma = pltpu.SemaphoreType.DMA
    shapes = [
        ((tok, width), BF),
        ((seq, chan), BF),
        ((seq, chan), BF),
        ((seq, chan), BF),
        ((chan, width), BF),
        ((2, 16, chan), BF),
        ((seq + 8, chan), F32),
        ((seq, chan), BF),
        ((ntp, tok, chan), BF),
        ((8, chan), F32),
        ((ntp, 8, chan), F32),
        ((ntp, tok, chan), BF),
        ((2, ntp, tok, chan), BF),
        ((ntp, chan, width), BF),
        ((tok, width), BF),
        ((8, tok), F32),
        ((2 * grp, 128), F32),
        ((2 * grp, fe), F32),
        ((2 * grp, fe), F32),
        ((8, width), F32),
        ((tok, width), BF),
        ((5, grp, tok), BF),
        ((NZ, 8, tok), F32),
        ((2, tok, width), BF),
        ((2, tok, width), BF),
        ((2, grp, tok), BF),
        ((2, grp, tok), BF),
        ((2, grp, width), BF),
        ((2, grp, width // 2), BF),
        ((2, grp, width), BF),
        ((2, grp, width // 2), BF),
        ((2, grp, width // 2), BF),
        ((5, grp, width), BF),
        ((8 * grp, width), BF),
        ((8 * grp, width), BF),
        ((grp, width), BF),
        ((2, grp, width), BF),
        ((2, grp, width), BF),
        ((2, grp, width), BF),
        ((2, grp, width // 2), BF),
        ((2, grp, width // 2), BF),
        ((2, grp, width), BF),
        ((2, grp, width // 2), BF),
        ((2, tok, width), BF),
        ((2, tok, width), BF),
        ((2, tok, width), BF),
        ((2, tok, width), BF),
        ((2 * grp, fe), BF),
        ((width, fe), BF),
        ((width, fe), BF),
        ((fe, width), BF),
    ]
    sems = [(5,), (NC,), (3,), (14,), (3,), (4, NC), (2,), (2, 2), (5, 2, NC), (5,), (7,), (2, NC), (2, NC), (5, 2, NC)]
    return pl.pallas_call(
        layer_kernel,
        out_shape=jax.ShapeDtypeStruct((tok, width), BF),
        in_specs=[hbm] * 8 + [vmem] * 6,
        out_specs=hbm,
        scratch_shapes=[pltpu.VMEM(s, t) for s, t in shapes] + [dma(s) for s in sems],
        compiler_params=pltpu.CompilerParams(
            collective_id=0, has_side_effects=True, vmem_limit_bytes=61 * 1024 * 1024
        ),
        name="layer",
    )(
        residual_in,
        gate_outer,
        gate_inner,
        conv_input,
        out_weight,
        expert_gate,
        expert_up,
        expert_down,
        conv_taps,
        norm_gain,
        moe_gain,
        expert_ids.T,
        group_prob.reshape(1, tok),
        route_prob.T,
    )


def solution(mesh):
    in_specs = (
        P(("sp", "tp"), None),
        P("sp", "tp"),
        P("sp", "tp"),
        P("sp", "tp"),
        P(None, "tp"),
        P("tp"),
        P("tp", None),
        P(),
        P(("sp", "tp"), None),
        P(("sp", "tp")),
        P(("sp", "tp"), None),
        P("sp", None, None),
        P("sp", None, None),
        P("sp", None, None),
    )
    out_specs = P(("sp", "tp"), None)
    return jax.shard_map(body, mesh=mesh, in_specs=in_specs, out_specs=out_specs, check_vma=False)
```

```python
import jax
import jax.numpy as jnp
from jax import lax
from jax.experimental import pallas as pl
from jax.experimental.pallas import tpu as pltpu
from jax.sharding import PartitionSpec as P

EPSILON = 1e-06
NZ = 8
CAP = 16
NC = 4
MESH = pl.DeviceIdType.MESH
BF = jnp.bfloat16
F32 = jnp.float32


def layer_kernel(
    rin_hbm,
    go_hbm,
    gi_hbm,
    ci_hbm,
    ow_hbm,
    wg_hbm,
    wu_hbm,
    wd_hbm,
    taps_ref,
    gain_ref,
    mgain_ref,
    ids_ref,
    group_ref,
    route_ref,
    out_ref,
    rin,
    go,
    gi,
    ci,
    ow,
    halo,
    inner,
    mixed,
    mixrel,
    gainsrc,
    gainrel,
    normed,
    normed_near,
    wrel,
    res_ref,
    meta_ref,
    squares,
    gate,
    value,
    mgain,
    sel,
    metas,
    hop1,
    hop2,
    sel3,
    sel4,
    pack3,
    pack4,
    gather3,
    gather4,
    pass4,
    packed,
    arrived,
    results,
    ret0,
    ret1,
    ret2,
    got3,
    back4,
    got4,
    ret3,
    ret4,
    send2,
    part2,
    send1,
    part1,
    hid,
    wg,
    wu,
    wd,
    isem,
    wsem,
    ssem,
    trecv,
    arecv,
    nrecv,
    mrecv,
    zrecv,
    xrecv,
    yrecv,
    grecv,
    brecv,
    rrecv,
):
    tok, width = res_ref.shape
    nsp = lax.axis_size("sp")
    ntp = lax.axis_size("tp")
    nj = nsp // NZ
    grp = nj * CAP
    seq, chan = mixed.shape
    others = grp - CAP
    cw = width // NC
    hw = cw // 2
    sp = lax.axis_index("sp")
    tp = lax.axis_index("tp")
    z = sp // nj
    me_j = sp % nj
    step = (1, -1)
    near = (1, NZ - 1)
    far = (2, NZ - 2)
    both = [(n, d) for n in range(NC) for d in (0, 1)]

    def zval(offset):
        return lax.rem(z + offset + NZ, NZ)

    def zid(offset):
        return (zval(offset) * nj + me_j, tp)

    def jid(offset):
        return (z * nj + lax.rem(me_j + offset, nj), tp)

    def tid(offset):
        return (sp, lax.rem(tp + offset, ntp))

    after = (lax.rem(sp + 1, nsp), tp)
    before = (lax.rem(sp + nsp - 1, nsp), tp)
    core = lax.rem(me_j, 2)
    partner = (z * nj + me_j + 1 - 2 * core, tp)

    def cols_of(n):
        return slice(n * cw, (n + 1) * cw)

    def half_of(n):
        return slice(n * hw, (n + 1) * hw)

    def part_of(n, d):
        return slice(n * cw + d * hw, n * cw + (d + 1) * hw)

    def slot_rows(b, j):
        return pl.ds(pl.multiple_of(b * grp + j * CAP, CAP), CAP)

    def block_rows(b):
        return slice(b * grp, (b + 1) * grp)

    near_z, far_z, back_near, back_far, xs, ys, gs, bs, ring, rows_t, gains_t, halo_t, metas_z, normed_z = range(14)

    def remote(src, dst, send, recv, device):
        return pltpu.make_async_remote_copy(
            src_ref=src, dst_ref=dst, send_sem=send, recv_sem=recv, device_id=device, device_id_type=MESH
        )

    def wait_bytes(ref, sem):
        pltpu.make_async_copy(ref, ref, sem).wait()

    def make_slots():
        expert = lax.broadcasted_iota(jnp.int32, (nsp, tok), 0)
        hot = [jnp.where(expert == ids_ref[k : k + 1, :], 1.0, 0.0) for k in (0, 1)]
        earlier_tok = lax.broadcasted_iota(jnp.int32, (tok, tok), 0) < lax.broadcasted_iota(jnp.int32, (tok, tok), 1)
        upper = jnp.where(earlier_tok, 1.0, 0.0).astype(BF)
        rank = [jnp.dot(h.astype(BF), upper, preferred_element_type=F32) for h in hot]
        count = jnp.sum(hot[0], axis=1, keepdims=True)
        slot = expert.astype(F32) * CAP
        meta_ref[0:1, :] = jnp.sum((rank[0] + slot) * hot[0], axis=0, keepdims=True)
        meta_ref[1:2, :] = jnp.sum((rank[1] + count + slot) * hot[1], axis=0, keepdims=True)
        meta_ref[2:3, :] = group_ref[...] * route_ref[0:1, :] / (route_ref[0:1, :] + route_ref[1:2, :])
        meta_ref[3:4, :] = group_ref[...] * route_ref[1:2, :] / (route_ref[0:1, :] + route_ref[1:2, :])
        meta_ref[4:8, :] = jnp.zeros((4, tok), F32)

    icopies = [
        pltpu.make_async_copy(src, dst, isem.at[i])
        for i, (src, dst) in enumerate(((ow_hbm, ow), (rin_hbm, rin), (gi_hbm, gi), (ci_hbm, ci), (go_hbm, go)))
    ]
    wcopies = [
        pltpu.make_async_copy(wg_hbm.at[0], wg, wsem.at[0]),
        pltpu.make_async_copy(wu_hbm.at[0], wu, wsem.at[1]),
        pltpu.make_async_copy(wd_hbm.at[0], wd, wsem.at[2]),
    ]
    barrier = pltpu.get_barrier_semaphore()
    for offset in (1, -1):
        pl.semaphore_signal(barrier, inc=1, device_id=zid(offset), device_id_type=MESH)
    for offset in range(1, nj):
        pl.semaphore_signal(barrier, inc=1, device_id=jid(offset), device_id_type=MESH)
    for offset in range(1, ntp):
        pl.semaphore_signal(barrier, inc=1, device_id=tid(offset), device_id_type=MESH)
    for ident in (after, before):
        pl.semaphore_signal(barrier, inc=1, device_id=ident, device_id_type=MESH)
    for copy in icopies:
        copy.start()
    make_slots()
    with jax.named_scope("barrier"):
        pl.semaphore_wait(barrier, nj + ntp + 2)

    def mcopy(hop, d):
        src = metas.at[near[d]] if hop else meta_ref
        dst = metas.at[far[d] if hop else near[d]]
        return remote(src, dst, ssem.at[metas_z], mrecv.at[hop, d], zid(step[d]))

    def zcopy(hop, d, n):
        cols = cols_of(n)
        if hop == 0:
            src, dst = rin.at[:, cols], hop1.at[d, :, cols]
        elif hop == 1:
            src, dst = hop1.at[d, :, cols], hop2.at[d, :, cols]
        elif hop == 2:
            src, dst = gather3.at[d, :, cols], arrived.at[block_rows(5 + d), cols]
        elif hop == 3:
            src, dst = gather4.at[d, :, half_of(n)], pass4.at[d, :, half_of(n)]
        else:
            src, dst = pass4.at[d, :, half_of(n)], arrived.at[block_rows(7), part_of(n, d)]
        return remote(src, dst, ssem.at[near_z if hop < 2 else far_z], zrecv.at[hop, d, n], zid(step[d]))

    def meta_of(offset):
        return meta_ref if offset == 0 else metas.at[offset]

    def slots_of(target):
        return (lax.broadcasted_iota(jnp.int32, (grp, tok), 0) + target * grp).astype(F32)

    def select(offset, target):
        ref = meta_of(offset)
        slot = slots_of(target)
        hit = jnp.where(slot == ref[0:1, :], 1.0, 0.0) + jnp.where(slot == ref[1:2, :], 1.0, 0.0)
        return hit.astype(BF)

    def spread(offset, target):
        ref = meta_of(offset)
        slot = slots_of(target)
        hit = jnp.where(slot == ref[0:1, :], ref[2:3, :], 0.0) + jnp.where(slot == ref[1:2, :], ref[3:4, :], 0.0)
        return hit.astype(BF)

    def combine(weights, rows):
        return lax.dot_general(weights, rows, (((0,), (0,)), ((), ())), preferred_element_type=F32)

    def ytarget(b):
        return ret0 if b == 0 else ret1.at[b - 1] if b < 3 else ret2.at[b - 3]

    def xstart(b, n):
        cols = cols_of(n)
        for offset in range(1, nj):
            their = slot_rows(0, lax.rem(me_j + offset, nj))
            src, dst = packed.at[b, their, cols], arrived.at[slot_rows(b, me_j), cols]
            remote(src, dst, ssem.at[xs], xrecv.at[b], jid(offset)).start()
        arrived[slot_rows(b, me_j), cols] = packed[b, slot_rows(0, me_j), cols]

    def xwait(b):
        wait_bytes(arrived.at[b * grp : b * grp + others, :], xrecv.at[b])

    def ypart(b, part):
        return (slice(0, width), b) if b < 3 else (slice(part * (width // 2), (part + 1) * (width // 2)), 3 + 2 * (b - 3) + part)

    def ystart(b, part=0):
        dst = ytarget(b)
        cols, index = ypart(b, part)
        for offset in range(1, nj):
            their = slot_rows(b, lax.rem(me_j + offset, nj))
            src = results.at[their, cols]
            remote(src, dst.at[slot_rows(0, me_j), cols], ssem.at[ys], yrecv.at[index], jid(offset)).start()
        dst[slot_rows(0, me_j), cols] = results[slot_rows(b, me_j), cols]

    def ywait(b, part=0):
        cols, index = ypart(b, part)
        wait_bytes(ytarget(b).at[0:others, cols], yrecv.at[index])

    def exchange(src, dst, d, cols, send, recv):
        mine = slot_rows(0, me_j)
        for offset in range(1, nj):
            their = slot_rows(0, lax.rem(me_j + offset, nj))
            remote(src.at[d, their, cols], dst.at[d, mine, cols], send, recv, jid(offset)).start()
        dst[d, mine, cols] = src[d, mine, cols]

    def pack(b, block, n, go_now=True):
        cols = cols_of(n)
        packed[b, :, cols] = jnp.dot(sel[b], block[:, cols], preferred_element_type=F32).astype(BF)
        if go_now:
            xstart(b, n)

    def own_cols(n):
        return pl.ds(pl.multiple_of(n * cw + core * hw, hw), hw)

    def quarter_cols(n, d):
        return pl.ds(pl.multiple_of(n * cw + core * hw + d * (hw // 2), hw // 2), hw // 2)

    def acopy(kind, n):
        if kind == 0:
            src, dst, device = ow.at[:, own_cols(n)], wrel.at[3, :, own_cols(n)], tid(1)
        elif kind == 1:
            src, dst, device = ow.at[:, own_cols(n)], wrel.at[1, :, own_cols(n)], tid(ntp - 1)
        elif kind == 2:
            cols = quarter_cols(n, 0)
            src, dst, device = wrel.at[3, :, cols], wrel.at[2, :, cols], tid(1)
        elif kind == 3:
            cols = quarter_cols(n, 1)
            src, dst, device = wrel.at[1, :, cols], wrel.at[2, :, cols], tid(ntp - 1)
        else:
            cols = own_cols(n)
            block = (3, 1, 2)[kind - 4]
            src, dst, device = wrel.at[block, :, cols], wrel.at[block, :, cols], partner
        return remote(src, dst, ssem.at[ring], arecv.at[(0, 1, 2, 2, 3, 3, 3)[kind], n], device)

    def tcopy(offset):
        rows = pl.ds(pl.multiple_of(lax.rem(tp + offset, ntp) * tok, tok), tok)
        return remote(mixed.at[rows, :], mixrel.at[ntp - offset], ssem.at[rows_t], trecv.at[0], tid(offset))

    def gcopy(offset):
        return remote(gainsrc, gainrel.at[ntp - offset], ssem.at[gains_t], trecv.at[1], tid(offset))

    def hcopy(i):
        src = (gi_hbm, ci_hbm)[i]
        return remote(src.at[seq - 16 : seq, :], halo.at[i], ssem.at[halo_t], trecv.at[2], after)

    def pass_on(n):
        acopy(0, n).wait_recv()
        acopy(2, n).start()
        acopy(4, n).start()
        acopy(1, n).wait_recv()
        acopy(3, n).start()
        acopy(5, n).start()

    for i in (0, 1):
        hcopy(i).start()
    for d in (0, 1):
        mcopy(0, d).start()
    with jax.named_scope("inputs"):
        icopies[0].wait()
    for kind in (0, 1):
        acopy(kind, 0).start()
    with jax.named_scope("rin"):
        icopies[1].wait()
    for n in range(NC - 1):
        for d in (0, 1):
            zcopy(0, d, n).start()
    mgain[...] = jnp.broadcast_to(mgain_ref[...].astype(F32)[None, :], mgain.shape)
    gainsrc[...] = jnp.broadcast_to(gain_ref[...].astype(F32)[None, :], gainsrc.shape)
    for offset in range(1, ntp):
        gcopy(offset).start()
    for i in (2, 3, 4):
        icopies[i].wait()
    for copy in wcopies:
        copy.start()
    taps = taps_ref[...].astype(F32)
    kw = taps_ref.shape[0]
    with jax.named_scope("conv"):
        inner[8 : 8 + seq, :] = gi[...].astype(F32) * ci[...].astype(F32)

        def mix(first, rows):
            filtered = taps[0:1, :] * inner[9 - kw + first : 9 - kw + first + rows, :]
            for k in range(1, kw):
                filtered = filtered + taps[k : k + 1, :] * inner[9 - kw + k + first : 9 - kw + k + first + rows, :]
            mixed[first : first + rows, :] = (go[first : first + rows, :].astype(F32) * filtered).astype(BF)

        mix(tok, seq - tok)
    for offset in range(1, ntp):
        pl.when(lax.rem(tp + offset, ntp) != 0)(tcopy(offset).start)
    with jax.named_scope("pass0"):
        pass_on(0)
    with jax.named_scope("halo"):
        wait_bytes(halo, trecv.at[2])
    earlier = halo[0, 8:16, :].astype(F32) * halo[1, 8:16, :].astype(F32)
    inner[0:8, :] = jnp.where(sp > 0, earlier, 0.0)
    mix(0, tok)
    for offset in range(1, ntp):
        pl.when(lax.rem(tp + offset, ntp) == 0)(tcopy(offset).start)
    mixrel[0] = mixed[pl.ds(pl.multiple_of(tp * tok, tok), tok), :]

    with jax.named_scope("rows"):
        wait_bytes(mixrel.at[1:ntp], trecv.at[0])
        wait_bytes(gainrel.at[1:ntp], trecv.at[1])
    gainrel[0] = gainsrc[...]
    for n in (1, 2):
        for kind in (0, 1):
            acopy(kind, n).start()
    with jax.named_scope("norm"):
        square = jnp.zeros((tok, 1), F32)
        for o in range(ntp):
            part = mixrel[o].astype(F32)
            square = square + jnp.sum(part * part, axis=1, keepdims=True)
        factor = lax.rsqrt(square / (chan * ntp) + EPSILON)
        for o in range(ntp):
            normed[o] = (mixrel[o].astype(F32) * factor * gainrel[o, 0:1, :]).astype(BF)

    def ncopy(d):
        return remote(normed, normed_near.at[d], ssem.at[normed_z], nrecv.at[d], zid(step[d]))

    for d in (0, 1):
        ncopy(d).start()
    for d in (0, 1):
        zcopy(0, d, NC - 1).start()

    def selections():
        sel[0] = select(0, z)
        for d in (0, 1):
            mcopy(0, d).wait_recv()
            mcopy(1, d).start()
            sel[1 + d] = select(near[d], z)

    def far_selections():
        for d in (0, 1):
            mcopy(1, d).wait_recv()
            sel[3 + d] = select(far[d], z)
            sel3[d] = select(far[d], zval(step[d]))
            sel4[d] = select(far[d], zval(2 * step[d]))

    def project(values, rows, n):
        cols = cols_of(n)
        total = values[:, cols].astype(F32) + jnp.dot(rows[0], ow[:, cols], preferred_element_type=F32)
        for o in range(1, ntp):
            total = total + jnp.dot(rows[o], wrel[o, :, cols], preferred_element_type=F32)
        return total.astype(BF)

    for n in range(NC):
        with jax.named_scope(f"ring{n}"):
            wait_bytes(wrel.at[2, :, 0:hw], arecv.at[2, n])
            acopy(6, n).start()
            wait_bytes(wrel.at[1:4, :, 0:hw], arecv.at[3, n])
        with jax.named_scope(f"proj{n}"):
            res_ref[:, cols_of(n)] = project(rin, normed, n)
        if n == 0:
            with jax.named_scope("selections"):
                selections()
        with jax.named_scope(f"own{n}"):
            pack(0, res_ref, n)
        for later in ((1, 2), (3,), (), ())[n]:
            with jax.named_scope(f"pass{later}"):
                pass_on(later)
            if later == 1:
                for kind in (0, 1):
                    acopy(kind, 3).start()

    def expert_in(first, count, n, fresh):
        rows = count * grp
        base = first * grp
        cols = pl.ds(pl.multiple_of(n * cw, cw), cw)
        vals = arrived[base : base + rows, cols].astype(F32)
        x = (vals * mgain[0:1, cols]).astype(BF)
        parts = jnp.sum(vals * vals, axis=1, keepdims=True)
        g = jnp.dot(x, wg[cols, :], preferred_element_type=F32)
        u = jnp.dot(x, wu[cols, :], preferred_element_type=F32)
        if fresh:
            squares[0:rows, :] = jnp.broadcast_to(parts, (rows, 128))
            gate[0:rows, :] = g
            value[0:rows, :] = u
        else:
            squares[0:rows, :] += jnp.broadcast_to(parts, (rows, 128))
            gate[0:rows, :] += g
            value[0:rows, :] += u

    def expert_mid(count):
        rows = count * grp
        factor = lax.rsqrt(squares[0:rows, 0:1] / width + EPSILON)
        g = gate[0:rows, :] * factor
        hid[0:rows, :] = (g * jax.nn.sigmoid(g) * (value[0:rows, :] * factor)).astype(BF)

    def expert_out(first, count, n):
        rows = count * grp
        cols = pl.ds(pl.multiple_of(n * cw, cw), cw)
        r = jnp.dot(hid[0:rows, :], wd[:, cols], preferred_element_type=F32)
        results[first * grp : first * grp + rows, cols] = r.astype(BF)

    def experts(first, count):
        expert_in(first, count, 0, True)

        def more(n, carry):
            expert_in(first, count, n, False)
            return carry

        lax.fori_loop(1, NC, more, 0)
        expert_mid(count)

        def out_cols(n, carry):
            expert_out(first, count, n)
            return carry

        lax.fori_loop(0, NC, out_cols, 0)

    with jax.named_scope("normed"):
        for d in (0, 1):
            ncopy(d).wait_recv()
    for n, d in both:
        with jax.named_scope(f"hop1_{n}{d}"):
            zcopy(0, d, n).wait_recv()
        hop1[d, :, cols_of(n)] = project(hop1.at[d], normed_near.at[d], n)
        zcopy(1, d, n).start()
        pack(1 + d, hop1.at[d], n)
    with jax.named_scope("far_selections"):
        far_selections()
    for copy in wcopies:
        copy.wait()
    xwait(0)
    with jax.named_scope("exp0"):
        experts(0, 1)

    def hop3_out(n):
        for d in (0, 1):
            with jax.named_scope(f"ex{n}{d}"):
                wait_bytes(gather3.at[d, 0:others, 0 : cw + hw], grecv.at[d, n])
            zcopy(3, d, n).start()
            zcopy(2, d, n).start()

    for n in range(NC):
        for d in (0, 1):
            with jax.named_scope(f"hop2_{n}{d}"):
                zcopy(1, d, n).wait_recv()
            part = hop2[d, :, cols_of(n)]
            pack3[d, :, cols_of(n)] = jnp.dot(sel3[d], part, preferred_element_type=F32).astype(BF)
            part = hop2[d, :, part_of(n, d)]
            pack4[d, :, half_of(n)] = jnp.dot(sel4[d], part, preferred_element_type=F32).astype(BF)
            exchange(pack4, gather4, d, half_of(n), ssem.at[gs], grecv.at[d, n])
            exchange(pack3, gather3, d, cols_of(n), ssem.at[gs], grecv.at[d, n])
            pack(3 + d, hop2.at[d], n, False)
        if n > 0:
            hop3_out(n - 1)
            if n < 3:
                xstart(3, n - 1)
                xstart(4, n - 1)
        if n == 1:
            xwait(1)
            xwait(2)
            with jax.named_scope("exp12"):
                experts(1, 2)
    hop3_out(NC - 1)
    for n in (2, 3):
        xstart(3, n)
        xstart(4, n)

    def rcopy(kind, d, n):
        cols = cols_of(n)
        if kind == 0:
            src, dst = results.at[block_rows(7), part_of(n, d)], back4.at[d, :, half_of(n)]
        elif kind == 1:
            src, dst = results.at[block_rows(5 + d), cols], got3.at[d, :, cols]
        elif kind == 2:
            src, dst = back4.at[d, :, half_of(n)], got4.at[d, :, half_of(n)]
        elif kind == 3:
            src, dst = send2.at[d, :, cols], part2.at[d, :, cols]
        else:
            src, dst = send1.at[d, :, cols], part1.at[d, :, cols]
        return remote(src, dst, ssem.at[back_near if kind > 2 else back_far], rrecv.at[kind, d, n], zid(-step[d]))

    for n in range(NC):
        for d in (0, 1):
            with jax.named_scope(f"hop3_{n}{d}"):
                zcopy(3, d, n).wait_recv()
            zcopy(4, d, n).start()
        if n == NC - 1:
            ystart(1)
        with jax.named_scope(f"hop3w{n}"):
            for d in (0, 1):
                zcopy(2, d, n).wait_recv()
        with jax.named_scope(f"in56_{n}"):
            expert_in(5, 2, n, n == 0)
    with jax.named_scope("out56"):
        expert_mid(2)
        for n in range(NC):
            expert_out(5, 2, n)
            if n < 2:
                for d in (0, 1):
                    rcopy(1, d, n).start()
    with jax.named_scope("xw34"):
        xwait(3)
        xwait(4)
    with jax.named_scope("exp34"):
        experts(3, 2)
    ystart(3)
    ystart(4)
    for n in range(NC):
        with jax.named_scope(f"hop4w{n}"):
            for d in (0, 1):
                zcopy(4, d, n).wait_recv()
        with jax.named_scope(f"in7_{n}"):
            expert_in(7, 1, n, n == 0)
    with jax.named_scope("out7"):
        expert_mid(1)
        for n in range(NC):
            expert_out(7, 1, n)
            for d in (0, 1):
                rcopy(0, d, n).start()
    def slots3_in(n):
        for d in (0, 1):
            with jax.named_scope(f"r3_{n}{d}"):
                rcopy(1, d, n).wait_recv()
            exchange(got3, ret3, d, cols_of(n), ssem.at[bs], brecv.at[d, n])

    slots3_in(0)
    slots3_in(1)
    for n, d in both:
        with jax.named_scope(f"r4_{n}{d}"):
            rcopy(0, d, n).wait_recv()
        rcopy(2, d, n).start()
        if n < 2:
            rcopy(1, d, n + 2).start()

    def sums2_out(n):
        if n % 2 == 0:
            ywait(3, n // 2)
            ywait(4, n // 2)
        for d in (0, 1):
            with jax.named_scope(f"ex{n}{d}"):
                wait_bytes(ret3.at[d, 0:others, 0 : cw + hw], brecv.at[d, n])
            total = combine(spread(far[d], z), ret2[d, :, cols_of(n)])
            total = total + combine(spread(far[d], zval(step[d])), ret3[d, :, cols_of(n)])
            last = combine(spread(far[d], zval(2 * step[d])), ret4[d, :, half_of(n)])
            lo, hi = total[:, :hw], total[:, hw:]
            if d == 0:
                lo = lo + last
            else:
                hi = hi + last
            send2[d, :, part_of(n, 0)] = lo.astype(BF)
            send2[d, :, part_of(n, 1)] = hi.astype(BF)
            rcopy(3, d, n).start()

    def slots4_in(n):
        for d in (0, 1):
            with jax.named_scope(f"r3b_{n}{d}"):
                rcopy(2, d, n).wait_recv()
            exchange(got4, ret4, d, half_of(n), ssem.at[bs], brecv.at[d, n])

    slots4_in(0)
    ystart(3, 1)
    slots3_in(2)
    slots4_in(1)
    ystart(4, 1)
    sums2_out(0)
    slots3_in(3)
    slots4_in(2)
    sums2_out(1)
    slots4_in(3)
    sums2_out(2)
    ystart(2)
    sums2_out(3)
    with jax.named_scope("yw12"):
        ywait(1)
        ywait(2)
    ystart(0)
    for n, d in both:
        with jax.named_scope(f"r2_{n}{d}"):
            rcopy(3, d, n).wait_recv()
        cols = cols_of(n)
        total = part2[d, :, cols].astype(F32) + combine(spread(near[d], z), ret1[d, :, cols])
        send1[d, :, cols] = total.astype(BF)
        rcopy(4, d, n).start()
    ywait(0)
    own = spread(0, z)
    for n in range(NC):
        with jax.named_scope(f"r1_{n}"):
            rcopy(4, 0, n).wait_recv()
            rcopy(4, 1, n).wait_recv()
        cols = cols_of(n)
        total = res_ref[:, cols].astype(F32) + combine(own, ret0[:, cols])
        total = total + part1[0, :, cols].astype(F32) + part1[1, :, cols].astype(F32)
        out_ref[:, cols] = total.astype(BF)
    with jax.named_scope("ends"):
        flat = ((near_z, 4 * tok), (far_z, 4 * grp), (back_near, 4 * tok), (back_far, 4 * grp), (xs, 5 * others), (ys, 5 * others))
        flat += ((gs, 3 * others), (bs, 3 * others), (ring, 3 * chan), (rows_t, 3 * tok * chan // width), (normed_z, 2 * ntp * tok * chan // width))
        for kind, rows in flat:
            wait_bytes(arrived.at[0:rows, :], ssem.at[kind])
        wait_bytes(gainrel.at[1:ntp], ssem.at[gains_t])
        wait_bytes(halo, ssem.at[halo_t])
        wait_bytes(metas.at[0:4], ssem.at[metas_z])


def body(
    residual_in,
    gate_outer,
    gate_inner,
    conv_input,
    conv_taps,
    norm_gain,
    out_weight,
    moe_gain,
    expert_ids,
    group_prob,
    route_prob,
    expert_gate,
    expert_up,
    expert_down,
):
    tok, width = residual_in.shape
    seq, chan = conv_input.shape
    fe = expert_gate.shape[2]
    ntp = lax.axis_size("tp")
    nj = lax.axis_size("sp") // NZ
    grp = nj * CAP
    vmem = pl.BlockSpec(memory_space=pltpu.VMEM)
    hbm = pl.BlockSpec(memory_space=pl.ANY)
    dma = pltpu.SemaphoreType.DMA
    shapes = [
        ((tok, width), BF),
        ((seq, chan), BF),
        ((seq, chan), BF),
        ((seq, chan), BF),
        ((chan, width), BF),
        ((2, 16, chan), BF),
        ((seq + 8, chan), F32),
        ((seq, chan), BF),
        ((ntp, tok, chan), BF),
        ((8, chan), F32),
        ((ntp, 8, chan), F32),
        ((ntp, tok, chan), BF),
        ((2, ntp, tok, chan), BF),
        ((ntp, chan, width), BF),
        ((tok, width), BF),
        ((8, tok), F32),
        ((2 * grp, 128), F32),
        ((2 * grp, fe), F32),
        ((2 * grp, fe), F32),
        ((8, width), F32),
        ((5, grp, tok), BF),
        ((NZ, 8, tok), F32),
        ((2, tok, width), BF),
        ((2, tok, width), BF),
        ((2, grp, tok), BF),
        ((2, grp, tok), BF),
        ((2, grp, width), BF),
        ((2, grp, width // 2), BF),
        ((2, grp, width), BF),
        ((2, grp, width // 2), BF),
        ((2, grp, width // 2), BF),
        ((5, grp, width), BF),
        ((8 * grp, width), BF),
        ((8 * grp, width), BF),
        ((grp, width), BF),
        ((2, grp, width), BF),
        ((2, grp, width), BF),
        ((2, grp, width), BF),
        ((2, grp, width // 2), BF),
        ((2, grp, width // 2), BF),
        ((2, grp, width), BF),
        ((2, grp, width // 2), BF),
        ((2, tok, width), BF),
        ((2, tok, width), BF),
        ((2, tok, width), BF),
        ((2, tok, width), BF),
        ((2 * grp, fe), BF),
        ((width, fe), BF),
        ((width, fe), BF),
        ((fe, width), BF),
    ]
    sems = [(5,), (3,), (14,), (3,), (4, NC), (2,), (2, 2), (5, 2, NC), (5,), (7,), (2, NC), (2, NC), (5, 2, NC)]
    return pl.pallas_call(
        layer_kernel,
        out_shape=pltpu.VMEM((tok, width), BF),
        in_specs=[hbm] * 8 + [vmem] * 6,
        out_specs=vmem,
        scratch_shapes=[pltpu.VMEM(s, t) for s, t in shapes] + [dma(s) for s in sems],
        compiler_params=pltpu.CompilerParams(
            collective_id=0, has_side_effects=True, vmem_limit_bytes=61 * 1024 * 1024
        ),
        name="layer",
    )(
        residual_in,
        gate_outer,
        gate_inner,
        conv_input,
        out_weight,
        expert_gate,
        expert_up,
        expert_down,
        conv_taps,
        norm_gain,
        moe_gain,
        expert_ids.T,
        group_prob.reshape(1, tok),
        route_prob.T,
    )


def solution(mesh):
    in_specs = (
        P(("sp", "tp"), None),
        P("sp", "tp"),
        P("sp", "tp"),
        P("sp", "tp"),
        P(None, "tp"),
        P("tp"),
        P("tp", None),
        P(),
        P(("sp", "tp"), None),
        P(("sp", "tp")),
        P(("sp", "tp"), None),
        P("sp", None, None),
        P("sp", None, None),
        P("sp", None, None),
    )
    out_specs = P(("sp", "tp"), None)
    return jax.shard_map(body, mesh=mesh, in_specs=in_specs, out_specs=out_specs, check_vma=False)
```

```python
import jax
import jax.numpy as jnp
from jax import lax
from jax.experimental import pallas as pl
from jax.experimental.pallas import tpu as pltpu
from jax.sharding import PartitionSpec as P

EPSILON = 1e-06
NZ = 8
CAP = 16
NC = 4
MESH = pl.DeviceIdType.MESH
BF = jnp.bfloat16
F32 = jnp.float32


def layer_kernel(
    rin_hbm,
    go_hbm,
    gi_hbm,
    ci_hbm,
    ow_hbm,
    wg_hbm,
    wu_hbm,
    wd_hbm,
    taps_hbm,
    gain_hbm,
    mgain_hbm,
    ids_hbm,
    group_hbm,
    route_hbm,
    out_ref,
    taps_ref,
    gain_ref,
    mgain_ref,
    ids_ref,
    group_ref,
    route_ref,
    rin,
    go,
    gi,
    ci,
    ow,
    halo,
    inner,
    mixed,
    mixrel,
    gainsrc,
    gainrel,
    normed,
    normed_near,
    wrel,
    res_ref,
    meta_ref,
    squares,
    gate,
    value,
    mgain,
    sel,
    metas,
    hop1,
    hop2,
    sel3,
    sel4,
    pack3,
    pack4,
    gather3,
    gather4,
    pass4,
    packed,
    arrived,
    results,
    ret0,
    ret1,
    ret2,
    got3,
    back4,
    got4,
    ret3,
    ret4,
    send2,
    part2,
    send1,
    part1,
    hid,
    wg,
    wu,
    wd,
    isem,
    ssmall,
    wsem,
    ssem,
    trecv,
    arecv,
    nrecv,
    mrecv,
    zrecv,
    xrecv,
    yrecv,
    grecv,
    brecv,
    rrecv,
):
    tok, width = res_ref.shape
    nsp = lax.axis_size("sp")
    ntp = lax.axis_size("tp")
    nj = nsp // NZ
    grp = nj * CAP
    seq, chan = mixed.shape
    others = grp - CAP
    cw = width // NC
    hw = cw // 2
    sp = lax.axis_index("sp")
    tp = lax.axis_index("tp")
    z = sp // nj
    me_j = sp % nj
    step = (1, -1)
    near = (1, NZ - 1)
    far = (2, NZ - 2)
    both = [(n, d) for n in range(NC) for d in (0, 1)]

    def zval(offset):
        return lax.rem(z + offset + NZ, NZ)

    def zid(offset):
        return (zval(offset) * nj + me_j, tp)

    def jid(offset):
        return (z * nj + lax.rem(me_j + offset, nj), tp)

    def tid(offset):
        return (sp, lax.rem(tp + offset, ntp))

    after = (lax.rem(sp + 1, nsp), tp)
    before = (lax.rem(sp + nsp - 1, nsp), tp)
    core = lax.rem(me_j, 2)
    partner = (z * nj + me_j + 1 - 2 * core, tp)

    def cols_of(n):
        return slice(n * cw, (n + 1) * cw)

    def half_of(n):
        return slice(n * hw, (n + 1) * hw)

    def part_of(n, d):
        return slice(n * cw + d * hw, n * cw + (d + 1) * hw)

    def slot_rows(b, j):
        return pl.ds(pl.multiple_of(b * grp + j * CAP, CAP), CAP)

    def block_rows(b):
        return slice(b * grp, (b + 1) * grp)

    near_z, far_z, back_near, back_far, xs, ys, gs, bs, ring, rows_t, gains_t, halo_t, metas_z, normed_z = range(14)

    def remote(src, dst, send, recv, device):
        return pltpu.make_async_remote_copy(
            src_ref=src, dst_ref=dst, send_sem=send, recv_sem=recv, device_id=device, device_id_type=MESH
        )

    def wait_bytes(ref, sem):
        pltpu.make_async_copy(ref, ref, sem).wait()

    def make_slots():
        expert = lax.broadcasted_iota(jnp.int32, (nsp, tok), 0)
        hot = [jnp.where(expert == ids_ref[k : k + 1, :], 1.0, 0.0) for k in (0, 1)]
        earlier_tok = lax.broadcasted_iota(jnp.int32, (tok, tok), 0) < lax.broadcasted_iota(jnp.int32, (tok, tok), 1)
        upper = jnp.where(earlier_tok, 1.0, 0.0).astype(BF)
        rank = [jnp.dot(h.astype(BF), upper, preferred_element_type=F32) for h in hot]
        count = jnp.sum(hot[0], axis=1, keepdims=True)
        slot = expert.astype(F32) * CAP
        meta_ref[0:1, :] = jnp.sum((rank[0] + slot) * hot[0], axis=0, keepdims=True)
        meta_ref[1:2, :] = jnp.sum((rank[1] + count + slot) * hot[1], axis=0, keepdims=True)
        meta_ref[2:3, :] = group_ref[...] * route_ref[0:1, :] / (route_ref[0:1, :] + route_ref[1:2, :])
        meta_ref[3:4, :] = group_ref[...] * route_ref[1:2, :] / (route_ref[0:1, :] + route_ref[1:2, :])
        meta_ref[4:8, :] = jnp.zeros((4, tok), F32)

    smalls = ((ids_hbm, ids_ref), (group_hbm, group_ref), (route_hbm, route_ref))
    smalls += ((taps_hbm, taps_ref), (gain_hbm, gain_ref), (mgain_hbm, mgain_ref))
    scopies = [pltpu.make_async_copy(src, dst, ssmall.at[i]) for i, (src, dst) in enumerate(smalls)]
    icopies = [
        pltpu.make_async_copy(src, dst, isem.at[i])
        for i, (src, dst) in enumerate(((rin_hbm, rin), (ow_hbm, ow), (gi_hbm, gi), (ci_hbm, ci), (go_hbm, go)))
    ]
    wcopies = [
        pltpu.make_async_copy(wg_hbm.at[0], wg, wsem.at[0]),
        pltpu.make_async_copy(wu_hbm.at[0], wu, wsem.at[1]),
        pltpu.make_async_copy(wd_hbm.at[0], wd, wsem.at[2]),
    ]
    barrier = pltpu.get_barrier_semaphore()
    for offset in (1, -1):
        pl.semaphore_signal(barrier, inc=1, device_id=zid(offset), device_id_type=MESH)
    for offset in range(1, nj):
        pl.semaphore_signal(barrier, inc=1, device_id=jid(offset), device_id_type=MESH)
    for offset in range(1, ntp):
        pl.semaphore_signal(barrier, inc=1, device_id=tid(offset), device_id_type=MESH)
    for ident in (after, before):
        pl.semaphore_signal(barrier, inc=1, device_id=ident, device_id_type=MESH)
    for copy in icopies[:2] + scopies + icopies[2:]:
        copy.start()
    with jax.named_scope("barrier"):
        pl.semaphore_wait(barrier, nj + ntp + 2)

    def mcopy(hop, d):
        src = metas.at[near[d]] if hop else meta_ref
        dst = metas.at[far[d] if hop else near[d]]
        return remote(src, dst, ssem.at[metas_z], mrecv.at[hop, d], zid(step[d]))

    def zcopy(hop, d, n):
        cols = cols_of(n)
        if hop == 0:
            src, dst = rin.at[:, cols], hop1.at[d, :, cols]
        elif hop == 1:
            src, dst = hop1.at[d, :, cols], hop2.at[d, :, cols]
        elif hop == 2:
            src, dst = gather3.at[d, :, cols], arrived.at[block_rows(5 + d), cols]
        elif hop == 3:
            src, dst = gather4.at[d, :, half_of(n)], pass4.at[d, :, half_of(n)]
        else:
            src, dst = pass4.at[d, :, half_of(n)], arrived.at[block_rows(7), part_of(n, d)]
        return remote(src, dst, ssem.at[near_z if hop < 2 else far_z], zrecv.at[hop, d, n], zid(step[d]))

    def meta_of(offset):
        return meta_ref if offset == 0 else metas.at[offset]

    def slots_of(target):
        return (lax.broadcasted_iota(jnp.int32, (grp, tok), 0) + target * grp).astype(F32)

    def select(offset, target):
        ref = meta_of(offset)
        slot = slots_of(target)
        hit = jnp.where(slot == ref[0:1, :], 1.0, 0.0) + jnp.where(slot == ref[1:2, :], 1.0, 0.0)
        return hit.astype(BF)

    def spread(offset, target):
        ref = meta_of(offset)
        slot = slots_of(target)
        hit = jnp.where(slot == ref[0:1, :], ref[2:3, :], 0.0) + jnp.where(slot == ref[1:2, :], ref[3:4, :], 0.0)
        return hit.astype(BF)

    def combine(weights, rows):
        return lax.dot_general(weights, rows, (((0,), (0,)), ((), ())), preferred_element_type=F32)

    def ytarget(b):
        return ret0 if b == 0 else ret1.at[b - 1] if b < 3 else ret2.at[b - 3]

    def xstart(b, n):
        cols = cols_of(n)
        for offset in range(1, nj):
            their = slot_rows(0, lax.rem(me_j + offset, nj))
            src, dst = packed.at[b, their, cols], arrived.at[slot_rows(b, me_j), cols]
            remote(src, dst, ssem.at[xs], xrecv.at[b], jid(offset)).start()
        arrived[slot_rows(b, me_j), cols] = packed[b, slot_rows(0, me_j), cols]

    def xwait(b):
        wait_bytes(arrived.at[b * grp : b * grp + others, :], xrecv.at[b])

    def ypart(b, part):
        return (slice(0, width), b) if b < 3 else (slice(part * (width // 2), (part + 1) * (width // 2)), 3 + 2 * (b - 3) + part)

    def ystart(b, part=0):
        dst = ytarget(b)
        cols, index = ypart(b, part)
        for offset in range(1, nj):
            their = slot_rows(b, lax.rem(me_j + offset, nj))
            src = results.at[their, cols]
            remote(src, dst.at[slot_rows(0, me_j), cols], ssem.at[ys], yrecv.at[index], jid(offset)).start()
        dst[slot_rows(0, me_j), cols] = results[slot_rows(b, me_j), cols]

    def ywait(b, part=0):
        cols, index = ypart(b, part)
        wait_bytes(ytarget(b).at[0:others, cols], yrecv.at[index])

    def exchange(src, dst, d, cols, send, recv):
        mine = slot_rows(0, me_j)
        for offset in range(1, nj):
            their = slot_rows(0, lax.rem(me_j + offset, nj))
            remote(src.at[d, their, cols], dst.at[d, mine, cols], send, recv, jid(offset)).start()
        dst[d, mine, cols] = src[d, mine, cols]

    def pack(b, block, n, go_now=True):
        cols = cols_of(n)
        packed[b, :, cols] = jnp.dot(sel[b], block[:, cols], preferred_element_type=F32).astype(BF)
        if go_now:
            xstart(b, n)

    def own_cols(n):
        return pl.ds(pl.multiple_of(n * cw + core * hw, hw), hw)

    def quarter_cols(n, d):
        return pl.ds(pl.multiple_of(n * cw + core * hw + d * (hw // 2), hw // 2), hw // 2)

    def acopy(kind, n):
        if kind == 0:
            src, dst, device = ow.at[:, own_cols(n)], wrel.at[3, :, own_cols(n)], tid(1)
        elif kind == 1:
            src, dst, device = ow.at[:, own_cols(n)], wrel.at[1, :, own_cols(n)], tid(ntp - 1)
        elif kind == 2:
            cols = quarter_cols(n, 0)
            src, dst, device = wrel.at[3, :, cols], wrel.at[2, :, cols], tid(1)
        elif kind == 3:
            cols = quarter_cols(n, 1)
            src, dst, device = wrel.at[1, :, cols], wrel.at[2, :, cols], tid(ntp - 1)
        else:
            cols = own_cols(n)
            block = (3, 1, 2)[kind - 4]
            src, dst, device = wrel.at[block, :, cols], wrel.at[block, :, cols], partner
        return remote(src, dst, ssem.at[ring], arecv.at[(0, 1, 2, 2, 3, 3, 3)[kind], n], device)

    def tcopy(offset):
        rows = pl.ds(pl.multiple_of(lax.rem(tp + offset, ntp) * tok, tok), tok)
        return remote(mixed.at[rows, :], mixrel.at[ntp - offset], ssem.at[rows_t], trecv.at[0], tid(offset))

    def gcopy(offset):
        return remote(gainsrc, gainrel.at[ntp - offset], ssem.at[gains_t], trecv.at[1], tid(offset))

    def hcopy(i):
        src = (gi_hbm, ci_hbm)[i]
        return remote(src.at[seq - 16 : seq, :], halo.at[i], ssem.at[halo_t], trecv.at[2], after)

    def pass_on(n):
        acopy(0, n).wait_recv()
        acopy(2, n).start()
        acopy(4, n).start()
        acopy(1, n).wait_recv()
        acopy(3, n).start()
        acopy(5, n).start()

    for i in (0, 1):
        hcopy(i).start()
    icopies[0].wait()
    for d in (0, 1):
        zcopy(0, d, 0).start()
    icopies[1].wait()
    for kind in (0, 1):
        acopy(kind, 0).start()
    for copy in scopies:
        copy.wait()
    with jax.named_scope("slots"):
        make_slots()
    for d in (0, 1):
        mcopy(0, d).start()
    for n in range(1, NC - 1):
        for d in (0, 1):
            zcopy(0, d, n).start()
    mgain[...] = jnp.broadcast_to(mgain_ref[...].astype(F32)[None, :], mgain.shape)
    gainsrc[...] = jnp.broadcast_to(gain_ref[...].astype(F32)[None, :], gainsrc.shape)
    for offset in range(1, ntp):
        gcopy(offset).start()
    for i in (2, 3, 4):
        icopies[i].wait()
    for copy in wcopies:
        copy.start()
    taps = taps_ref[...].astype(F32)
    kw = taps_ref.shape[0]
    with jax.named_scope("conv"):
        inner[8 : 8 + seq, :] = gi[...].astype(F32) * ci[...].astype(F32)

        def mix(first, rows):
            filtered = taps[0:1, :] * inner[9 - kw + first : 9 - kw + first + rows, :]
            for k in range(1, kw):
                filtered = filtered + taps[k : k + 1, :] * inner[9 - kw + k + first : 9 - kw + k + first + rows, :]
            mixed[first : first + rows, :] = (go[first : first + rows, :].astype(F32) * filtered).astype(BF)

        mix(tok, seq - tok)
    for offset in range(1, ntp):
        pl.when(lax.rem(tp + offset, ntp) != 0)(tcopy(offset).start)
    with jax.named_scope("pass0"):
        pass_on(0)
    with jax.named_scope("halo"):
        wait_bytes(halo, trecv.at[2])
    earlier = halo[0, 8:16, :].astype(F32) * halo[1, 8:16, :].astype(F32)
    inner[0:8, :] = jnp.where(sp > 0, earlier, 0.0)
    mix(0, tok)
    for offset in range(1, ntp):
        pl.when(lax.rem(tp + offset, ntp) == 0)(tcopy(offset).start)
    mixrel[0] = mixed[pl.ds(pl.multiple_of(tp * tok, tok), tok), :]

    with jax.named_scope("rows"):
        wait_bytes(mixrel.at[1:ntp], trecv.at[0])
        wait_bytes(gainrel.at[1:ntp], trecv.at[1])
    gainrel[0] = gainsrc[...]
    for n in (1, 2):
        for kind in (0, 1):
            acopy(kind, n).start()
    with jax.named_scope("norm"):
        square = jnp.zeros((tok, 1), F32)
        for o in range(ntp):
            part = mixrel[o].astype(F32)
            square = square + jnp.sum(part * part, axis=1, keepdims=True)
        factor = lax.rsqrt(square / (chan * ntp) + EPSILON)
        for o in range(ntp):
            normed[o] = (mixrel[o].astype(F32) * factor * gainrel[o, 0:1, :]).astype(BF)

    def ncopy(d):
        return remote(normed, normed_near.at[d], ssem.at[normed_z], nrecv.at[d], zid(step[d]))

    for d in (0, 1):
        ncopy(d).start()
    for d in (0, 1):
        zcopy(0, d, NC - 1).start()

    def selections():
        sel[0] = select(0, z)
        for d in (0, 1):
            mcopy(0, d).wait_recv()
            mcopy(1, d).start()
            sel[1 + d] = select(near[d], z)

    def far_selections():
        for d in (0, 1):
            mcopy(1, d).wait_recv()
            sel[3 + d] = select(far[d], z)
            sel3[d] = select(far[d], zval(step[d]))
            sel4[d] = select(far[d], zval(2 * step[d]))

    def project(values, rows, n):
        cols = cols_of(n)
        total = values[:, cols].astype(F32) + jnp.dot(rows[0], ow[:, cols], preferred_element_type=F32)
        for o in range(1, ntp):
            total = total + jnp.dot(rows[o], wrel[o, :, cols], preferred_element_type=F32)
        return total.astype(BF)

    for n in range(NC):
        with jax.named_scope(f"ring{n}"):
            wait_bytes(wrel.at[2, :, 0:hw], arecv.at[2, n])
            acopy(6, n).start()
            wait_bytes(wrel.at[1:4, :, 0:hw], arecv.at[3, n])
        with jax.named_scope(f"proj{n}"):
            res_ref[:, cols_of(n)] = project(rin, normed, n)
        if n == 0:
            with jax.named_scope("selections"):
                selections()
        with jax.named_scope(f"own{n}"):
            pack(0, res_ref, n)
        for later in ((1, 2), (3,), (), ())[n]:
            with jax.named_scope(f"pass{later}"):
                pass_on(later)
            if later == 1:
                for kind in (0, 1):
                    acopy(kind, 3).start()

    def expert_in(first, count, n, fresh):
        rows = count * grp
        base = first * grp
        cols = pl.ds(pl.multiple_of(n * cw, cw), cw)
        vals = arrived[base : base + rows, cols].astype(F32)
        x = (vals * mgain[0:1, cols]).astype(BF)
        parts = jnp.sum(vals * vals, axis=1, keepdims=True)
        g = jnp.dot(x, wg[cols, :], preferred_element_type=F32)
        u = jnp.dot(x, wu[cols, :], preferred_element_type=F32)
        if fresh:
            squares[0:rows, :] = jnp.broadcast_to(parts, (rows, 128))
            gate[0:rows, :] = g
            value[0:rows, :] = u
        else:
            squares[0:rows, :] += jnp.broadcast_to(parts, (rows, 128))
            gate[0:rows, :] += g
            value[0:rows, :] += u

    def expert_mid(count):
        rows = count * grp
        factor = lax.rsqrt(squares[0:rows, 0:1] / width + EPSILON)
        g = gate[0:rows, :] * factor
        hid[0:rows, :] = (g * jax.nn.sigmoid(g) * (value[0:rows, :] * factor)).astype(BF)

    def expert_out(first, count, n):
        rows = count * grp
        cols = pl.ds(pl.multiple_of(n * cw, cw), cw)
        r = jnp.dot(hid[0:rows, :], wd[:, cols], preferred_element_type=F32)
        results[first * grp : first * grp + rows, cols] = r.astype(BF)

    def experts(first, count):
        expert_in(first, count, 0, True)

        def more(n, carry):
            expert_in(first, count, n, False)
            return carry

        lax.fori_loop(1, NC, more, 0)
        expert_mid(count)

        def out_cols(n, carry):
            expert_out(first, count, n)
            return carry

        lax.fori_loop(0, NC, out_cols, 0)

    with jax.named_scope("normed"):
        for d in (0, 1):
            ncopy(d).wait_recv()
    for n, d in both:
        with jax.named_scope(f"hop1_{n}{d}"):
            zcopy(0, d, n).wait_recv()
        hop1[d, :, cols_of(n)] = project(hop1.at[d], normed_near.at[d], n)
        zcopy(1, d, n).start()
        pack(1 + d, hop1.at[d], n)
    with jax.named_scope("far_selections"):
        far_selections()
    for copy in wcopies:
        copy.wait()
    xwait(0)
    with jax.named_scope("exp0"):
        experts(0, 1)

    def hop3_out(n):
        for d in (0, 1):
            with jax.named_scope(f"ex{n}{d}"):
                wait_bytes(gather3.at[d, 0:others, 0 : cw + hw], grecv.at[d, n])
            zcopy(3, d, n).start()
            zcopy(2, d, n).start()

    for n in range(NC):
        for d in (0, 1):
            with jax.named_scope(f"hop2_{n}{d}"):
                zcopy(1, d, n).wait_recv()
            part = hop2[d, :, cols_of(n)]
            pack3[d, :, cols_of(n)] = jnp.dot(sel3[d], part, preferred_element_type=F32).astype(BF)
            part = hop2[d, :, part_of(n, d)]
            pack4[d, :, half_of(n)] = jnp.dot(sel4[d], part, preferred_element_type=F32).astype(BF)
            exchange(pack4, gather4, d, half_of(n), ssem.at[gs], grecv.at[d, n])
            exchange(pack3, gather3, d, cols_of(n), ssem.at[gs], grecv.at[d, n])
            pack(3 + d, hop2.at[d], n, False)
        if n > 0:
            hop3_out(n - 1)
            if n < 3:
                xstart(3, n - 1)
                xstart(4, n - 1)
        if n == 1:
            xwait(1)
            xwait(2)
            with jax.named_scope("exp12"):
                experts(1, 2)
    hop3_out(NC - 1)
    for n in (2, 3):
        xstart(3, n)
        xstart(4, n)

    def rcopy(kind, d, n):
        cols = cols_of(n)
        if kind == 0:
            src, dst = results.at[block_rows(7), part_of(n, d)], back4.at[d, :, half_of(n)]
        elif kind == 1:
            src, dst = results.at[block_rows(5 + d), cols], got3.at[d, :, cols]
        elif kind == 2:
            src, dst = back4.at[d, :, half_of(n)], got4.at[d, :, half_of(n)]
        elif kind == 3:
            src, dst = send2.at[d, :, cols], part2.at[d, :, cols]
        else:
            src, dst = send1.at[d, :, cols], part1.at[d, :, cols]
        return remote(src, dst, ssem.at[back_near if kind > 2 else back_far], rrecv.at[kind, d, n], zid(-step[d]))

    for n in range(NC):
        for d in (0, 1):
            with jax.named_scope(f"hop3_{n}{d}"):
                zcopy(3, d, n).wait_recv()
            zcopy(4, d, n).start()
        if n == NC - 1:
            ystart(1)
        with jax.named_scope(f"hop3w{n}"):
            for d in (0, 1):
                zcopy(2, d, n).wait_recv()
        with jax.named_scope(f"in56_{n}"):
            expert_in(5, 2, n, n == 0)
    with jax.named_scope("out56"):
        expert_mid(2)
        for n in range(NC):
            expert_out(5, 2, n)
            if n < 2:
                for d in (0, 1):
                    rcopy(1, d, n).start()
    with jax.named_scope("xw34"):
        xwait(3)
        xwait(4)
    with jax.named_scope("exp34"):
        experts(3, 2)
    ystart(3)
    ystart(4)
    for n in range(NC):
        with jax.named_scope(f"hop4w{n}"):
            for d in (0, 1):
                zcopy(4, d, n).wait_recv()
        with jax.named_scope(f"in7_{n}"):
            expert_in(7, 1, n, n == 0)
    with jax.named_scope("out7"):
        expert_mid(1)
        for n in range(NC):
            expert_out(7, 1, n)
            for d in (0, 1):
                rcopy(0, d, n).start()
    def slots3_in(n):
        for d in (0, 1):
            with jax.named_scope(f"r3_{n}{d}"):
                rcopy(1, d, n).wait_recv()
            exchange(got3, ret3, d, cols_of(n), ssem.at[bs], brecv.at[d, n])

    slots3_in(0)
    slots3_in(1)
    for n, d in both:
        with jax.named_scope(f"r4_{n}{d}"):
            rcopy(0, d, n).wait_recv()
        rcopy(2, d, n).start()
        if n < 2:
            rcopy(1, d, n + 2).start()

    def sums2_out(n):
        if n % 2 == 0:
            ywait(3, n // 2)
            ywait(4, n // 2)
        for d in (0, 1):
            with jax.named_scope(f"ex{n}{d}"):
                wait_bytes(ret3.at[d, 0:others, 0 : cw + hw], brecv.at[d, n])
            total = combine(spread(far[d], z), ret2[d, :, cols_of(n)])
            total = total + combine(spread(far[d], zval(step[d])), ret3[d, :, cols_of(n)])
            last = combine(spread(far[d], zval(2 * step[d])), ret4[d, :, half_of(n)])
            lo, hi = total[:, :hw], total[:, hw:]
            if d == 0:
                lo = lo + last
            else:
                hi = hi + last
            send2[d, :, part_of(n, 0)] = lo.astype(BF)
            send2[d, :, part_of(n, 1)] = hi.astype(BF)
            rcopy(3, d, n).start()

    def slots4_in(n):
        for d in (0, 1):
            with jax.named_scope(f"r3b_{n}{d}"):
                rcopy(2, d, n).wait_recv()
            exchange(got4, ret4, d, half_of(n), ssem.at[bs], brecv.at[d, n])

    slots4_in(0)
    ystart(3, 1)
    slots3_in(2)
    slots4_in(1)
    ystart(4, 1)
    sums2_out(0)
    slots3_in(3)
    slots4_in(2)
    sums2_out(1)
    slots4_in(3)
    sums2_out(2)
    ystart(2)
    sums2_out(3)
    with jax.named_scope("yw12"):
        ywait(1)
        ywait(2)
    ystart(0)
    for n, d in both:
        with jax.named_scope(f"r2_{n}{d}"):
            rcopy(3, d, n).wait_recv()
        cols = cols_of(n)
        total = part2[d, :, cols].astype(F32) + combine(spread(near[d], z), ret1[d, :, cols])
        send1[d, :, cols] = total.astype(BF)
        rcopy(4, d, n).start()
    ywait(0)
    own = spread(0, z)
    for n in range(NC):
        with jax.named_scope(f"r1_{n}"):
            rcopy(4, 0, n).wait_recv()
            rcopy(4, 1, n).wait_recv()
        cols = cols_of(n)
        total = res_ref[:, cols].astype(F32) + combine(own, ret0[:, cols])
        total = total + part1[0, :, cols].astype(F32) + part1[1, :, cols].astype(F32)
        out_ref[:, cols] = total.astype(BF)
    with jax.named_scope("ends"):
        flat = ((near_z, 4 * tok), (far_z, 4 * grp), (back_near, 4 * tok), (back_far, 4 * grp), (xs, 5 * others), (ys, 5 * others))
        flat += ((gs, 3 * others), (bs, 3 * others), (ring, 3 * chan), (rows_t, 3 * tok * chan // width), (normed_z, 2 * ntp * tok * chan // width))
        for kind, rows in flat:
            wait_bytes(arrived.at[0:rows, :], ssem.at[kind])
        wait_bytes(gainrel.at[1:ntp], ssem.at[gains_t])
        wait_bytes(halo, ssem.at[halo_t])
        wait_bytes(metas.at[0:4], ssem.at[metas_z])


def body(
    residual_in,
    gate_outer,
    gate_inner,
    conv_input,
    conv_taps,
    norm_gain,
    out_weight,
    moe_gain,
    expert_ids,
    group_prob,
    route_prob,
    expert_gate,
    expert_up,
    expert_down,
):
    tok, width = residual_in.shape
    seq, chan = conv_input.shape
    fe = expert_gate.shape[2]
    ntp = lax.axis_size("tp")
    nj = lax.axis_size("sp") // NZ
    grp = nj * CAP
    vmem = pl.BlockSpec(memory_space=pltpu.VMEM)
    hbm = pl.BlockSpec(memory_space=pl.ANY)
    dma = pltpu.SemaphoreType.DMA
    shapes = [
        ((conv_taps.shape[0], chan), BF),
        ((chan,), BF),
        ((width,), BF),
        ((2, tok), jnp.int32),
        ((1, tok), F32),
        ((2, tok), F32),
        ((tok, width), BF),
        ((seq, chan), BF),
        ((seq, chan), BF),
        ((seq, chan), BF),
        ((chan, width), BF),
        ((2, 16, chan), BF),
        ((seq + 8, chan), F32),
        ((seq, chan), BF),
        ((ntp, tok, chan), BF),
        ((8, chan), F32),
        ((ntp, 8, chan), F32),
        ((ntp, tok, chan), BF),
        ((2, ntp, tok, chan), BF),
        ((ntp, chan, width), BF),
        ((tok, width), BF),
        ((8, tok), F32),
        ((2 * grp, 128), F32),
        ((2 * grp, fe), F32),
        ((2 * grp, fe), F32),
        ((8, width), F32),
        ((5, grp, tok), BF),
        ((NZ, 8, tok), F32),
        ((2, tok, width), BF),
        ((2, tok, width), BF),
        ((2, grp, tok), BF),
        ((2, grp, tok), BF),
        ((2, grp, width), BF),
        ((2, grp, width // 2), BF),
        ((2, grp, width), BF),
        ((2, grp, width // 2), BF),
        ((2, grp, width // 2), BF),
        ((5, grp, width), BF),
        ((8 * grp, width), BF),
        ((8 * grp, width), BF),
        ((grp, width), BF),
        ((2, grp, width), BF),
        ((2, grp, width), BF),
        ((2, grp, width), BF),
        ((2, grp, width // 2), BF),
        ((2, grp, width // 2), BF),
        ((2, grp, width), BF),
        ((2, grp, width // 2), BF),
        ((2, tok, width), BF),
        ((2, tok, width), BF),
        ((2, tok, width), BF),
        ((2, tok, width), BF),
        ((2 * grp, fe), BF),
        ((width, fe), BF),
        ((width, fe), BF),
        ((fe, width), BF),
    ]
    sems = [(5,), (6,), (3,), (14,), (3,), (4, NC), (2,), (2, 2), (5, 2, NC), (5,), (7,), (2, NC), (2, NC), (5, 2, NC)]
    return pl.pallas_call(
        layer_kernel,
        out_shape=pltpu.VMEM((tok, width), BF),
        in_specs=[hbm] * 14,
        out_specs=vmem,
        scratch_shapes=[pltpu.VMEM(s, t) for s, t in shapes] + [dma(s) for s in sems],
        compiler_params=pltpu.CompilerParams(
            collective_id=0, has_side_effects=True, vmem_limit_bytes=61 * 1024 * 1024
        ),
        name="layer",
    )(
        residual_in,
        gate_outer,
        gate_inner,
        conv_input,
        out_weight,
        expert_gate,
        expert_up,
        expert_down,
        conv_taps,
        norm_gain,
        moe_gain,
        expert_ids.T,
        group_prob.reshape(1, tok),
        route_prob.T,
    )


def solution(mesh):
    in_specs = (
        P(("sp", "tp"), None),
        P("sp", "tp"),
        P("sp", "tp"),
        P("sp", "tp"),
        P(None, "tp"),
        P("tp"),
        P("tp", None),
        P(),
        P(("sp", "tp"), None),
        P(("sp", "tp")),
        P(("sp", "tp"), None),
        P("sp", None, None),
        P("sp", None, None),
        P("sp", None, None),
    )
    out_specs = P(("sp", "tp"), None)
    return jax.shard_map(body, mesh=mesh, in_specs=in_specs, out_specs=out_specs, check_vma=False)
```

```python
import jax
import jax.numpy as jnp
from jax import lax
from jax.experimental import pallas as pl
from jax.experimental.pallas import tpu as pltpu
from jax.sharding import PartitionSpec as P

EPSILON = 1e-06
NZ = 8
CAP = 16
NC = 4
MESH = pl.DeviceIdType.MESH
BF = jnp.bfloat16
F32 = jnp.float32


def layer_kernel(
    rin_hbm,
    go_hbm,
    gi_hbm,
    ci_hbm,
    ow_hbm,
    wg_hbm,
    wu_hbm,
    wd_hbm,
    taps_hbm,
    gain_hbm,
    mgain_hbm,
    ids_hbm,
    group_hbm,
    route_hbm,
    out_ref,
    taps_ref,
    gain_ref,
    mgain_ref,
    ids_ref,
    group_ref,
    route_ref,
    rin,
    go,
    gi,
    ci,
    ow,
    halo,
    inner,
    mixed,
    mixrel,
    gainsrc,
    gainrel,
    normed,
    normed_near,
    wrel,
    res_ref,
    meta_ref,
    squares,
    gate,
    value,
    mgain,
    sel,
    metas,
    hop1,
    hop2,
    sel3,
    sel4,
    pack3,
    pack4,
    gather3,
    gather4,
    pass4,
    packed,
    arrived,
    results,
    ret0,
    ret1,
    ret2,
    got3,
    back4,
    got4,
    ret3,
    ret4,
    send2,
    part2,
    send1,
    part1,
    hid,
    wg,
    wu,
    wd,
    isem,
    ssmall,
    wsem,
    ssem,
    trecv,
    arecv,
    nrecv,
    mrecv,
    zrecv,
    xrecv,
    yrecv,
    grecv,
    brecv,
    rrecv,
):
    tok, width = res_ref.shape
    nsp = lax.axis_size("sp")
    ntp = lax.axis_size("tp")
    nj = nsp // NZ
    grp = nj * CAP
    seq, chan = mixed.shape
    others = grp - CAP
    cw = width // NC
    hw = cw // 2
    sp = lax.axis_index("sp")
    tp = lax.axis_index("tp")
    z = sp // nj
    me_j = sp % nj
    step = (1, -1)
    near = (1, NZ - 1)
    far = (2, NZ - 2)
    both = [(n, d) for n in range(NC) for d in (0, 1)]

    def zval(offset):
        return lax.rem(z + offset + NZ, NZ)

    def zid(offset):
        return (zval(offset) * nj + me_j, tp)

    def jid(offset):
        return (z * nj + lax.rem(me_j + offset, nj), tp)

    def tid(offset):
        return (sp, lax.rem(tp + offset, ntp))

    after = (lax.rem(sp + 1, nsp), tp)
    before = (lax.rem(sp + nsp - 1, nsp), tp)
    core = lax.rem(me_j, 2)
    partner = (z * nj + me_j + 1 - 2 * core, tp)

    def cols_of(n):
        return slice(n * cw, (n + 1) * cw)

    def half_of(n):
        return slice(n * hw, (n + 1) * hw)

    def part_of(n, d):
        return slice(n * cw + d * hw, n * cw + (d + 1) * hw)

    def slot_rows(b, j):
        return pl.ds(pl.multiple_of(b * grp + j * CAP, CAP), CAP)

    def block_rows(b):
        return slice(b * grp, (b + 1) * grp)

    near_z, far_z, back_near, back_far, xs, ys, gs, bs, ring, rows_t, gains_t, halo_t, metas_z, normed_z = range(14)

    def remote(src, dst, send, recv, device):
        return pltpu.make_async_remote_copy(
            src_ref=src, dst_ref=dst, send_sem=send, recv_sem=recv, device_id=device, device_id_type=MESH
        )

    def wait_bytes(ref, sem):
        pltpu.make_async_copy(ref, ref, sem).wait()

    def make_slots():
        expert = lax.broadcasted_iota(jnp.int32, (nsp, tok), 0)
        hot = [jnp.where(expert == ids_ref[k : k + 1, :], 1.0, 0.0) for k in (0, 1)]
        earlier_tok = lax.broadcasted_iota(jnp.int32, (tok, tok), 0) < lax.broadcasted_iota(jnp.int32, (tok, tok), 1)
        upper = jnp.where(earlier_tok, 1.0, 0.0).astype(BF)
        rank = [jnp.dot(h.astype(BF), upper, preferred_element_type=F32) for h in hot]
        count = jnp.sum(hot[0], axis=1, keepdims=True)
        slot = expert.astype(F32) * CAP
        meta_ref[0:1, :] = jnp.sum((rank[0] + slot) * hot[0], axis=0, keepdims=True)
        meta_ref[1:2, :] = jnp.sum((rank[1] + count + slot) * hot[1], axis=0, keepdims=True)
        meta_ref[2:3, :] = group_ref[...] * route_ref[0:1, :] / (route_ref[0:1, :] + route_ref[1:2, :])
        meta_ref[3:4, :] = group_ref[...] * route_ref[1:2, :] / (route_ref[0:1, :] + route_ref[1:2, :])
        meta_ref[4:8, :] = jnp.zeros((4, tok), F32)

    smalls = ((ids_hbm, ids_ref), (group_hbm, group_ref), (route_hbm, route_ref))
    smalls += ((taps_hbm, taps_ref), (gain_hbm, gain_ref), (mgain_hbm, mgain_ref))
    scopies = [pltpu.make_async_copy(src, dst, ssmall.at[i]) for i, (src, dst) in enumerate(smalls)]
    icopies = [
        pltpu.make_async_copy(src, dst, isem.at[i])
        for i, (src, dst) in enumerate(((rin_hbm, rin), (ow_hbm, ow), (gi_hbm, gi), (ci_hbm, ci), (go_hbm, go)))
    ]
    wcopies = [
        pltpu.make_async_copy(wg_hbm.at[0], wg, wsem.at[0]),
        pltpu.make_async_copy(wu_hbm.at[0], wu, wsem.at[1]),
        pltpu.make_async_copy(wd_hbm.at[0], wd, wsem.at[2]),
    ]
    barrier = pltpu.get_barrier_semaphore()
    for offset in (1, -1):
        pl.semaphore_signal(barrier, inc=1, device_id=zid(offset), device_id_type=MESH)
    for offset in range(1, nj):
        pl.semaphore_signal(barrier, inc=1, device_id=jid(offset), device_id_type=MESH)
    for offset in range(1, ntp):
        pl.semaphore_signal(barrier, inc=1, device_id=tid(offset), device_id_type=MESH)
    for ident in (after, before):
        pl.semaphore_signal(barrier, inc=1, device_id=ident, device_id_type=MESH)
    for copy in icopies[:2] + scopies + icopies[2:]:
        copy.start()
    with jax.named_scope("barrier"):
        pl.semaphore_wait(barrier, nj + ntp + 2)

    def mcopy(hop, d):
        src = metas.at[near[d]] if hop else meta_ref
        dst = metas.at[far[d] if hop else near[d]]
        return remote(src, dst, ssem.at[metas_z], mrecv.at[hop, d], zid(step[d]))

    def zcopy(hop, d, n):
        cols = cols_of(n)
        if hop == 0:
            src, dst = rin.at[:, cols], hop1.at[d, :, cols]
        elif hop == 1:
            src, dst = hop1.at[d, :, cols], hop2.at[d, :, cols]
        elif hop == 2:
            src, dst = gather3.at[d, :, cols], arrived.at[block_rows(5 + d), cols]
        elif hop == 3:
            src, dst = gather4.at[d, :, half_of(n)], pass4.at[d, :, half_of(n)]
        else:
            src, dst = pass4.at[d, :, half_of(n)], arrived.at[block_rows(7), part_of(n, d)]
        return remote(src, dst, ssem.at[near_z if hop < 2 else far_z], zrecv.at[(0, 2, 4, 5, 7)[hop] + (0 if hop in (2, 4) else d), n], zid(step[d]))

    def meta_of(offset):
        return meta_ref if offset == 0 else metas.at[offset]

    def slots_of(target):
        return (lax.broadcasted_iota(jnp.int32, (grp, tok), 0) + target * grp).astype(F32)

    def select(offset, target):
        ref = meta_of(offset)
        slot = slots_of(target)
        hit = jnp.where(slot == ref[0:1, :], 1.0, 0.0) + jnp.where(slot == ref[1:2, :], 1.0, 0.0)
        return hit.astype(BF)

    def spread(offset, target):
        ref = meta_of(offset)
        slot = slots_of(target)
        hit = jnp.where(slot == ref[0:1, :], ref[2:3, :], 0.0) + jnp.where(slot == ref[1:2, :], ref[3:4, :], 0.0)
        return hit.astype(BF)

    def combine(weights, rows):
        return lax.dot_general(weights, rows, (((0,), (0,)), ((), ())), preferred_element_type=F32)

    def ytarget(b):
        return ret0 if b == 0 else ret1.at[b - 1] if b < 3 else ret2.at[b - 3]

    def xstart(b, n):
        cols = cols_of(n)
        for offset in range(1, nj):
            their = slot_rows(0, lax.rem(me_j + offset, nj))
            src, dst = packed.at[b, their, cols], arrived.at[slot_rows(b, me_j), cols]
            remote(src, dst, ssem.at[xs], xrecv.at[b], jid(offset)).start()
        arrived[slot_rows(b, me_j), cols] = packed[b, slot_rows(0, me_j), cols]

    def xwait(b):
        wait_bytes(arrived.at[b * grp : b * grp + others, :], xrecv.at[b])

    def ypart(b, part):
        return (slice(0, width), b) if b < 3 else (slice(part * (width // 2), (part + 1) * (width // 2)), 3 + 2 * (b - 3) + part)

    def ystart(b, part=0):
        dst = ytarget(b)
        cols, index = ypart(b, part)
        for offset in range(1, nj):
            their = slot_rows(b, lax.rem(me_j + offset, nj))
            src = results.at[their, cols]
            remote(src, dst.at[slot_rows(0, me_j), cols], ssem.at[ys], yrecv.at[index], jid(offset)).start()
        dst[slot_rows(0, me_j), cols] = results[slot_rows(b, me_j), cols]

    def ywait(b, part=0):
        cols, index = ypart(b, part)
        wait_bytes(ytarget(b).at[0:others, cols], yrecv.at[index])

    def exchange(src, dst, d, cols, send, recv):
        mine = slot_rows(0, me_j)
        for offset in range(1, nj):
            their = slot_rows(0, lax.rem(me_j + offset, nj))
            remote(src.at[d, their, cols], dst.at[d, mine, cols], send, recv, jid(offset)).start()
        dst[d, mine, cols] = src[d, mine, cols]

    def pack(b, block, n, go_now=True):
        cols = cols_of(n)
        packed[b, :, cols] = jnp.dot(sel[b], block[:, cols], preferred_element_type=F32).astype(BF)
        if go_now:
            xstart(b, n)

    def own_cols(n):
        return pl.ds(pl.multiple_of(n * cw + core * hw, hw), hw)

    def quarter_cols(n, d):
        return pl.ds(pl.multiple_of(n * cw + core * hw + d * (hw // 2), hw // 2), hw // 2)

    def acopy(kind, n):
        if kind == 0:
            src, dst, device = ow.at[:, own_cols(n)], wrel.at[3, :, own_cols(n)], tid(1)
        elif kind == 1:
            src, dst, device = ow.at[:, own_cols(n)], wrel.at[1, :, own_cols(n)], tid(ntp - 1)
        elif kind == 2:
            cols = quarter_cols(n, 0)
            src, dst, device = wrel.at[3, :, cols], wrel.at[2, :, cols], tid(1)
        elif kind == 3:
            cols = quarter_cols(n, 1)
            src, dst, device = wrel.at[1, :, cols], wrel.at[2, :, cols], tid(ntp - 1)
        else:
            cols = own_cols(n)
            block = (3, 1, 2)[kind - 4]
            src, dst, device = wrel.at[block, :, cols], wrel.at[block, :, cols], partner
        return remote(src, dst, ssem.at[ring], arecv.at[(0, 1, 2, 2, 3, 3, 3)[kind], n], device)

    def tcopy(offset):
        rows = pl.ds(pl.multiple_of(lax.rem(tp + offset, ntp) * tok, tok), tok)
        return remote(mixed.at[rows, :], mixrel.at[ntp - offset], ssem.at[rows_t], trecv.at[0], tid(offset))

    def gcopy(offset):
        return remote(gainsrc, gainrel.at[ntp - offset], ssem.at[gains_t], trecv.at[1], tid(offset))

    def hcopy(i):
        src = (gi_hbm, ci_hbm)[i]
        return remote(src.at[seq - 16 : seq, :], halo.at[i], ssem.at[halo_t], trecv.at[2], after)

    def pass_on(n):
        acopy(0, n).wait_recv()
        acopy(2, n).start()
        acopy(4, n).start()
        acopy(1, n).wait_recv()
        acopy(3, n).start()
        acopy(5, n).start()

    for i in (0, 1):
        hcopy(i).start()
    icopies[0].wait()
    for d in (0, 1):
        zcopy(0, d, 0).start()
    icopies[1].wait()
    for kind in (0, 1):
        acopy(kind, 0).start()
    for copy in scopies:
        copy.wait()
    with jax.named_scope("slots"):
        make_slots()
    for d in (0, 1):
        mcopy(0, d).start()
    for n in range(1, NC - 1):
        for d in (0, 1):
            zcopy(0, d, n).start()
    mgain[...] = jnp.broadcast_to(mgain_ref[...].astype(F32)[None, :], mgain.shape)
    gainsrc[...] = jnp.broadcast_to(gain_ref[...].astype(F32)[None, :], gainsrc.shape)
    for offset in range(1, ntp):
        gcopy(offset).start()
    for i in (2, 3, 4):
        icopies[i].wait()
    for copy in wcopies:
        copy.start()
    taps = taps_ref[...].astype(F32)
    kw = taps_ref.shape[0]
    with jax.named_scope("conv"):
        inner[8 : 8 + seq, :] = gi[...].astype(F32) * ci[...].astype(F32)

        def mix(first, rows):
            filtered = taps[0:1, :] * inner[9 - kw + first : 9 - kw + first + rows, :]
            for k in range(1, kw):
                filtered = filtered + taps[k : k + 1, :] * inner[9 - kw + k + first : 9 - kw + k + first + rows, :]
            mixed[first : first + rows, :] = (go[first : first + rows, :].astype(F32) * filtered).astype(BF)

        mix(tok, seq - tok)
    for offset in range(1, ntp):
        pl.when(lax.rem(tp + offset, ntp) != 0)(tcopy(offset).start)
    with jax.named_scope("pass0"):
        pass_on(0)
    with jax.named_scope("halo"):
        wait_bytes(halo, trecv.at[2])
    earlier = halo[0, 8:16, :].astype(F32) * halo[1, 8:16, :].astype(F32)
    inner[0:8, :] = jnp.where(sp > 0, earlier, 0.0)
    mix(0, tok)
    for offset in range(1, ntp):
        pl.when(lax.rem(tp + offset, ntp) == 0)(tcopy(offset).start)
    mixrel[0] = mixed[pl.ds(pl.multiple_of(tp * tok, tok), tok), :]

    with jax.named_scope("rows"):
        wait_bytes(mixrel.at[1:ntp], trecv.at[0])
        wait_bytes(gainrel.at[1:ntp], trecv.at[1])
    gainrel[0] = gainsrc[...]
    for n in (1, 2):
        for kind in (0, 1):
            acopy(kind, n).start()
    with jax.named_scope("norm"):
        square = jnp.zeros((tok, 1), F32)
        for o in range(ntp):
            part = mixrel[o].astype(F32)
            square = square + jnp.sum(part * part, axis=1, keepdims=True)
        factor = lax.rsqrt(square / (chan * ntp) + EPSILON)
        for o in range(ntp):
            normed[o] = (mixrel[o].astype(F32) * factor * gainrel[o, 0:1, :]).astype(BF)

    def ncopy(d):
        return remote(normed, normed_near.at[d], ssem.at[normed_z], nrecv.at[d], zid(step[d]))

    for d in (0, 1):
        ncopy(d).start()
    for d in (0, 1):
        zcopy(0, d, NC - 1).start()

    def selections():
        sel[0] = select(0, z)
        for d in (0, 1):
            mcopy(0, d).wait_recv()
            mcopy(1, d).start()
            sel[1 + d] = select(near[d], z)

    def far_selections():
        for d in (0, 1):
            mcopy(1, d).wait_recv()
            sel[3 + d] = select(far[d], z)
            sel3[d] = select(far[d], zval(step[d]))
            sel4[d] = select(far[d], zval(2 * step[d]))

    def project(values, rows, n):
        cols = cols_of(n)
        total = values[:, cols].astype(F32) + jnp.dot(rows[0], ow[:, cols], preferred_element_type=F32)
        for o in range(1, ntp):
            total = total + jnp.dot(rows[o], wrel[o, :, cols], preferred_element_type=F32)
        return total.astype(BF)

    for n in range(NC):
        with jax.named_scope(f"ring{n}"):
            wait_bytes(wrel.at[2, :, 0:hw], arecv.at[2, n])
            acopy(6, n).start()
            wait_bytes(wrel.at[1:4, :, 0:hw], arecv.at[3, n])
        with jax.named_scope(f"proj{n}"):
            res_ref[:, cols_of(n)] = project(rin, normed, n)
        if n == 0:
            with jax.named_scope("selections"):
                selections()
        with jax.named_scope(f"own{n}"):
            pack(0, res_ref, n)
        for later in ((1, 2), (3,), (), ())[n]:
            with jax.named_scope(f"pass{later}"):
                pass_on(later)
            if later == 1:
                for kind in (0, 1):
                    acopy(kind, 3).start()

    def expert_in(first, count, n, fresh):
        rows = count * grp
        base = first * grp
        cols = pl.ds(pl.multiple_of(n * cw, cw), cw)
        vals = arrived[base : base + rows, cols].astype(F32)
        x = (vals * mgain[0:1, cols]).astype(BF)
        parts = jnp.sum(vals * vals, axis=1, keepdims=True)
        g = jnp.dot(x, wg[cols, :], preferred_element_type=F32)
        u = jnp.dot(x, wu[cols, :], preferred_element_type=F32)
        if fresh:
            squares[0:rows, :] = jnp.broadcast_to(parts, (rows, 128))
            gate[0:rows, :] = g
            value[0:rows, :] = u
        else:
            squares[0:rows, :] += jnp.broadcast_to(parts, (rows, 128))
            gate[0:rows, :] += g
            value[0:rows, :] += u

    def expert_mid(count):
        rows = count * grp
        factor = lax.rsqrt(squares[0:rows, 0:1] / width + EPSILON)
        g = gate[0:rows, :] * factor
        hid[0:rows, :] = (g * jax.nn.sigmoid(g) * (value[0:rows, :] * factor)).astype(BF)

    def expert_out(first, count, n):
        rows = count * grp
        cols = pl.ds(pl.multiple_of(n * cw, cw), cw)
        r = jnp.dot(hid[0:rows, :], wd[:, cols], preferred_element_type=F32)
        results[first * grp : first * grp + rows, cols] = r.astype(BF)

    def experts(first, count):
        expert_in(first, count, 0, True)

        def more(n, carry):
            expert_in(first, count, n, False)
            return carry

        lax.fori_loop(1, NC, more, 0)
        expert_mid(count)

        def out_cols(n, carry):
            expert_out(first, count, n)
            return carry

        lax.fori_loop(0, NC, out_cols, 0)

    with jax.named_scope("normed"):
        for d in (0, 1):
            ncopy(d).wait_recv()
    for n, d in both:
        with jax.named_scope(f"hop1_{n}{d}"):
            zcopy(0, d, n).wait_recv()
        hop1[d, :, cols_of(n)] = project(hop1.at[d], normed_near.at[d], n)
        zcopy(1, d, n).start()
        pack(1 + d, hop1.at[d], n)
    with jax.named_scope("far_selections"):
        far_selections()
    for copy in wcopies:
        copy.wait()
    xwait(0)
    with jax.named_scope("exp0"):
        experts(0, 1)

    def hop3_out(n):
        for d in (0, 1):
            with jax.named_scope(f"ex{n}{d}"):
                wait_bytes(gather3.at[d, 0:others, 0 : cw + hw], grecv.at[d, n])
            zcopy(3, d, n).start()
            zcopy(2, d, n).start()

    for n in range(NC):
        for d in (0, 1):
            with jax.named_scope(f"hop2_{n}{d}"):
                zcopy(1, d, n).wait_recv()
            part = hop2[d, :, cols_of(n)]
            pack3[d, :, cols_of(n)] = jnp.dot(sel3[d], part, preferred_element_type=F32).astype(BF)
            part = hop2[d, :, part_of(n, d)]
            pack4[d, :, half_of(n)] = jnp.dot(sel4[d], part, preferred_element_type=F32).astype(BF)
            exchange(pack4, gather4, d, half_of(n), ssem.at[gs], grecv.at[d, n])
            exchange(pack3, gather3, d, cols_of(n), ssem.at[gs], grecv.at[d, n])
            pack(3 + d, hop2.at[d], n, False)
        if n > 0:
            hop3_out(n - 1)
            if n < 3:
                xstart(3, n - 1)
                xstart(4, n - 1)
        if n == 1:
            xwait(1)
            xwait(2)
            with jax.named_scope("exp12"):
                experts(1, 2)
    hop3_out(NC - 1)
    for n in (2, 3):
        xstart(3, n)
        xstart(4, n)

    def rcopy(kind, d, n):
        cols = cols_of(n)
        if kind == 0:
            src, dst = results.at[block_rows(7), part_of(n, d)], back4.at[d, :, half_of(n)]
        elif kind == 1:
            src, dst = results.at[block_rows(5 + d), cols], got3.at[d, :, cols]
        elif kind == 2:
            src, dst = back4.at[d, :, half_of(n)], got4.at[d, :, half_of(n)]
        elif kind == 3:
            src, dst = send2.at[d, :, cols], part2.at[d, :, cols]
        else:
            src, dst = send1.at[d, :, cols], part1.at[d, :, cols]
        return remote(src, dst, ssem.at[back_near if kind > 2 else back_far], rrecv.at[8 if kind == 4 else 2 * kind + d, n], zid(-step[d]))

    for n in range(NC):
        for d in (0, 1):
            with jax.named_scope(f"hop3_{n}{d}"):
                zcopy(3, d, n).wait_recv()
            zcopy(4, d, n).start()
        if n == NC - 1:
            ystart(1)
        with jax.named_scope(f"hop3w{n}"):
            wait_bytes(arrived.at[5 * grp : 7 * grp, cols_of(n)], zrecv.at[4, n])
        with jax.named_scope(f"in56_{n}"):
            expert_in(5, 2, n, n == 0)
    with jax.named_scope("out56"):
        expert_mid(2)
        for n in range(NC):
            expert_out(5, 2, n)
            if n < 2:
                for d in (0, 1):
                    rcopy(1, d, n).start()
    with jax.named_scope("xw34"):
        xwait(3)
        xwait(4)
    with jax.named_scope("exp34"):
        experts(3, 2)
    ystart(3)
    ystart(4)
    for n in range(NC):
        with jax.named_scope(f"hop4w{n}"):
            wait_bytes(arrived.at[block_rows(7), cols_of(n)], zrecv.at[7, n])
        with jax.named_scope(f"in7_{n}"):
            expert_in(7, 1, n, n == 0)
    with jax.named_scope("out7"):
        expert_mid(1)
        for n in range(NC):
            expert_out(7, 1, n)
            for d in (0, 1):
                rcopy(0, d, n).start()
    def slots3_in(n):
        for d in (0, 1):
            with jax.named_scope(f"r3_{n}{d}"):
                rcopy(1, d, n).wait_recv()
            exchange(got3, ret3, d, cols_of(n), ssem.at[bs], brecv.at[d, n])

    slots3_in(0)
    slots3_in(1)
    for n, d in both:
        with jax.named_scope(f"r4_{n}{d}"):
            rcopy(0, d, n).wait_recv()
        rcopy(2, d, n).start()
        if n < 2:
            rcopy(1, d, n + 2).start()

    def sums2_out(n):
        if n % 2 == 0:
            ywait(3, n // 2)
            ywait(4, n // 2)
        for d in (0, 1):
            with jax.named_scope(f"ex{n}{d}"):
                wait_bytes(ret3.at[d, 0:others, 0 : cw + hw], brecv.at[d, n])
            total = combine(spread(far[d], z), ret2[d, :, cols_of(n)])
            total = total + combine(spread(far[d], zval(step[d])), ret3[d, :, cols_of(n)])
            last = combine(spread(far[d], zval(2 * step[d])), ret4[d, :, half_of(n)])
            lo, hi = total[:, :hw], total[:, hw:]
            if d == 0:
                lo = lo + last
            else:
                hi = hi + last
            send2[d, :, part_of(n, 0)] = lo.astype(BF)
            send2[d, :, part_of(n, 1)] = hi.astype(BF)
            rcopy(3, d, n).start()

    def slots4_in(n):
        for d in (0, 1):
            with jax.named_scope(f"r3b_{n}{d}"):
                rcopy(2, d, n).wait_recv()
            exchange(got4, ret4, d, half_of(n), ssem.at[bs], brecv.at[d, n])

    slots4_in(0)
    ystart(3, 1)
    slots3_in(2)
    slots4_in(1)
    ystart(4, 1)
    sums2_out(0)
    slots3_in(3)
    slots4_in(2)
    sums2_out(1)
    slots4_in(3)
    sums2_out(2)
    ystart(2)
    sums2_out(3)
    with jax.named_scope("yw12"):
        ywait(1)
        ywait(2)
    ystart(0)
    for n, d in both:
        cols = cols_of(n)
        here = combine(spread(near[d], z), ret1[d, :, cols])
        with jax.named_scope(f"r2_{n}{d}"):
            rcopy(3, d, n).wait_recv()
        total = part2[d, :, cols].astype(F32) + here
        send1[d, :, cols] = total.astype(BF)
        rcopy(4, d, n).start()
    ywait(0)
    own = spread(0, z)
    for n in range(NC):
        cols = cols_of(n)
        total = res_ref[:, cols].astype(F32) + combine(own, ret0[:, cols])
        with jax.named_scope(f"r1_{n}"):
            wait_bytes(part1.at[:, :, cols], rrecv.at[8, n])
        total = total + part1[0, :, cols].astype(F32) + part1[1, :, cols].astype(F32)
        out_ref[:, cols] = total.astype(BF)
    with jax.named_scope("ends"):
        flat = ((near_z, 4 * tok), (far_z, 4 * grp), (back_near, 4 * tok), (back_far, 4 * grp), (xs, 5 * others), (ys, 5 * others))
        flat += ((gs, 3 * others), (bs, 3 * others), (ring, 3 * chan), (rows_t, 3 * tok * chan // width), (normed_z, 2 * ntp * tok * chan // width))
        for kind, rows in flat:
            wait_bytes(arrived.at[0:rows, :], ssem.at[kind])
        wait_bytes(gainrel.at[1:ntp], ssem.at[gains_t])
        wait_bytes(halo, ssem.at[halo_t])
        wait_bytes(metas.at[0:4], ssem.at[metas_z])


def body(
    residual_in,
    gate_outer,
    gate_inner,
    conv_input,
    conv_taps,
    norm_gain,
    out_weight,
    moe_gain,
    expert_ids,
    group_prob,
    route_prob,
    expert_gate,
    expert_up,
    expert_down,
):
    tok, width = residual_in.shape
    seq, chan = conv_input.shape
    fe = expert_gate.shape[2]
    ntp = lax.axis_size("tp")
    nj = lax.axis_size("sp") // NZ
    grp = nj * CAP
    vmem = pl.BlockSpec(memory_space=pltpu.VMEM)
    hbm = pl.BlockSpec(memory_space=pl.ANY)
    dma = pltpu.SemaphoreType.DMA
    shapes = [
        ((conv_taps.shape[0], chan), BF),
        ((chan,), BF),
        ((width,), BF),
        ((2, tok), jnp.int32),
        ((1, tok), F32),
        ((2, tok), F32),
        ((tok, width), BF),
        ((seq, chan), BF),
        ((seq, chan), BF),
        ((seq, chan), BF),
        ((chan, width), BF),
        ((2, 16, chan), BF),
        ((seq + 8, chan), F32),
        ((seq, chan), BF),
        ((ntp, tok, chan), BF),
        ((8, chan), F32),
        ((ntp, 8, chan), F32),
        ((ntp, tok, chan), BF),
        ((2, ntp, tok, chan), BF),
        ((ntp, chan, width), BF),
        ((tok, width), BF),
        ((8, tok), F32),
        ((2 * grp, 128), F32),
        ((2 * grp, fe), F32),
        ((2 * grp, fe), F32),
        ((8, width), F32),
        ((5, grp, tok), BF),
        ((NZ, 8, tok), F32),
        ((2, tok, width), BF),
        ((2, tok, width), BF),
        ((2, grp, tok), BF),
        ((2, grp, tok), BF),
        ((2, grp, width), BF),
        ((2, grp, width // 2), BF),
        ((2, grp, width), BF),
        ((2, grp, width // 2), BF),
        ((2, grp, width // 2), BF),
        ((5, grp, width), BF),
        ((8 * grp, width), BF),
        ((8 * grp, width), BF),
        ((grp, width), BF),
        ((2, grp, width), BF),
        ((2, grp, width), BF),
        ((2, grp, width), BF),
        ((2, grp, width // 2), BF),
        ((2, grp, width // 2), BF),
        ((2, grp, width), BF),
        ((2, grp, width // 2), BF),
        ((2, tok, width), BF),
        ((2, tok, width), BF),
        ((2, tok, width), BF),
        ((2, tok, width), BF),
        ((2 * grp, fe), BF),
        ((width, fe), BF),
        ((width, fe), BF),
        ((fe, width), BF),
    ]
    sems = [(5,), (6,), (3,), (14,), (3,), (4, NC), (2,), (2, 2), (8, NC), (5,), (7,), (2, NC), (2, NC), (9, NC)]
    return pl.pallas_call(
        layer_kernel,
        out_shape=pltpu.VMEM((tok, width), BF),
        in_specs=[hbm] * 14,
        out_specs=vmem,
        scratch_shapes=[pltpu.VMEM(s, t) for s, t in shapes] + [dma(s) for s in sems],
        compiler_params=pltpu.CompilerParams(
            collective_id=0, has_side_effects=True, vmem_limit_bytes=61 * 1024 * 1024
        ),
        name="layer",
    )(
        residual_in,
        gate_outer,
        gate_inner,
        conv_input,
        out_weight,
        expert_gate,
        expert_up,
        expert_down,
        conv_taps,
        norm_gain,
        moe_gain,
        expert_ids.T,
        group_prob.reshape(1, tok),
        route_prob.T,
    )


def solution(mesh):
    in_specs = (
        P(("sp", "tp"), None),
        P("sp", "tp"),
        P("sp", "tp"),
        P("sp", "tp"),
        P(None, "tp"),
        P("tp"),
        P("tp", None),
        P(),
        P(("sp", "tp"), None),
        P(("sp", "tp")),
        P(("sp", "tp"), None),
        P("sp", None, None),
        P("sp", None, None),
        P("sp", None, None),
    )
    out_specs = P(("sp", "tp"), None)
    return jax.shard_map(body, mesh=mesh, in_specs=in_specs, out_specs=out_specs, check_vma=False)
```
